32 devices in a mesh: ep: 8 (over z, core), tp: 4 (over y, x).
Axes of the slice: x: 2, y: 2, z: 4, core: 2. Of those that a mesh axis runs over, the one named last changes fastest.
Arguments:
- query_vectors: bfloat16 [4096, 4096], P('ep', 'tp'), may hold values from -6 to 6
- key_vectors: bfloat16 [4096, 2048], P('ep', 'tp'), may hold values from -6 to 6
- value_vectors: bfloat16 [4096, 2048], P('ep', 'tp'), may hold values from -64 to 64
- query_gain: float32 [128], replicated, may hold values from 0.1 to 1.9
- key_gain: float32 [128], replicated, may hold values from 0.1 to 1.9
- sink_logits: float32 [32], P('tp'), may hold values from 3 to 7
- moe_rows: bfloat16 [1280, 4096], P('ep', 'tp'), may hold values from -6 to 6
- norm_gain: float32 [4096], replicated, may hold values from 0.1 to 1.9
- expert_ids: int32 [1280, 4], P('ep'), may hold values from 0 to 7, all different within a row; in each aligned block of 160 rows (0 to 159, 160 to 319, ...) at most 120 rows name the same one
- route_weights: float32 [1280, 4], P('ep'), may hold values from 0.25 to 2.5
- expert_gate: bfloat16 [8, 4096, 2048], P('ep', None, 'tp'), may hold values from -0.09375 to 0.09375
- expert_up: bfloat16 [8, 4096, 2048], P('ep', None, 'tp'), may hold values from -0.09375 to 0.09375
- expert_down: bfloat16 [8, 2048, 4096], P('ep', None, 'tp'), may hold values from -0.125 to 0.125
- shared_gate: bfloat16 [4096, 512], P(None, 'tp'), may hold values from -0.09375 to 0.09375
- shared_up: bfloat16 [4096, 512], P(None, 'tp'), may hold values from -0.09375 to 0.09375
- shared_down: bfloat16 [512, 4096], P(None, 'tp'), may hold values from -0.25 to 0.25
Outputs:
- attended: bfloat16 [4096, 4096], P('ep', 'tp')
- moe_out: bfloat16 [1280, 4096], P('ep', 'tp')
The draws below stay inside these ranges and needn't reach their ends.
Inputs may be any that keep to these rules, and one draw needn't show every extreme that they name: `expert_ids`: each row names 4 different experts. Within the rows of one index of ep (aligned blocks of 160 rows), no expert is named by more than 120 rows, and in some block one expert is named by exactly 120.
All inputs are finite; a program needn't handle non-finite values.
Results may differ from the reference program's by a relative error of at most 0.0071.
Values may be sent and summed in bfloat16 or wider, within the bound.
A program may use at most 128 MiB of HBM per device.

```python
import math
import jax
import jax.numpy as jnp
import numpy as np
from jax import lax

HEAD_DIM = 128
HEADS = 32
KV_HEADS = 16
GROUP = 2
WINDOW = 128
GRID_W = 64
TOK_A = 512
SEQ_A = 4096
D = 4096
F = 2048
FS = 512
TOP_K = 4
TOK_B = 160
TOKENS_B = 1280
EXPERTS = 8
CAP = 120


def levels(stream_key, shape, shards, least, largest):
    def one(position, parts):
        steps = jax.random.uniform(jax.random.fold_in(jax.random.fold_in(stream_key, 6), position), (parts,), jnp.float32, least / len(shards), largest / len(shards))
        return jnp.repeat(jnp.exp(steps), shape[position] // parts).reshape((-1,) + (1,) * (len(shape) - position - 1))

    loudness = one(*shards[0])
    for cut in shards[1:]:
        loudness = loudness * one(*cut)
    return loudness


def shared_out(key, own, number, rows, number_of, top, bound, lean):
    sequence = jax.random.permutation(key, number_of)
    heavy_load, ordinary = portions_of(number_of, rows * top, bound, lean, True), portions_of(number_of, rows * top, bound, lean, False)
    places = jnp.arange(number_of)

    def named(sizes, offset_by):
        used = int((sizes > 0).sum())
        fixed = max(1, used // 4)
        shifted = fixed + (places - fixed + offset_by * (used - fixed)) % max(1, number_of - fixed)
        return jnp.zeros((number_of,), jnp.int32).at[sequence[jnp.where(places < fixed, places, shifted)]].set(jnp.asarray(sizes, jnp.int32))

    sizes = jnp.where(number % 4 == 0, named(heavy_load, number // 4), named(ordinary, number - number // 4 - 1))
    mixed = jax.random.permutation(jax.random.fold_in(own, 3), number_of)
    giver, receiver = mixed[0:number_of // 2 * 2:2], mixed[1:number_of // 2 * 2:2]
    room = jnp.minimum(sizes[giver] - 1, bound - sizes[receiver]) // 2
    room = jnp.where((giver == sequence[0]) | (receiver == sequence[0]) | (sizes[receiver] == 0), 0, jnp.maximum(room, 0))
    shifted = jax.random.randint(jax.random.fold_in(own, 4), (number_of // 2,), 0, 1 << 20) % (room + 1)
    sizes = sizes.at[giver].add(-shifted).at[receiver].add(shifted)
    items = jnp.searchsorted(jnp.cumsum(sizes), jnp.arange(rows * top), side="right").astype(jnp.int32)
    table = items.reshape(top, rows).T
    table = table[jax.random.permutation(jax.random.fold_in(own, 1), rows)]
    offset_by = jax.random.randint(jax.random.fold_in(own, 2), (rows, 1), 0, top)
    return jnp.take_along_axis(table, (jnp.arange(top)[None, :] + offset_by) % top, axis=1)


def portions_of(amount, total, most, skew, full):
    portions = [(1 << 20) // math.isqrt(standing ** skew) + 1 for standing in range(1, amount + 1)]
    largest = most if full else min(most, max(-(-total // amount), total * portions[0] // sum(portions)))
    least = 1 if total - largest >= amount - 1 else 0
    holding, rest = [largest] + [least] * (amount - 1), total - largest - least * (amount - 1)
    while rest > 0:
        free = [i for i in range(1, amount) if holding[i] < largest] or [i for i in range(1, amount) if holding[i] < most]
        pool, budget = sum([portions[i] for i in free]), rest
        for i in free:
            extra = min(most - holding[i], max(1, budget * portions[i] // pool), rest)
            holding[i] = holding[i] + extra
            rest = rest - extra
    return np.array(holding)


def gaussian(own_key, shape, width, reach, cuts=(), kind=jnp.bfloat16):
    result = width * jax.random.normal(own_key, shape, jnp.float32)
    if cuts:
        result = result * levels(own_key, shape, cuts, -0.22, 0.18)
    return jnp.clip(result, -reach, reach).astype(kind)


def setup_inputs(seed: int = 0) -> dict:
    seeds = jax.random.split(jax.random.key(seed), 17)
    query_vectors = gaussian(seeds[0], (SEQ_A, HEADS * HEAD_DIM), 1.0, 6.0, ((0, 8), (1, 4)))
    key_vectors = gaussian(seeds[1], (SEQ_A, KV_HEADS * HEAD_DIM), 1.0, 6.0, ((0, 8), (1, 4)))
    value_vectors = gaussian(seeds[2], (SEQ_A, KV_HEADS * HEAD_DIM), 12.0, 64.0, ((0, 8), (1, 4)))
    query_gain = jnp.clip(1.0 + 0.18 * jax.random.normal(seeds[3], (HEAD_DIM,), jnp.float32), 0.1, 1.9)
    key_gain = jnp.clip(1.0 + 0.18 * jax.random.normal(seeds[4], (HEAD_DIM,), jnp.float32), 0.1, 1.9)
    sink_logits = jnp.clip(3.0 + 4.0 * jax.random.uniform(seeds[5], (HEADS,), jnp.float32) ** levels(seeds[5], (HEADS,), ((0, 4),), -0.2, 0.2), 3.0, 7.0)
    moe_rows = gaussian(seeds[6], (TOKENS_B, D), 1.0, 6.0, ((0, 8), (1, 4)))
    norm_gain = jnp.clip(1.0 + 0.18 * jax.random.normal(seeds[7], (D,), jnp.float32), 0.1, 1.9)
    expert_ids_keys = jax.random.split(jax.random.fold_in(seeds[8], 1), TOKENS_B // TOK_B)
    expert_ids_turns = jax.random.permutation(jax.random.fold_in(seeds[8], 3), TOKENS_B // TOK_B)
    expert_ids = jax.vmap(lambda own, number: shared_out(jax.random.fold_in(seeds[8], 2), own, number, TOK_B, EXPERTS, TOP_K, CAP, 2))(expert_ids_keys, expert_ids_turns).reshape((TOKENS_B, TOP_K))
    route_weights = jnp.clip(jnp.exp(math.log(2.5) - 2.3025851 * jax.random.uniform(seeds[9], (TOKENS_B, TOP_K), jnp.float32) ** levels(seeds[9], (TOKENS_B, TOP_K), ((0, 8),), -0.2, 0.2)), 0.25, 2.5)
    expert_gate = gaussian(seeds[10], (EXPERTS, D, F), D ** -0.5, 0.09375, ((0, 8), (2, 4)))
    expert_up = gaussian(seeds[11], (EXPERTS, D, F), D ** -0.5, 0.09375, ((0, 8), (2, 4)))
    expert_down = gaussian(seeds[12], (EXPERTS, F, D), F ** -0.5, 0.125, ((0, 8), (2, 4)))
    shared_gate = gaussian(seeds[13], (D, FS), D ** -0.5, 0.09375, ((1, 4),))
    shared_up = gaussian(seeds[14], (D, FS), D ** -0.5, 0.09375, ((1, 4),))
    shared_down = gaussian(seeds[15], (FS, D), FS ** -0.5, 0.25, ((1, 4),))
    return dict(query_vectors=query_vectors, key_vectors=key_vectors, value_vectors=value_vectors, query_gain=query_gain, key_gain=key_gain, sink_logits=sink_logits, moe_rows=moe_rows, norm_gain=norm_gain, expert_ids=expert_ids, route_weights=route_weights, expert_gate=expert_gate, expert_up=expert_up, expert_down=expert_down, shared_gate=shared_gate, shared_up=shared_up, shared_down=shared_down)


epsilon = 1e-06
rotary_base = 10000.0

def half_turn(halves):
    leading, trailing = jnp.split(halves, 2, axis=-1)
    return jnp.concatenate([-trailing, leading], axis=-1)

def rotate_heads(vectors, head_gain, positions):
    floats = vectors.astype(jnp.float32)
    normed = floats * lax.rsqrt(lax.optimization_barrier(jnp.mean(floats * floats, axis=-1, keepdims=True)) + epsilon) * head_gain
    quarter = HEAD_DIM // 4
    freq_index = jnp.arange(quarter, dtype=jnp.int32).astype(jnp.float32)
    inverse = rotary_base ** (-4.0 * freq_index / HEAD_DIM)
    grid_row = (positions // GRID_W).astype(jnp.float32)[:, None] * inverse
    grid_col = (positions % GRID_W).astype(jnp.float32)[:, None] * inverse
    angles = jnp.concatenate([grid_row, grid_row, grid_col, grid_col], axis=-1)[:, None, :]
    row_half, col_half = jnp.split(normed, 2, axis=-1)
    turned = jnp.concatenate([half_turn(row_half), half_turn(col_half)], axis=-1)
    return (normed * jnp.cos(angles) + turned * jnp.sin(angles)).astype(jnp.bfloat16)

def activate(block_rows, gate_weight, up_weight, factor):
    gate_sum = jnp.dot(block_rows, gate_weight, preferred_element_type=jnp.float32) * factor[:, None]
    up_sum = jnp.dot(block_rows, up_weight, preferred_element_type=jnp.float32) * factor[:, None]
    return (jax.nn.silu(gate_sum) * up_sum).astype(jnp.bfloat16)

def windowed(query_vectors, key_vectors, value_vectors, query_gain, key_gain, sink_logits):
    positions = jnp.arange(SEQ_A, dtype=jnp.int32)
    queries = rotate_heads(query_vectors.reshape(SEQ_A, HEADS, HEAD_DIM), query_gain, positions)
    turned_keys = rotate_heads(key_vectors.reshape(SEQ_A, KV_HEADS, HEAD_DIM), key_gain, positions)
    values = value_vectors.reshape(SEQ_A, KV_HEADS, HEAD_DIM)
    padding = ((WINDOW, WINDOW), (0, 0), (0, 0))
    padded_keys = jnp.pad(turned_keys, padding)
    padded_values = jnp.pad(values, padding)
    blocks = SEQ_A // TOK_A
    query_blocks = queries.reshape(blocks, TOK_A, KV_HEADS, GROUP, HEAD_DIM)
    sink_scale = jnp.exp(sink_logits).reshape(KV_HEADS, GROUP)
    extent = TOK_A + 2 * WINDOW
    score_scale = HEAD_DIM ** (-0.5)

    def attend_block(packed):
        query_block, block_index = packed
        first_row = (block_index * TOK_A).astype(jnp.int32)
        near_keys = lax.dynamic_slice_in_dim(padded_keys, first_row, extent, 0)
        near_values = lax.dynamic_slice_in_dim(padded_values, first_row, extent, 0)
        query_pos = first_row + jnp.arange(TOK_A, dtype=jnp.int32)
        key_pos = first_row - WINDOW + jnp.arange(extent, dtype=jnp.int32)
        inside = (jnp.abs(query_pos[:, None] - key_pos[None, :]) <= WINDOW) & (key_pos >= 0)[None, :] & (key_pos < SEQ_A)[None, :]
        scores = jnp.einsum('qhgd,khd->hgqk', query_block.astype(jnp.float32), near_keys.astype(jnp.float32)) * score_scale
        raised = jnp.where(inside, jnp.exp(scores), 0.0)
        denominator = sink_scale[:, :, None] + lax.optimization_barrier(jnp.sum(raised, axis=-1))
        weights = (raised / denominator[..., None]).astype(jnp.bfloat16)
        mixed = jnp.einsum('hgqk,khd->qhgd', weights.astype(jnp.float32), near_values.astype(jnp.float32))
        return mixed.astype(jnp.bfloat16).reshape(TOK_A, HEADS * HEAD_DIM)
    outputs = lax.map(attend_block, (query_blocks, jnp.arange(blocks, dtype=jnp.int32)))
    return outputs.reshape(SEQ_A, HEADS * HEAD_DIM)

def moe_layer(moe_rows, norm_gain, expert_ids, route_weights, expert_gate, expert_up, expert_down, shared_gate, shared_up, shared_down):
    floats = moe_rows.astype(jnp.float32)
    inverse_rms = lax.rsqrt(lax.optimization_barrier(jnp.mean(floats * floats, axis=-1)) + epsilon)
    scaled = (floats * norm_gain).astype(jnp.bfloat16)
    shared_hidden = activate(scaled, shared_gate, shared_up, inverse_rms)
    shared_result = jnp.dot(shared_hidden, shared_down, preferred_element_type=jnp.float32)
    blocks = TOKENS_B // TOK_B
    flat_ids = expert_ids.reshape(blocks, TOK_B * TOP_K).astype(jnp.int32)
    onehot = (flat_ids[:, :, None] == jnp.arange(EXPERTS, dtype=jnp.int32)[None, None, :]).astype(jnp.int32)
    slot_index = lax.optimization_barrier(jnp.sum((jnp.cumsum(onehot, axis=1) - onehot) * onehot, axis=-1)).astype(jnp.int32)
    owner_row = jnp.arange(TOK_B * TOP_K, dtype=jnp.int32) // TOP_K
    scaled_blocks = scaled.reshape(blocks, TOK_B, D)
    rms_blocks = inverse_rms.reshape(blocks, TOK_B)
    capacity_index = jnp.arange(CAP, dtype=jnp.int32)

    def one_expert(packed):
        expert, gate_weight, up_weight, down_weight = packed
        matches = (flat_ids == expert)[:, :, None] & (slot_index[:, :, None] == capacity_index[None, None, :])
        present = jnp.any(matches, axis=1)
        source_row = lax.optimization_barrier(jnp.sum(jnp.where(matches, owner_row[None, :, None], 0), axis=1)).astype(jnp.int32)
        picked = jnp.take_along_axis(scaled_blocks, source_row[:, :, None], axis=1)
        picked = jnp.where(present[:, :, None], picked, jnp.zeros((), jnp.bfloat16))
        factor = jnp.where(present, jnp.take_along_axis(rms_blocks, source_row, axis=1), 0.0)
        hidden = activate(picked.reshape(blocks * CAP, D), gate_weight, up_weight, factor.reshape(blocks * CAP))
        return jnp.dot(hidden, down_weight, preferred_element_type=jnp.float32).astype(jnp.bfloat16).reshape(blocks, CAP, D)
    results = lax.map(one_expert, (jnp.arange(EXPERTS, dtype=jnp.int32), expert_gate, expert_up, expert_down))
    block_ids = expert_ids.reshape(blocks, TOK_B, TOP_K).astype(jnp.int32)
    block_slots = slot_index.reshape(blocks, TOK_B, TOP_K)
    source_block = jnp.arange(blocks, dtype=jnp.int32)[:, None, None]
    gathered = results[block_ids, source_block, block_slots]
    routed = lax.optimization_barrier(jnp.sum(route_weights.reshape(blocks, TOK_B, TOP_K, 1) * gathered.astype(jnp.float32), axis=2))
    return (shared_result + routed.reshape(TOKENS_B, D)).astype(jnp.bfloat16)

def reference(query_vectors, key_vectors, value_vectors, query_gain, key_gain, sink_logits, moe_rows, norm_gain, expert_ids, route_weights, expert_gate, expert_up, expert_down, shared_gate, shared_up, shared_down):
    attended = windowed(query_vectors, key_vectors, value_vectors, query_gain, key_gain, sink_logits)
    moe_out = moe_layer(moe_rows, norm_gain, expert_ids, route_weights, expert_gate, expert_up, expert_down, shared_gate, shared_up, shared_down)
    return (attended, moe_out)
```

```python
import functools
import math

import jax
import jax.numpy as jnp
from jax import lax
from jax.experimental import pallas as pl
from jax.experimental.pallas import tpu as pltpu
from jax.sharding import PartitionSpec as P

HEAD_DIM = 128
WINDOW = 128
GRID_W = 64
D = 4096
TOP_K = 4


epsilon = 1e-06
rotary_base = 10000.0


def padded_2(block, sides, width):
    for axis, dim in sides:
        count = lax.axis_size(axis)
        forward = [(i, i + 1) for i in range(count - 1)]
        backward = [(target, source) for source, target in forward]
        low = lax.ppermute(
            lax.slice_in_dim(block, block.shape[dim] - width, None, axis=dim), axis, forward
        )
        high = lax.ppermute(lax.slice_in_dim(block, 0, width, axis=dim), axis, backward)
        block = jnp.concatenate([low, block, high], axis=dim)
    return block


def half_turn(halves):
    leading, trailing = jnp.split(halves, 2, axis=-1)
    return jnp.concatenate([-trailing, leading], axis=-1)


def rotate_heads(vectors, head_gain, positions):
    floats = vectors.astype(jnp.float32)
    normed = (
        floats * lax.rsqrt(jnp.mean(floats * floats, axis=-1, keepdims=True) + epsilon) * head_gain
    )
    quarter = HEAD_DIM // 4
    freq_index = jnp.arange(quarter, dtype=jnp.int32).astype(jnp.float32)
    inverse = rotary_base ** (-4.0 * freq_index / HEAD_DIM)
    grid_row = (positions // GRID_W).astype(jnp.float32)[:, None] * inverse
    grid_col = (positions % GRID_W).astype(jnp.float32)[:, None] * inverse
    angles = jnp.concatenate([grid_row, grid_row, grid_col, grid_col], axis=-1)[:, None, :]
    row_half, col_half = jnp.split(normed, 2, axis=-1)
    turned = jnp.concatenate([half_turn(row_half), half_turn(col_half)], axis=-1)
    return (normed * jnp.cos(angles) + turned * jnp.sin(angles)).astype(jnp.bfloat16)


def attend_window(query_vectors, key_vectors, value_vectors, query_gain, key_gain, sink_logits):
    length = query_vectors.shape[0]
    heads_here = sink_logits.shape[0]
    kv_here = key_vectors.shape[1] // HEAD_DIM
    grouping = heads_here // kv_here
    shard_start = lax.axis_index("ep") * length
    positions = shard_start + jnp.arange(length, dtype=jnp.int32)
    queries = rotate_heads(
        query_vectors.reshape(length, heads_here, HEAD_DIM), query_gain, positions
    )
    turned_keys = rotate_heads(key_vectors.reshape(length, kv_here, HEAD_DIM), key_gain, positions)
    turned_keys = turned_keys.reshape(length, kv_here * HEAD_DIM)
    padded = padded_2(jnp.stack([turned_keys, value_vectors]), (("ep", 1),), WINDOW)
    extent = length + 2 * WINDOW
    near_keys = padded[0].reshape(extent, kv_here, HEAD_DIM)
    near_values = padded[1].reshape(extent, kv_here, HEAD_DIM)
    key_pos = shard_start - WINDOW + jnp.arange(extent, dtype=jnp.int32)
    inside = (
        (jnp.abs(positions[:, None] - key_pos[None, :]) <= WINDOW)
        & (key_pos >= 0)[None, :]
        & (key_pos < lax.axis_size("ep") * length)[None, :]
    )
    scores = jnp.einsum(
        "qhgd,khd->hgqk",
        queries.reshape(length, kv_here, grouping, HEAD_DIM),
        near_keys,
        preferred_element_type=jnp.float32,
    ) * HEAD_DIM ** (-0.5)
    raised = jnp.where(inside, jnp.exp(scores), 0.0)
    denominator = jnp.exp(sink_logits).reshape(kv_here, grouping)[:, :, None] + jnp.sum(
        raised, axis=-1
    )
    weights = (raised / denominator[..., None]).astype(jnp.bfloat16)
    mixed = jnp.einsum("hgqk,khd->qhgd", weights, near_values, preferred_element_type=jnp.float32)
    return mixed.astype(jnp.bfloat16).reshape(length, heads_here * HEAD_DIM)


def project(block_rows, gain_piece, gate_rows, up_rows):
    floats = block_rows.astype(jnp.float32)
    weighted = (floats * gain_piece).astype(jnp.bfloat16)
    gate_sum = jnp.dot(weighted, gate_rows, preferred_element_type=jnp.float32)
    up_sum = jnp.dot(weighted, up_rows, preferred_element_type=jnp.float32)
    return (gate_sum, up_sum, jnp.sum(floats * floats, axis=1))


def activate(gate_sum, up_sum, squares):
    factor = lax.rsqrt(squares / D + epsilon)[:, None]
    return (jax.nn.silu(gate_sum * factor) * (up_sum * factor)).astype(jnp.bfloat16)


def shards(
    query_vectors,
    key_vectors,
    value_vectors,
    query_gain,
    key_gain,
    sink_logits,
    moe_rows,
    norm_gain,
    expert_ids,
    route_weights,
    expert_gate,
    expert_up,
    expert_down,
    shared_gate,
    shared_up,
    shared_down,
):
    attended = attend_window(
        query_vectors, key_vectors, value_vectors, query_gain, key_gain, sink_logits
    )
    ep_size = lax.axis_size("ep")
    tokens_here, width_here = moe_rows.shape
    capacity = max(2, 3 * tokens_here * TOP_K // (2 * ep_size))
    slots_all = ep_size * capacity
    flat_ids = expert_ids.reshape(-1)
    onehot = (flat_ids[:, None] == jnp.arange(ep_size, dtype=jnp.int32)[None, :]).astype(jnp.int32)
    slot_index = jnp.sum((jnp.cumsum(onehot, axis=0) - onehot) * onehot, axis=1)
    target = flat_ids * capacity + slot_index
    matches = target[None, :] == jnp.arange(slots_all, dtype=jnp.int32)[:, None]
    present = jnp.any(matches, axis=1)
    owner_row = jnp.arange(tokens_here * TOP_K, dtype=jnp.int32) // TOP_K
    source_row = jnp.sum(jnp.where(matches, owner_row[None, :], 0), axis=1)
    local_gate = expert_gate[0]
    local_up = expert_up[0]
    local_down = expert_down[0]
    units_here = local_gate.shape[1]
    shared_units = shared_gate.shape[1]
    outgoing = jnp.where(
        present[:, None], jnp.take(moe_rows, source_row, axis=0), jnp.zeros((), jnp.bfloat16)
    )
    arrived = lax.all_to_all(
        outgoing.reshape(ep_size, capacity, width_here),
        "ep",
        split_axis=0,
        concat_axis=0,
        tiled=True,
    )
    arrived = arrived.reshape(slots_all, width_here)
    routed = project(
        lax.all_gather(arrived, "tp", axis=1, tiled=True), norm_gain, local_gate, local_up
    )
    shared = project(
        lax.all_gather(moe_rows, "tp", axis=1, tiled=True), norm_gain, shared_gate, shared_up
    )
    gate_sum, up_sum, squares, shared_gsum, shared_usum, own_squares = tuple(
        (new_term for new_term in routed + shared)
    )
    hidden = activate(gate_sum, up_sum, squares)
    shared_hidden = activate(shared_gsum, shared_usum, own_squares)
    packing = units_here // shared_units
    stacked = jnp.concatenate(
        [hidden, shared_hidden.reshape(tokens_here // packing, units_here)], axis=0
    )
    columns = local_down.shape[1]
    portion = lax.all_gather(stacked, "tp", axis=1, tiled=True)
    shards_in = portion.shape[1] // units_here
    routed = jnp.dot(portion[:slots_all], local_down, preferred_element_type=jnp.float32)
    shared_piece = portion[slots_all:].reshape(
        tokens_here // packing, shards_in, packing, shared_units
    )
    shared_piece = shared_piece.transpose(0, 2, 1, 3).reshape(tokens_here, shards_in * shared_units)
    shared = jnp.dot(shared_piece, shared_down, preferred_element_type=jnp.float32)
    returned = lax.all_to_all(
        routed.astype(jnp.bfloat16).reshape(ep_size, capacity, columns),
        "ep",
        split_axis=0,
        concat_axis=0,
        tiled=True,
    )
    returned = returned.reshape(slots_all, columns)
    picked = jnp.take(returned, target, axis=0).reshape(tokens_here, TOP_K, columns)
    combined = shared + jnp.sum(route_weights[:, :, None] * picked.astype(jnp.float32), axis=1)
    return (attended, combined.astype(jnp.bfloat16))


F32 = jnp.float32
BF16 = jnp.bfloat16
MESH = pl.DeviceIdType.MESH
LANES = 128


def line_kernel(
    sizes,
    q_hbm,
    k_hbm,
    v_hbm,
    qgain_ref,
    kgain_ref,
    sink_ref,
    x_hbm,
    gain_ref,
    ids_ref,
    rw_ref,
    gate_hbm,
    up_hbm,
    down_hbm,
    sgate_hbm,
    sup_hbm,
    sdown_hbm,
    att_hbm,
    out_hbm,
    xbuf,
    gate,
    up,
    down,
    sgate,
    sup,
    sdown,
    qraw,
    qbuf,
    kraw,
    kbuf,
    vbuf,
    abuf,
    obuf,
    base,
    cos_ref,
    sin_ref,
    wbuf,
    scaled,
    factor,
    hid,
    hbuf,
    shbuf,
    pbuf,
    prx,
    qtx,
    qrx,
    lsem,
    asem,
    osem,
    zts,
    ztr,
    zds,
    zdr,
    xs,
    xr,
    ys,
    yr,
    fs,
    fr,
    ps,
    pr,
    hxs,
    hxr,
    hys,
    hyr,
    gxs,
    gxr,
    gys,
    gyr,
    ss,
    sr,
    ws,
    wr,
    ks,
    kr,
    pps,
    ppr,
    qqs,
    qqr,
):
    ep, tp, nz, tok, width, cap, tok_a, kv_heads, group, units, columns, sunits = sizes
    e = lax.axis_index("ep")
    t = lax.axis_index("tp")
    z, c = e // 2, e % 2
    other = 1 - c
    partner = z * 2 + other
    tx, ty = t % 2, t // 2
    xn = ty * 2 + (1 - tx)
    yn = (1 - ty) * 2 + tx
    dn = (1 - ty) * 2 + (1 - tx)
    half = tok // 2
    slots = 2 * cap
    hcut = (slots // 2 + 15) // 16 * 16
    row_c = pl.multiple_of(c * tok, 16)
    row_o = pl.multiple_of(other * tok, 16)
    has_up, has_down = z < nz - 1, z > 0
    is_end = (z == 0) | (z == nz - 1)
    is_mid = jnp.logical_not(is_end)

    def by_z(*values):
        r = values[0]
        for i in range(1, nz):
            r = jnp.where(z == i, values[i], r)
        return r

    order = (z, by_z(1, 2, 1, 2), by_z(3, 3, 0, 0), by_z(2, 0, 3, 1))
    k1, k2 = by_z(1, 2, 1, 2), by_z(2, 0, 3, 1)
    k3, k4 = by_z(1, 0, 3, 2), by_z(3, 3, 0, 0)
    k5, k6 = by_z(3, 2, 1, 0), by_z(2, 3, 0, 1)

    def at_step(s):
        r = order[0]
        for i in range(1, nz):
            r = jnp.where(s == i, order[i], r)
        return r

    def rc(src, dst, s_sem, r_sem, dev):
        return pltpu.make_async_remote_copy(
            src_ref=src,
            dst_ref=dst,
            send_sem=s_sem,
            recv_sem=r_sem,
            device_id=dev,
            device_id_type=MESH,
        )

    loads = [
        (x_hbm, xbuf.at[z, t, pl.ds(row_c, tok), :]),
        (q_hbm, qraw),
        (k_hbm, kraw.at[pl.ds(WINDOW, tok_a), :]),
        (v_hbm, vbuf.at[pl.ds(WINDOW, tok_a), :]),
        (gate_hbm.at[0], gate),
        (up_hbm.at[0], up),
        (sgate_hbm, sgate),
        (sup_hbm, sup),
        (down_hbm.at[0], down),
        (sdown_hbm, sdown),
    ]
    copies = [pltpu.make_async_copy(a, b, lsem.at[i]) for i, (a, b) in enumerate(loads)]

    barrier = pltpu.get_barrier_semaphore()
    for d in range(1, ep):
        pl.semaphore_signal(barrier, inc=1, device_id=((e + d) % ep, t), device_id_type=MESH)
    for d in range(1, tp):
        pl.semaphore_signal(barrier, inc=1, device_id=(e, (t + d) % tp), device_id_type=MESH)
    for cp in copies:
        cp.start()

    quarter = HEAD_DIM // 4
    half_head = HEAD_DIM // 2
    extent = tok_a + 2 * WINDOW
    grid_rows = extent // GRID_W
    first_row = (e * tok_a - WINDOW) // GRID_W

    def angles(count, start):
        lane = lax.broadcasted_iota(jnp.int32, (count, LANES), 1)
        place = lax.broadcasted_iota(jnp.int32, (count, LANES), 0)
        exponent = (lane % quarter).astype(F32) * (-4.0 / HEAD_DIM)
        return (place + start).astype(F32) * jnp.exp(exponent * math.log(rotary_base))

    row_pad = (grid_rows + 7) // 8 * 8
    row_angles = angles(row_pad, first_row)
    col_angles = angles(GRID_W, 0)
    row_cos, row_sin = jnp.cos(row_angles), jnp.sin(row_angles)
    col_cos, col_sin = jnp.cos(col_angles), jnp.sin(col_angles)
    lane64 = lax.broadcasted_iota(jnp.int32, (GRID_W, LANES), 1)
    sign = jnp.where(lane64 % half_head < quarter, -1.0, 1.0)
    for g in range(grid_rows):
        rows = slice(g * GRID_W, (g + 1) * GRID_W)
        cos_ref[rows, :] = jnp.where(lane64 < half_head, row_cos[g : g + 1, :], col_cos)
        sin_ref[rows, :] = jnp.where(lane64 < half_head, row_sin[g : g + 1, :], col_sin) * sign

    padded_tok = wbuf.shape[2]
    expert = lax.broadcasted_iota(jnp.int32, (tok, LANES), 1)
    by_token = jnp.zeros((tok, LANES), F32)
    for k in range(TOP_K):
        by_token += jnp.where(ids_ref[:, k : k + 1] == expert, rw_ref[:, k : k + 1], 0.0)
    if padded_tok > tok:
        by_token = jnp.concatenate(
            [by_token, jnp.zeros((padded_tok - tok, LANES), F32)], axis=0
        )
    wbuf[e] = by_token.T[:ep, :]

    pl.semaphore_wait(barrier, ep + tp - 2)

    def unit(zi, ti, row, first=0, count=tok):
        return xbuf.at[zi, ti, pl.ds(row + first, count), :]

    up_z = jnp.minimum(z + 1, nz - 1) * 2 + c
    down_z = jnp.maximum(z - 1, 0) * 2 + c

    def zt_copy(zi, way):
        u = unit(zi, t, row_c)
        return rc(u, u, zts.at[zi, way], ztr.at[zi], ((up_z, down_z)[way], t))

    def zd_copy(zi, way):
        u = unit(zi, dn, row_c)
        return rc(u, u, zds.at[zi, way], zdr.at[zi], ((up_z, down_z)[way], t))

    def along(zi, what):
        @pl.when((zi <= z) & has_up)
        def _():
            what(0)

        @pl.when((zi >= z) & has_down)
        def _():
            what(1)

    def send_t(zi):
        along(zi, lambda way: zt_copy(zi, way).start())

    def send_d(zi):
        along(zi, lambda way: zd_copy(zi, way).start())

    def xy_copy(zi, which, piece, first, count):
        u = unit(zi, t, row_c, first, count)
        sems = (xs, xr) if which == 0 else (ys, yr)
        return rc(u, u, sems[0].at[zi, piece], sems[1].at[zi, piece], (e, (xn, yn)[which]))

    def xy_landed(zi, which, piece, first, count):
        u = unit(zi, (xn, yn)[which], row_c, first, count)
        sems = (xs, xr) if which == 0 else (ys, yr)
        return rc(u, u, sems[0].at[zi, piece], sems[1].at[zi, piece], (e, (xn, yn)[which]))

    def diagonal(which):
        source, first = ((yn, half), (xn, 0))[which]
        u = unit(z, source, row_c, first, half)
        return rc(u, u, fs.at[which], fr.at[which], (e, (xn, yn)[which]))

    def diagonal_landed(which):
        u = unit(z, dn, row_c, (half, 0)[which], half)
        return rc(u, u, fs.at[which], fr.at[which], (e, (xn, yn)[which]))

    def p_copy(zi, ti):
        u = unit(zi, ti, row_c)
        return rc(u, u, ps.at[zi, ti], pr.at[zi, ti], (partner, t))

    def p_landed(zi, ti):
        u = unit(zi, ti, row_o)
        return rc(u, u, ps.at[zi, ti], pr.at[zi, ti], (partner, t))

    h_parts = ((0, hcut), (hcut, slots - hcut))

    def h_copy(zi, which, piece):
        u = hbuf.at[zi, t, pl.ds(*h_parts[piece]), :]
        sems = (hxs, hxr) if which == 0 else (hys, hyr)
        return rc(u, u, sems[0].at[zi, piece], sems[1].at[zi, piece], (e, (xn, yn)[which]))

    def h_landed(zi, which, piece):
        u = hbuf.at[zi, (xn, yn)[which], pl.ds(*h_parts[piece]), :]
        sems = (hxs, hxr) if which == 0 else (hys, hyr)
        return rc(u, u, sems[0].at[zi, piece], sems[1].at[zi, piece], (e, (xn, yn)[which]))

    def g_copy(zi, which):
        u = hbuf.at[zi, (yn, xn)[which], pl.ds(*h_parts[1 - which]), :]
        sems = (gxs, gxr) if which == 0 else (gys, gyr)
        return rc(u, u, sems[0].at[zi], sems[1].at[zi], (e, (xn, yn)[which]))

    def g_landed(zi, which):
        u = hbuf.at[zi, dn, pl.ds(*h_parts[1 - which]), :]
        sems = (gxs, gxr) if which == 0 else (gys, gyr)
        return rc(u, u, sems[0].at[zi], sems[1].at[zi], (e, (xn, yn)[which]))

    def s_copy(d):
        u = shbuf.at[t]
        return rc(u, u, ss.at[d], sr.at[t], (e, (t + d) % tp))

    def s_landed(ti):
        u = shbuf.at[ti]
        return rc(u, u, ss.at[0], sr.at[ti], (e, xn))

    def w_copy(d):
        u = wbuf.at[e]
        return rc(u, u, ws.at[d], wr.at[e], ((e + d) % ep, t))

    def w_landed(ei):
        u = wbuf.at[ei]
        return rc(u, u, ws.at[0], wr.at[ei], (partner, t))

    after, before = jnp.minimum(e + 1, ep - 1), jnp.maximum(e - 1, 0)
    tail, first = pl.ds(tok_a, WINDOW), pl.ds(WINDOW, WINDOW)
    low, high = pl.ds(0, WINDOW), pl.ds(WINDOW + tok_a, WINDOW)
    halo_up = [
        rc(b.at[tail, :], b.at[low, :], ks.at[i], kr.at[i], (after, t))
        for i, b in enumerate((kraw, vbuf))
    ]
    halo_down = [
        rc(b.at[first, :], b.at[high, :], ks.at[2 + i], kr.at[2 + i], (before, t))
        for i, b in enumerate((kraw, vbuf))
    ]

    def pp_copy(zi, n):
        return rc(pbuf.at[zi, n, other], prx.at[zi, n], pps.at[zi, n], ppr.at[zi, n], (partner, t))

    def qq_copy(zi, n):
        return rc(qtx.at[zi, n], qrx.at[z, n], qqs.at[zi, n], qqr.at[z, n], (zi * 2 + c, t))

    def qq_landed(zi, n):
        return rc(qrx.at[zi, n], qrx.at[zi, n], qqs.at[zi, n], qqr.at[zi, n], (partner, t))

    copies[0].wait()
    xy_copy(z, 0, 0, 0, half).start()
    xy_copy(z, 1, 1, half, half).start()
    send_t(z)
    xy_copy(z, 0, 1, half, half).start()
    xy_copy(z, 1, 0, 0, half).start()
    p_copy(z, t).start()
    for d in range(1, ep):
        w_copy(d).start()
    for i in (1, 2, 3):
        copies[i].wait()

    @pl.when(c == 0)
    def _():
        for h in halo_up:
            h.start()

    @pl.when(c == 1)
    def _():
        for h in halo_down:
            h.start()

    @pl.when(e == 0)
    def _():
        kraw[0:WINDOW, :] = jnp.zeros((WINDOW, kv_heads * HEAD_DIM), BF16)
        vbuf[0:WINDOW, :] = jnp.zeros((WINDOW, kv_heads * HEAD_DIM), BF16)

    @pl.when(e == ep - 1)
    def _():
        end = slice(WINDOW + tok_a, 2 * WINDOW + tok_a)
        kraw[end, :] = jnp.zeros((WINDOW, kv_heads * HEAD_DIM), BF16)
        vbuf[end, :] = jnp.zeros((WINDOW, kv_heads * HEAD_DIM), BF16)

    trows = 64
    lane = lax.broadcasted_iota(jnp.int32, (trows, LANES), 1)
    leading = (lane % half_head) < quarter

    def turn(block, head_gain, cos, sin):
        v = block.astype(F32)
        v = v * lax.rsqrt(jnp.mean(v * v, axis=-1, keepdims=True) + epsilon) * head_gain
        swapped = jnp.where(
            leading,
            pltpu.roll(v, HEAD_DIM - quarter, 1),
            pltpu.roll(v, quarter, 1),
        )
        return (v * cos + swapped * sin).astype(BF16)

    heads = kv_heads * group

    def turn_rows(src, dst, count, head_gain, lo, hi, shift):
        def body(i, carry):
            rows = pl.ds(pl.multiple_of(i * trows, trows), trows)
            table = pl.ds(pl.multiple_of(i * trows + shift, trows), trows)
            cos, sin = cos_ref[table, :], sin_ref[table, :]
            for h in range(count):
                cols = slice(h * HEAD_DIM, (h + 1) * HEAD_DIM)
                dst[rows, cols] = turn(src[rows, cols], head_gain, cos, sin)
            return carry

        lax.fori_loop(lo, hi, body, 0)

    nq = tok_a // WINDOW
    per_window = WINDOW // trows
    turn_rows(qraw, qbuf, heads, qgain_ref[...], 0, nq * per_window, WINDOW)

    xy_landed(z, 0, 0, 0, half).wait_recv()
    diagonal(1).start()
    xy_landed(z, 1, 1, half, half).wait_recv()
    diagonal(0).start()

    turn_rows(kraw, kbuf, kv_heads, kgain_ref[...], per_window, (nq + 1) * per_window, 0)

    def take_t(zi):
        u = unit(zi, t, row_c)
        rc(u, u, zts.at[zi, 0], ztr.at[zi], (e, xn)).wait_recv()
        xy_copy(zi, 0, 0, 0, tok).start()
        xy_copy(zi, 1, 0, 0, tok).start()
        send_t(zi)
        p_copy(zi, t).start()

    def wait_d(zi):
        u = unit(zi, dn, row_c)
        rc(u, u, zds.at[zi, 0], zdr.at[zi], (e, xn)).wait_recv()
        p_copy(zi, dn).start()

    def take_xy(zi):
        xy_landed(zi, 0, 0, 0, tok).wait_recv()
        p_copy(zi, xn).start()
        xy_landed(zi, 1, 0, 0, tok).wait_recv()
        p_copy(zi, yn).start()

    take_t(k1)

    @pl.when(is_mid)
    def _():
        take_t(k2)

    span = 3 * WINDOW
    near = lax.broadcasted_iota(jnp.int32, (WINDOW, WINDOW), 1)
    mine = lax.broadcasted_iota(jnp.int32, (WINDOW, WINDOW), 0)
    exp_scale = HEAD_DIM ** (-0.5)

    def attend(qb):
        rows = pl.ds(pl.multiple_of(qb * WINDOW, WINDOW), WINDOW)
        keys = pl.ds(pl.multiple_of(qb * WINDOW, WINDOW), span)
        in_low = (near >= mine) & ((e > 0) | (qb > 0))
        in_high = (near <= mine) & ((e < ep - 1) | (qb < nq - 1))
        sinks = jnp.exp(sink_ref[...])
        for kh in range(kv_heads):
            kcols = slice(kh * HEAD_DIM, (kh + 1) * HEAD_DIM)
            kk = kbuf[keys, kcols]
            vv = vbuf[keys, kcols]
            for g in range(group):
                h = kh * group + g
                qcols = slice(h * HEAD_DIM, (h + 1) * HEAD_DIM)
                scores = lax.dot_general(
                    qbuf[rows, qcols], kk, (((1,), (1,)), ((), ())), preferred_element_type=F32
                )
                raised = jnp.exp(scores * exp_scale)
                parts = [
                    jnp.where(in_low, raised[:, :WINDOW], 0.0),
                    raised[:, WINDOW : 2 * WINDOW],
                    jnp.where(in_high, raised[:, 2 * WINDOW :], 0.0),
                ]
                total = jnp.sum(parts[0] + parts[1] + parts[2], axis=-1, keepdims=True)
                inverse = 1.0 / (total + sinks[:, h : h + 1])
                weights = jnp.concatenate([(p * inverse).astype(BF16) for p in parts], axis=1)
                abuf[rows, qcols] = jnp.dot(
                    weights, vv, preferred_element_type=F32
                ).astype(BF16)

    def att_copy(qb):
        rows = pl.ds(pl.multiple_of(qb * WINDOW, WINDOW), WINDOW)
        return pltpu.make_async_copy(abuf.at[rows, :], att_hbm.at[rows, :], asem.at[qb])

    upper = (
        lax.broadcasted_iota(jnp.int32, (tok, tok), 0)
        < lax.broadcasted_iota(jnp.int32, (tok, tok), 1)
    ).astype(F32)

    def picks(block):
        weight = wbuf[block, pl.ds(e, 1), :][:, :tok]
        named = jnp.where(weight > 0.0, 1.0, 0.0)
        rank = jnp.dot(
            jnp.broadcast_to(named, (16, tok)).astype(BF16),
            upper.astype(BF16),
            preferred_element_type=F32,
        )[0:1, :]
        slot = lax.broadcasted_iota(jnp.int32, (cap, tok), 0).astype(F32)
        hot = jnp.where((slot == rank) & (named > 0.0), 1.0, 0.0)
        return hot, jnp.sum(hot * weight, axis=1, keepdims=True)

    chunk = 32

    def silu_pair(g, u, f):
        g = g * f
        return g / (1.0 + jnp.exp(-g)) * (u * f)

    tile = min(256, units)

    def project_pair(zi):
        def scale(i, carry):
            rows = pl.ds(pl.multiple_of(i * chunk, chunk), chunk)
            squares = jnp.zeros((chunk, 1), F32)
            for ti in range(tp):
                v = xbuf[zi, ti, rows, :].astype(F32)
                squares += jnp.sum(v * v, axis=1, keepdims=True)
                cols = slice(ti * width, (ti + 1) * width)
                scaled[rows, cols] = (v * gain_ref[:, cols]).astype(BF16)
            f = lax.rsqrt(squares / (tp * width) + epsilon)
            factor[rows, :] = jnp.broadcast_to(f, (chunk, LANES))
            return carry

        lax.fori_loop(0, 2 * tok // chunk, scale, 0)

        def columns_of(n, carry):
            cols = pl.ds(pl.multiple_of(n * tile, tile), tile)
            g = jnp.dot(scaled[...], gate[:, cols], preferred_element_type=F32)
            u = jnp.dot(scaled[...], up[:, cols], preferred_element_type=F32)
            hid[:, cols] = silu_pair(g, u, factor[:, 0:1]).astype(BF16)
            return carry

        lax.fori_loop(0, units // tile, columns_of, 0)
        parts = []
        for ci in range(2):
            hot, _ = picks(zi * 2 + ci)
            parts.append(
                jnp.dot(
                    hot.astype(BF16),
                    hid[ci * tok : (ci + 1) * tok, :],
                    preferred_element_type=F32,
                )
            )
        hbuf[zi, t] = jnp.concatenate(parts, axis=0).astype(BF16)

    def shared_up():
        rows = pl.ds(row_c, tok)
        g = jnp.dot(scaled[rows, :], sgate[...], preferred_element_type=F32)
        u = jnp.dot(scaled[rows, :], sup[...], preferred_element_type=F32)
        shbuf[t] = silu_pair(g, u, factor[rows, 0:1]).astype(BF16)

    ctile = min(256, columns)
    chalf = columns // 2
    per_half = chalf // ctile

    def down_pair(zi):
        picked = [picks(zi * 2 + ci) for ci in range(2)]
        slot_weight = jnp.concatenate([p[1] for p in picked], axis=0)

        def columns_of(n, carry):
            cols = pl.ds(pl.multiple_of(n * ctile, ctile), ctile)
            acc = jnp.zeros((slots, ctile), F32)
            for ti in range(tp):
                acc += jnp.dot(
                    hbuf[zi, ti],
                    down[ti * units : (ti + 1) * units, cols],
                    preferred_element_type=F32,
                )
            weighted = acc.astype(BF16).astype(F32) * slot_weight
            part = n // per_half
            put = pl.ds(pl.multiple_of((n % per_half) * ctile, ctile), ctile)
            for ci in range(2):
                spread = lax.dot_general(
                    picked[ci][0].astype(BF16),
                    weighted[ci * cap : (ci + 1) * cap, :].astype(BF16),
                    (((0,), (0,)), ((), ())),
                    preferred_element_type=F32,
                )
                pbuf[zi, part, ci, :, put] = spread.astype(BF16)

            @pl.when(n % per_half == per_half - 1)
            def _():
                pp_copy(zi, part).start()

            return carry

        lax.fori_loop(0, columns // ctile, columns_of, 0)

    qorder = (1, 2, 0, 3)

    def step(s, carry):
        zi = at_step(s)

        @pl.when(s == 1)
        def _():
            @pl.when(is_end)
            def _():
                take_t(k2)

        @pl.when(s == 2)
        def _():
            @pl.when(is_mid)
            def _():
                wait_d(k6)
                send_d(k6)
                send_d(k5)

            @pl.when(e > 0)
            def _():
                for h in halo_up:
                    h.wait_recv()

            @pl.when(e < ep - 1)
            def _():
                for h in halo_down:
                    h.wait_recv()

            turn_rows(kraw, kbuf, kv_heads, kgain_ref[...], 0, per_window, 0)
            last = (nq + 1) * per_window
            turn_rows(kraw, kbuf, kv_heads, kgain_ref[...], last, last + per_window, 0)

        @pl.when((s == 1) | (s == 3))
        def _():
            take_xy(zi)

        @pl.when(s < nz)
        def _():
            qb = qorder[0]
            for i in range(1, nz):
                qb = jnp.where(s == i, qorder[i], qb)
            attend(qb)
            att_copy(qb).start()

            @pl.when(s == 0)
            def _():
                for piece, which in ((1, 0), (0, 1)):
                    xy_landed(z, which, piece, piece * half, half).wait_recv()
                    p_copy(z, (xn, yn)[which]).start()
                for which in range(2):
                    diagonal_landed(which).wait_recv()
                p_copy(z, dn).start()
                send_d(z)

                @pl.when((c == 1) & (e < ep - 1))
                def _():
                    for h in halo_up:
                        h.start()

                @pl.when((c == 0) & (e > 0))
                def _():
                    for h in halo_down:
                        h.start()

                for d in range(1, ep):
                    w_landed((e + d) % ep).wait_recv()
                for cp in copies[4:]:
                    cp.wait()

            @pl.when(s == 1)
            def _():
                wait_d(k3)
                send_d(k3)

                @pl.when(is_mid)
                def _():
                    take_t(k4)
                    wait_d(k5)

            @pl.when(s == 2)
            def _():
                take_xy(zi)

                @pl.when(is_end)
                def _():
                    wait_d(k5)

            @pl.when((s == 3) & is_end)
            def _():
                wait_d(k6)

            for ti in range(tp):
                p_landed(zi, ti).wait_recv()
            project_pair(zi)

            @pl.when((s == 1) & is_end)
            def _():
                take_t(k4)

            h_copy(zi, 0, 0).start()
            h_copy(zi, 1, 1).start()
            h_copy(zi, 0, 1).start()
            h_copy(zi, 1, 0).start()

            @pl.when(s == 0)
            def _():
                shared_up()
                for d in range(1, tp):
                    s_copy(d).start()

        @pl.when((s >= 1) & (s < nz + 1))
        def _():
            zp = at_step(s - 1)
            h_landed(zp, 0, 0).wait_recv()
            g_copy(zp, 1).start()
            h_landed(zp, 1, 1).wait_recv()
            g_copy(zp, 0).start()

        @pl.when((s >= 3) & (s < nz + 3))
        def _():
            zq = at_step(s - 3)
            h_landed(zq, 0, 1).wait_recv()
            h_landed(zq, 1, 0).wait_recv()
            g_landed(zq, 0).wait_recv()
            g_landed(zq, 1).wait_recv()
            down_pair(zq)
            for n in range(2):
                pp_copy(zq, n).wait_recv()
                qtx[zq, n] = (pbuf[zq, n, c].astype(F32) + prx[zq, n].astype(F32)).astype(BF16)

                @pl.when(s > 3)
                def _():
                    qq_copy(zq, n).start()

        return carry

    lax.fori_loop(0, nz + 3, step, 0)

    for d in range(1, tp):
        s_landed((t + d) % tp).wait_recv()
    for n in range(columns // ctile):
        cols = slice(n * ctile, (n + 1) * ctile)
        put = slice(n % per_half * ctile, (n % per_half + 1) * ctile)
        acc = qtx[z, n // per_half, :, put].astype(F32)
        for ti in range(tp):
            acc += jnp.dot(
                shbuf[ti],
                sdown[ti * sunits : (ti + 1) * sunits, cols],
                preferred_element_type=F32,
            )
        base[:, cols] = acc

    outs = []
    for n in range(2):
        for i in range(1, nz):
            qq_landed(order[i], n).wait_recv()
        cols = slice(n * chalf, (n + 1) * chalf)
        acc = base[:, cols]
        for i in range(1, nz):
            acc += qrx[order[i], n].astype(F32)
        obuf[n] = acc.astype(BF16)
        outs.append(pltpu.make_async_copy(obuf.at[n], out_hbm.at[:, cols], osem.at[n]))
        outs[-1].start()

    def drain(zi, carry):
        along(zi, lambda way: zt_copy(zi, way).wait_send())
        along(zi, lambda way: zd_copy(zi, way).wait_send())
        for which in range(2):
            g_copy(zi, which).wait_send()
            for piece in range(2):
                h_copy(zi, which, piece).wait_send()
        for n in range(2):
            pp_copy(zi, n).wait_send()
        for ti in range(tp):
            p_copy(zi, ti).wait_send()

        @pl.when(zi != z)
        def _():
            for which in range(2):
                xy_copy(zi, which, 0, 0, tok).wait_send()
            for n in range(2):
                qq_copy(zi, n).wait_send()

        return carry

    lax.fori_loop(0, nz, drain, 0)
    for which in range(2):
        diagonal(which).wait_send()
        for piece in range(2):
            xy_copy(z, which, piece, piece * half, half).wait_send()
    for d in range(1, tp):
        s_copy(d).wait_send()
    for d in range(1, ep):
        w_copy(d).wait_send()

    @pl.when(e < ep - 1)
    def _():
        for h in halo_up:
            h.wait_send()

    @pl.when(e > 0)
    def _():
        for h in halo_down:
            h.wait_send()

    for qb in range(nq):
        att_copy(qb).wait()
    for cp in outs:
        cp.wait()


def fast_shards(
    query_vectors,
    key_vectors,
    value_vectors,
    query_gain,
    key_gain,
    sink_logits,
    moe_rows,
    norm_gain,
    expert_ids,
    route_weights,
    expert_gate,
    expert_up,
    expert_down,
    shared_gate,
    shared_up,
    shared_down,
):
    ep, tp = lax.axis_size("ep"), lax.axis_size("tp")
    nz = ep // 2
    tok, width = moe_rows.shape
    cap = max(2, 3 * tok * TOP_K // (2 * ep))
    tok_a = query_vectors.shape[0]
    heads = sink_logits.shape[0]
    kv_heads = key_vectors.shape[1] // HEAD_DIM
    group = heads // kv_heads
    units = expert_gate.shape[2]
    columns = expert_down.shape[2]
    sunits = shared_gate.shape[1]
    sizes = (ep, tp, nz, tok, width, cap, tok_a, kv_heads, group, units, columns, sunits)
    full = tp * width
    extent = tok_a + 2 * WINDOW
    padded_tok = (tok + LANES - 1) // LANES * LANES
    nq = tok_a // WINDOW

    vm = pl.BlockSpec(memory_space=pltpu.VMEM)
    hb = pl.BlockSpec(memory_space=pl.ANY)
    dma = pltpu.SemaphoreType.DMA
    slots = 2 * cap
    kvw = kv_heads * HEAD_DIM
    qw = heads * HEAD_DIM
    one, two, four = [dma((nz,))] * 2, [dma((nz, 2))] * 2, [dma((nz, tp))] * 2
    return pl.pallas_call(
        functools.partial(line_kernel, sizes),
        out_shape=(
            jax.ShapeDtypeStruct((tok_a, qw), BF16),
            jax.ShapeDtypeStruct((tok, columns), BF16),
        ),
        in_specs=[hb, hb, hb, vm, vm, vm, hb, vm, vm, vm, hb, hb, hb, hb, hb, hb],
        out_specs=(hb, hb),
        scratch_shapes=[
            pltpu.VMEM((nz, tp, 2 * tok, width), BF16),
            pltpu.VMEM((full, units), BF16),
            pltpu.VMEM((full, units), BF16),
            pltpu.VMEM((tp * units, columns), BF16),
            pltpu.VMEM((full, sunits), BF16),
            pltpu.VMEM((full, sunits), BF16),
            pltpu.VMEM((tp * sunits, columns), BF16),
            pltpu.VMEM((tok_a, qw), BF16),
            pltpu.VMEM((tok_a, qw), BF16),
            pltpu.VMEM((extent, kvw), BF16),
            pltpu.VMEM((extent, kvw), BF16),
            pltpu.VMEM((extent, kvw), BF16),
            pltpu.VMEM((tok_a, qw), BF16),
            pltpu.VMEM((2, tok, columns // 2), BF16),
            pltpu.VMEM((tok, columns), F32),
            pltpu.VMEM((extent, LANES), F32),
            pltpu.VMEM((extent, LANES), F32),
            pltpu.VMEM((ep, ep, padded_tok), F32),
            pltpu.VMEM((2 * tok, full), BF16),
            pltpu.VMEM((2 * tok, LANES), F32),
            pltpu.VMEM((2 * tok, units), BF16),
            pltpu.VMEM((nz, tp, slots, units), BF16),
            pltpu.VMEM((tp, tok, sunits), BF16),
            pltpu.VMEM((nz, 2, 2, tok, columns // 2), BF16),
            pltpu.VMEM((nz, 2, tok, columns // 2), BF16),
            pltpu.VMEM((nz, 2, tok, columns // 2), BF16),
            pltpu.VMEM((nz, 2, tok, columns // 2), BF16),
            dma((10,)),
            dma((nq,)),
            dma((2,)),
            dma((nz, 2)),
            dma((nz,)),
            dma((nz, 2)),
            dma((nz,)),
        ]
        + two * 2
        + [dma((2,))] * 2
        + four
        + two * 2
        + one * 2
        + [dma((tp,))] * 2
        + [dma((ep,))] * 2
        + [dma((4,))] * 2
        + two * 2,
        compiler_params=pltpu.CompilerParams(
            collective_id=0, has_side_effects=True, vmem_limit_bytes=60 * 1024 * 1024
        ),
    )(
        query_vectors,
        key_vectors,
        value_vectors,
        query_gain[None, :],
        key_gain[None, :],
        sink_logits[None, :],
        moe_rows,
        norm_gain[None, :],
        expert_ids,
        route_weights,
        expert_gate,
        expert_up,
        expert_down,
        shared_gate,
        shared_up,
        shared_down,
    )


def choose(*args):
    ep, tp = lax.axis_size("ep"), lax.axis_size("tp")
    query, rows = args[0], args[6]
    kv_heads = args[1].shape[1] // HEAD_DIM
    tok, width = rows.shape
    cap = max(2, 3 * tok * TOP_K // (2 * ep))
    gathered = ep * tok * tp * width * 2
    fits = (
        gathered <= 16 * 1024 * 1024
        and tp == 4
        and ep == 8
        and (2 * cap) % 16 == 0
        and cap % 8 == 0
        and query.shape[0] % GRID_W == 0
        and query.shape[0] == WINDOW * (ep // 2)
        and tok % 32 == 0
        and tok <= 2 * LANES
    )
    return fast_shards(*args) if fits else shards(*args)


def solution(mesh):
    placed = (
        P("ep", "tp"),
        P("ep", "tp"),
        P("ep", "tp"),
        P(),
        P(),
        P("tp"),
        P("ep", "tp"),
        P(),
        P("ep", None),
        P("ep", None),
        P("ep", None, "tp"),
        P("ep", None, "tp"),
        P("ep", None, "tp"),
        P(None, "tp"),
        P(None, "tp"),
        P(None, "tp"),
    )
    return jax.shard_map(
        choose,
        mesh=mesh,
        in_specs=placed,
        out_specs=(P("ep", "tp"), P("ep", "tp")),
        check_vma=False,
    )
```

```python
import functools
import math

import jax
import jax.numpy as jnp
from jax import lax
from jax.experimental import pallas as pl
from jax.experimental.pallas import tpu as pltpu
from jax.sharding import PartitionSpec as P

HEAD_DIM = 128
WINDOW = 128
GRID_W = 64
D = 4096
TOP_K = 4


epsilon = 1e-06
rotary_base = 10000.0


def padded_2(block, sides, width):
    for axis, dim in sides:
        count = lax.axis_size(axis)
        forward = [(i, i + 1) for i in range(count - 1)]
        backward = [(target, source) for source, target in forward]
        low = lax.ppermute(
            lax.slice_in_dim(block, block.shape[dim] - width, None, axis=dim), axis, forward
        )
        high = lax.ppermute(lax.slice_in_dim(block, 0, width, axis=dim), axis, backward)
        block = jnp.concatenate([low, block, high], axis=dim)
    return block


def half_turn(halves):
    leading, trailing = jnp.split(halves, 2, axis=-1)
    return jnp.concatenate([-trailing, leading], axis=-1)


def rotate_heads(vectors, head_gain, positions):
    floats = vectors.astype(jnp.float32)
    normed = (
        floats * lax.rsqrt(jnp.mean(floats * floats, axis=-1, keepdims=True) + epsilon) * head_gain
    )
    quarter = HEAD_DIM // 4
    freq_index = jnp.arange(quarter, dtype=jnp.int32).astype(jnp.float32)
    inverse = rotary_base ** (-4.0 * freq_index / HEAD_DIM)
    grid_row = (positions // GRID_W).astype(jnp.float32)[:, None] * inverse
    grid_col = (positions % GRID_W).astype(jnp.float32)[:, None] * inverse
    angles = jnp.concatenate([grid_row, grid_row, grid_col, grid_col], axis=-1)[:, None, :]
    row_half, col_half = jnp.split(normed, 2, axis=-1)
    turned = jnp.concatenate([half_turn(row_half), half_turn(col_half)], axis=-1)
    return (normed * jnp.cos(angles) + turned * jnp.sin(angles)).astype(jnp.bfloat16)


def attend_window(query_vectors, key_vectors, value_vectors, query_gain, key_gain, sink_logits):
    length = query_vectors.shape[0]
    heads_here = sink_logits.shape[0]
    kv_here = key_vectors.shape[1] // HEAD_DIM
    grouping = heads_here // kv_here
    shard_start = lax.axis_index("ep") * length
    positions = shard_start + jnp.arange(length, dtype=jnp.int32)
    queries = rotate_heads(
        query_vectors.reshape(length, heads_here, HEAD_DIM), query_gain, positions
    )
    turned_keys = rotate_heads(key_vectors.reshape(length, kv_here, HEAD_DIM), key_gain, positions)
    turned_keys = turned_keys.reshape(length, kv_here * HEAD_DIM)
    padded = padded_2(jnp.stack([turned_keys, value_vectors]), (("ep", 1),), WINDOW)
    extent = length + 2 * WINDOW
    near_keys = padded[0].reshape(extent, kv_here, HEAD_DIM)
    near_values = padded[1].reshape(extent, kv_here, HEAD_DIM)
    key_pos = shard_start - WINDOW + jnp.arange(extent, dtype=jnp.int32)
    inside = (
        (jnp.abs(positions[:, None] - key_pos[None, :]) <= WINDOW)
        & (key_pos >= 0)[None, :]
        & (key_pos < lax.axis_size("ep") * length)[None, :]
    )
    scores = jnp.einsum(
        "qhgd,khd->hgqk",
        queries.reshape(length, kv_here, grouping, HEAD_DIM),
        near_keys,
        preferred_element_type=jnp.float32,
    ) * HEAD_DIM ** (-0.5)
    raised = jnp.where(inside, jnp.exp(scores), 0.0)
    denominator = jnp.exp(sink_logits).reshape(kv_here, grouping)[:, :, None] + jnp.sum(
        raised, axis=-1
    )
    weights = (raised / denominator[..., None]).astype(jnp.bfloat16)
    mixed = jnp.einsum("hgqk,khd->qhgd", weights, near_values, preferred_element_type=jnp.float32)
    return mixed.astype(jnp.bfloat16).reshape(length, heads_here * HEAD_DIM)


def project(block_rows, gain_piece, gate_rows, up_rows):
    floats = block_rows.astype(jnp.float32)
    weighted = (floats * gain_piece).astype(jnp.bfloat16)
    gate_sum = jnp.dot(weighted, gate_rows, preferred_element_type=jnp.float32)
    up_sum = jnp.dot(weighted, up_rows, preferred_element_type=jnp.float32)
    return (gate_sum, up_sum, jnp.sum(floats * floats, axis=1))


def activate(gate_sum, up_sum, squares):
    factor = lax.rsqrt(squares / D + epsilon)[:, None]
    return (jax.nn.silu(gate_sum * factor) * (up_sum * factor)).astype(jnp.bfloat16)


def shards(
    query_vectors,
    key_vectors,
    value_vectors,
    query_gain,
    key_gain,
    sink_logits,
    moe_rows,
    norm_gain,
    expert_ids,
    route_weights,
    expert_gate,
    expert_up,
    expert_down,
    shared_gate,
    shared_up,
    shared_down,
):
    attended = attend_window(
        query_vectors, key_vectors, value_vectors, query_gain, key_gain, sink_logits
    )
    ep_size = lax.axis_size("ep")
    tokens_here, width_here = moe_rows.shape
    capacity = max(2, 3 * tokens_here * TOP_K // (2 * ep_size))
    slots_all = ep_size * capacity
    flat_ids = expert_ids.reshape(-1)
    onehot = (flat_ids[:, None] == jnp.arange(ep_size, dtype=jnp.int32)[None, :]).astype(jnp.int32)
    slot_index = jnp.sum((jnp.cumsum(onehot, axis=0) - onehot) * onehot, axis=1)
    target = flat_ids * capacity + slot_index
    matches = target[None, :] == jnp.arange(slots_all, dtype=jnp.int32)[:, None]
    present = jnp.any(matches, axis=1)
    owner_row = jnp.arange(tokens_here * TOP_K, dtype=jnp.int32) // TOP_K
    source_row = jnp.sum(jnp.where(matches, owner_row[None, :], 0), axis=1)
    local_gate = expert_gate[0]
    local_up = expert_up[0]
    local_down = expert_down[0]
    units_here = local_gate.shape[1]
    shared_units = shared_gate.shape[1]
    outgoing = jnp.where(
        present[:, None], jnp.take(moe_rows, source_row, axis=0), jnp.zeros((), jnp.bfloat16)
    )
    arrived = lax.all_to_all(
        outgoing.reshape(ep_size, capacity, width_here),
        "ep",
        split_axis=0,
        concat_axis=0,
        tiled=True,
    )
    arrived = arrived.reshape(slots_all, width_here)
    routed = project(
        lax.all_gather(arrived, "tp", axis=1, tiled=True), norm_gain, local_gate, local_up
    )
    shared = project(
        lax.all_gather(moe_rows, "tp", axis=1, tiled=True), norm_gain, shared_gate, shared_up
    )
    gate_sum, up_sum, squares, shared_gsum, shared_usum, own_squares = tuple(
        (new_term for new_term in routed + shared)
    )
    hidden = activate(gate_sum, up_sum, squares)
    shared_hidden = activate(shared_gsum, shared_usum, own_squares)
    packing = units_here // shared_units
    stacked = jnp.concatenate(
        [hidden, shared_hidden.reshape(tokens_here // packing, units_here)], axis=0
    )
    columns = local_down.shape[1]
    portion = lax.all_gather(stacked, "tp", axis=1, tiled=True)
    shards_in = portion.shape[1] // units_here
    routed = jnp.dot(portion[:slots_all], local_down, preferred_element_type=jnp.float32)
    shared_piece = portion[slots_all:].reshape(
        tokens_here // packing, shards_in, packing, shared_units
    )
    shared_piece = shared_piece.transpose(0, 2, 1, 3).reshape(tokens_here, shards_in * shared_units)
    shared = jnp.dot(shared_piece, shared_down, preferred_element_type=jnp.float32)
    returned = lax.all_to_all(
        routed.astype(jnp.bfloat16).reshape(ep_size, capacity, columns),
        "ep",
        split_axis=0,
        concat_axis=0,
        tiled=True,
    )
    returned = returned.reshape(slots_all, columns)
    picked = jnp.take(returned, target, axis=0).reshape(tokens_here, TOP_K, columns)
    combined = shared + jnp.sum(route_weights[:, :, None] * picked.astype(jnp.float32), axis=1)
    return (attended, combined.astype(jnp.bfloat16))


F32 = jnp.float32
BF16 = jnp.bfloat16
MESH = pl.DeviceIdType.MESH
LANES = 128


def line_kernel(
    sizes,
    q_hbm,
    k_hbm,
    v_hbm,
    qgain_hbm,
    kgain_hbm,
    sink_hbm,
    x_hbm,
    gain_hbm,
    ids_hbm,
    rw_hbm,
    gate_hbm,
    up_hbm,
    down_hbm,
    sgate_hbm,
    sup_hbm,
    sdown_hbm,
    att_hbm,
    out_hbm,
    xbuf,
    gate,
    up,
    down,
    sgate,
    sup,
    sdown,
    qraw,
    qbuf,
    kraw,
    kbuf,
    vbuf,
    abuf,
    obuf,
    base,
    cos_ref,
    sin_ref,
    wbuf,
    qgain_ref,
    kgain_ref,
    sink_ref,
    gain_ref,
    ids_ref,
    rw_ref,
    scaled,
    factor,
    hid,
    hbuf,
    shbuf,
    pbuf,
    prx,
    qtx,
    qrx,
    lsem,
    asem,
    osem,
    zts,
    ztr,
    zds,
    zdr,
    xs,
    xr,
    ys,
    yr,
    fs,
    fr,
    ps,
    pr,
    hxs,
    hxr,
    hys,
    hyr,
    gxs,
    gxr,
    gys,
    gyr,
    ss,
    sr,
    ws,
    wr,
    ks,
    kr,
    pps,
    ppr,
    qqs,
    qqr,
):
    ep, tp, nz, tok, width, cap, tok_a, kv_heads, group, units, columns, sunits = sizes
    e = lax.axis_index("ep")
    t = lax.axis_index("tp")
    z, c = e // 2, e % 2
    other = 1 - c
    partner = z * 2 + other
    tx, ty = t % 2, t // 2
    xn = ty * 2 + (1 - tx)
    yn = (1 - ty) * 2 + tx
    dn = (1 - ty) * 2 + (1 - tx)
    half = tok // 2
    slots = 2 * cap
    hcut = (slots // 2 + 15) // 16 * 16
    row_c = pl.multiple_of(c * tok, 16)
    row_o = pl.multiple_of(other * tok, 16)
    has_up, has_down = z < nz - 1, z > 0
    is_end = (z == 0) | (z == nz - 1)
    is_mid = jnp.logical_not(is_end)

    def by_z(*values):
        r = values[0]
        for i in range(1, nz):
            r = jnp.where(z == i, values[i], r)
        return r

    order = (z, by_z(1, 2, 1, 2), by_z(3, 3, 0, 0), by_z(2, 0, 3, 1))
    o1, o2, o3 = order[1:]
    k1, k2 = by_z(1, 2, 1, 2), by_z(2, 0, 3, 1)
    k3, k4 = by_z(1, 0, 3, 2), by_z(3, 3, 0, 0)
    k5, k6 = by_z(3, 2, 1, 0), by_z(2, 3, 0, 1)

    def table(s, values):
        r = jnp.int32(values[0])
        for i in range(1, len(values)):
            r = jnp.where(s == i, values[i], r)
        return r

    def by_kind(end, mid):
        return jnp.where(is_end, end, mid)

    def rc(src, dst, s_sem, r_sem, dev):
        return pltpu.make_async_remote_copy(
            src_ref=src,
            dst_ref=dst,
            send_sem=s_sem,
            recv_sem=r_sem,
            device_id=dev,
            device_id_type=MESH,
        )

    loads = [
        (x_hbm, xbuf.at[z, t, pl.ds(row_c, tok), :]),
        (q_hbm, qraw),
        (k_hbm, kraw.at[pl.ds(WINDOW, tok_a), :]),
        (v_hbm, vbuf.at[pl.ds(WINDOW, tok_a), :]),
        (gate_hbm.at[0], gate),
        (up_hbm.at[0], up),
        (sgate_hbm, sgate),
        (sup_hbm, sup),
        (down_hbm.at[0], down),
        (sdown_hbm, sdown),
        (ids_hbm, ids_ref),
        (rw_hbm, rw_ref),
        (qgain_hbm, qgain_ref),
        (kgain_hbm, kgain_ref),
        (sink_hbm, sink_ref),
        (gain_hbm, gain_ref),
    ]
    copies = [pltpu.make_async_copy(a, b, lsem.at[i]) for i, (a, b) in enumerate(loads)]

    barrier = pltpu.get_barrier_semaphore()
    for d in range(1, ep):
        pl.semaphore_signal(barrier, inc=1, device_id=((e + d) % ep, t), device_id_type=MESH)
    for d in range(1, tp):
        pl.semaphore_signal(barrier, inc=1, device_id=(e, (t + d) % tp), device_id_type=MESH)
    big = (4, 5, 6, 7, 8, 9)
    for i in (0, 10, 11, 1, 12, 2, 3, 13, 14, 15) + big:
        copies[i].start()

    quarter = HEAD_DIM // 4
    half_head = HEAD_DIM // 2
    extent = tok_a + 2 * WINDOW
    grid_rows = extent // GRID_W
    first_row = (e * tok_a - WINDOW) // GRID_W

    def angles(count, start):
        lane = lax.broadcasted_iota(jnp.int32, (count, LANES), 1)
        place = lax.broadcasted_iota(jnp.int32, (count, LANES), 0)
        exponent = (lane % quarter).astype(F32) * (-4.0 / HEAD_DIM)
        return (place + start).astype(F32) * jnp.exp(exponent * math.log(rotary_base))

    row_pad = (grid_rows + 7) // 8 * 8
    row_angles = angles(row_pad, first_row)
    col_angles = angles(GRID_W, 0)
    row_cos, row_sin = jnp.cos(row_angles), jnp.sin(row_angles)
    col_cos, col_sin = jnp.cos(col_angles), jnp.sin(col_angles)
    lane64 = lax.broadcasted_iota(jnp.int32, (GRID_W, LANES), 1)
    sign = jnp.where(lane64 % half_head < quarter, -1.0, 1.0)
    for g in range(grid_rows):
        rows = slice(g * GRID_W, (g + 1) * GRID_W)
        cos_ref[rows, :] = jnp.where(lane64 < half_head, row_cos[g : g + 1, :], col_cos)
        sin_ref[rows, :] = jnp.where(lane64 < half_head, row_sin[g : g + 1, :], col_sin) * sign

    copies[10].wait()
    copies[11].wait()
    expert = lax.broadcasted_iota(jnp.int32, (ep, tok), 0)
    by_token = jnp.zeros((ep, tok), F32)
    for k in range(TOP_K):
        by_token += jnp.where(ids_ref[k : k + 1, :] == expert, rw_ref[k : k + 1, :], 0.0)
    wbuf[e] = jnp.zeros(wbuf.shape[1:], F32)
    wbuf[e, :, :tok] = by_token

    pl.semaphore_wait(barrier, ep + tp - 2)

    def unit(zi, ti, row, first=0, count=tok):
        return xbuf.at[zi, ti, pl.ds(row + first, count), :]

    up_z = jnp.minimum(z + 1, nz - 1) * 2 + c
    down_z = jnp.maximum(z - 1, 0) * 2 + c

    def zt_copy(zi, way):
        u = unit(zi, t, row_c)
        return rc(u, u, zts.at[zi, way], ztr.at[zi], ((up_z, down_z)[way], t))

    def zd_copy(zi, way):
        u = unit(zi, dn, row_c)
        return rc(u, u, zds.at[zi, way], zdr.at[zi], ((up_z, down_z)[way], t))

    def along(zi, what):
        @pl.when((zi <= z) & has_up)
        def _():
            what(0)

        @pl.when((zi >= z) & has_down)
        def _():
            what(1)

    def send_t(zi):
        along(zi, lambda way: zt_copy(zi, way).start())

    def send_d(zi):
        along(zi, lambda way: zd_copy(zi, way).start())

    def xy_copy(zi, which, piece, first, count):
        u = unit(zi, t, row_c, first, count)
        sems = (xs, xr) if which == 0 else (ys, yr)
        return rc(u, u, sems[0].at[zi, piece], sems[1].at[zi, piece], (e, (xn, yn)[which]))

    def xy_landed(zi, which, piece, first, count):
        u = unit(zi, (xn, yn)[which], row_c, first, count)
        sems = (xs, xr) if which == 0 else (ys, yr)
        return rc(u, u, sems[0].at[zi, piece], sems[1].at[zi, piece], (e, (xn, yn)[which]))

    def diagonal(which):
        source, first = ((yn, half), (xn, 0))[which]
        u = unit(z, source, row_c, first, half)
        return rc(u, u, fs.at[which], fr.at[which], (e, (xn, yn)[which]))

    def diagonal_landed(which):
        u = unit(z, dn, row_c, (half, 0)[which], half)
        return rc(u, u, fs.at[which], fr.at[which], (e, (xn, yn)[which]))

    def p_copy(zi, ti):
        u = unit(zi, ti, row_c)
        return rc(u, u, ps.at[zi, ti], pr.at[zi, ti], (partner, t))

    def p_landed(zi, ti):
        u = unit(zi, ti, row_o)
        return rc(u, u, ps.at[zi, ti], pr.at[zi, ti], (partner, t))

    h_parts = ((0, hcut), (hcut, slots - hcut))

    def h_copy(zi, which, piece):
        u = hbuf.at[zi, t, pl.ds(*h_parts[piece]), :]
        sems = (hxs, hxr) if which == 0 else (hys, hyr)
        return rc(u, u, sems[0].at[zi, piece], sems[1].at[zi, piece], (e, (xn, yn)[which]))

    def h_landed(zi, which, piece):
        u = hbuf.at[zi, (xn, yn)[which], pl.ds(*h_parts[piece]), :]
        sems = (hxs, hxr) if which == 0 else (hys, hyr)
        return rc(u, u, sems[0].at[zi, piece], sems[1].at[zi, piece], (e, (xn, yn)[which]))

    def g_copy(zi, which):
        u = hbuf.at[zi, (yn, xn)[which], pl.ds(*h_parts[1 - which]), :]
        sems = (gxs, gxr) if which == 0 else (gys, gyr)
        return rc(u, u, sems[0].at[zi], sems[1].at[zi], (e, (xn, yn)[which]))

    def g_landed(zi, which):
        u = hbuf.at[zi, dn, pl.ds(*h_parts[1 - which]), :]
        sems = (gxs, gxr) if which == 0 else (gys, gyr)
        return rc(u, u, sems[0].at[zi], sems[1].at[zi], (e, (xn, yn)[which]))

    def s_copy(d):
        u = shbuf.at[t]
        return rc(u, u, ss.at[d], sr.at[t], (e, (t + d) % tp))

    def s_landed(ti):
        u = shbuf.at[ti]
        return rc(u, u, ss.at[0], sr.at[ti], (e, xn))

    def w_copy(d):
        u = wbuf.at[e]
        return rc(u, u, ws.at[d], wr.at[e], ((e + d) % ep, t))

    def w_landed(ei):
        u = wbuf.at[ei]
        return rc(u, u, ws.at[0], wr.at[ei], (partner, t))

    after, before = jnp.minimum(e + 1, ep - 1), jnp.maximum(e - 1, 0)
    tail, first = pl.ds(tok_a, WINDOW), pl.ds(WINDOW, WINDOW)
    low, high = pl.ds(0, WINDOW), pl.ds(WINDOW + tok_a, WINDOW)
    halo_up = [
        rc(b.at[tail, :], b.at[low, :], ks.at[i], kr.at[i], (after, t))
        for i, b in enumerate((kraw, vbuf))
    ]
    halo_down = [
        rc(b.at[first, :], b.at[high, :], ks.at[2 + i], kr.at[2 + i], (before, t))
        for i, b in enumerate((kraw, vbuf))
    ]

    def pp_copy(zi, n):
        return rc(pbuf.at[zi, n, other], prx.at[zi, n], pps.at[zi, n], ppr.at[zi, n], (partner, t))

    def qq_copy(zi, n):
        return rc(qtx.at[zi, n], qrx.at[z, n], qqs.at[zi, n], qqr.at[z, n], (zi * 2 + c, t))

    def qq_landed(zi, n):
        return rc(qrx.at[zi, n], qrx.at[zi, n], qqs.at[zi, n], qqr.at[zi, n], (partner, t))

    copies[0].wait()
    xy_copy(z, 0, 0, 0, half).start()
    xy_copy(z, 1, 1, half, half).start()
    send_t(z)
    xy_copy(z, 0, 1, half, half).start()
    xy_copy(z, 1, 0, 0, half).start()
    p_copy(z, t).start()
    for d in range(1, ep):
        w_copy(d).start()
    for i in (1, 2, 3, 12, 13, 14, 15):
        copies[i].wait()

    @pl.when(c == 0)
    def _():
        for h in halo_up:
            h.start()

    @pl.when(c == 1)
    def _():
        for h in halo_down:
            h.start()

    @pl.when(e == 0)
    def _():
        kraw[0:WINDOW, :] = jnp.zeros((WINDOW, kv_heads * HEAD_DIM), BF16)
        vbuf[0:WINDOW, :] = jnp.zeros((WINDOW, kv_heads * HEAD_DIM), BF16)

    @pl.when(e == ep - 1)
    def _():
        end = slice(WINDOW + tok_a, 2 * WINDOW + tok_a)
        kraw[end, :] = jnp.zeros((WINDOW, kv_heads * HEAD_DIM), BF16)
        vbuf[end, :] = jnp.zeros((WINDOW, kv_heads * HEAD_DIM), BF16)

    trows = WINDOW
    lane = lax.broadcasted_iota(jnp.int32, (trows, LANES), 1)
    leading = (lane % half_head) < quarter

    def turn(block, head_gain, cos, sin):
        v = block.astype(F32)
        v = v * lax.rsqrt(jnp.mean(v * v, axis=-1, keepdims=True) + epsilon) * head_gain
        swapped = jnp.where(
            leading,
            pltpu.roll(v, HEAD_DIM - quarter, 1),
            pltpu.roll(v, quarter, 1),
        )
        return (v * cos + swapped * sin).astype(BF16)

    heads = kv_heads * group

    def turn_rows(src, dst, count, head_gain, lo, hi, shift):
        def body(i, carry):
            rows = pl.ds(pl.multiple_of(i * trows, trows), trows)
            turned = pl.ds(pl.multiple_of(i * trows + shift, trows), trows)
            cos, sin = cos_ref[turned, :], sin_ref[turned, :]
            for h in range(count):
                cols = slice(h * HEAD_DIM, (h + 1) * HEAD_DIM)
                dst[rows, cols] = turn(src[rows, cols], head_gain, cos, sin)
            return carry

        lax.fori_loop(lo, hi, body, 0)

    nq = tok_a // WINDOW
    per_window = WINDOW // trows
    turn_rows(qraw, qbuf, heads, qgain_ref[...], 0, nq * per_window, WINDOW)

    xy_landed(z, 0, 0, 0, half).wait_recv()
    diagonal(1).start()
    xy_landed(z, 1, 1, half, half).wait_recv()
    diagonal(0).start()

    turn_rows(kraw, kbuf, kv_heads, kgain_ref[...], per_window, (nq + 1) * per_window, 0)

    def take_t(zi):
        u = unit(zi, t, row_c)
        rc(u, u, zts.at[zi, 0], ztr.at[zi], (e, xn)).wait_recv()
        xy_copy(zi, 0, 0, 0, tok).start()
        xy_copy(zi, 1, 0, 0, tok).start()
        send_t(zi)
        p_copy(zi, t).start()

    def wait_d(zi):
        u = unit(zi, dn, row_c)
        rc(u, u, zds.at[zi, 0], zdr.at[zi], (e, xn)).wait_recv()
        p_copy(zi, dn).start()

    def take_xy(zi):
        xy_landed(zi, 0, 0, 0, tok).wait_recv()
        p_copy(zi, xn).start()
        xy_landed(zi, 1, 0, 0, tok).wait_recv()
        p_copy(zi, yn).start()

    take_t(k1)

    @pl.when(is_mid)
    def _():
        take_t(k2)

    span = 3 * WINDOW
    near = lax.broadcasted_iota(jnp.int32, (WINDOW, WINDOW), 1)
    mine = lax.broadcasted_iota(jnp.int32, (WINDOW, WINDOW), 0)
    exp_scale = HEAD_DIM ** (-0.5)

    def attend(qb):
        rows = pl.ds(pl.multiple_of(qb * WINDOW, WINDOW), WINDOW)
        keys = pl.ds(pl.multiple_of(qb * WINDOW, WINDOW), span)
        in_low = (near >= mine) & ((e > 0) | (qb > 0))
        in_high = (near <= mine) & ((e < ep - 1) | (qb < nq - 1))
        sinks = jnp.exp(sink_ref[...])
        for kh in range(kv_heads):
            kcols = slice(kh * HEAD_DIM, (kh + 1) * HEAD_DIM)
            kk = kbuf[keys, kcols]
            vv = vbuf[keys, kcols]
            for g in range(group):
                h = kh * group + g
                qcols = slice(h * HEAD_DIM, (h + 1) * HEAD_DIM)
                scores = lax.dot_general(
                    qbuf[rows, qcols], kk, (((1,), (1,)), ((), ())), preferred_element_type=F32
                )
                raised = jnp.exp(scores * exp_scale)
                parts = [
                    jnp.where(in_low, raised[:, :WINDOW], 0.0),
                    raised[:, WINDOW : 2 * WINDOW],
                    jnp.where(in_high, raised[:, 2 * WINDOW :], 0.0),
                ]
                total = jnp.sum(parts[0] + parts[1] + parts[2], axis=-1, keepdims=True)
                inverse = 1.0 / (total + sinks[:, h : h + 1])
                weights = jnp.concatenate([(p * inverse).astype(BF16) for p in parts], axis=1)
                abuf[rows, qcols] = jnp.dot(
                    weights, vv, preferred_element_type=F32
                ).astype(BF16)

    def att_copy(qb):
        rows = pl.ds(pl.multiple_of(qb * WINDOW, WINDOW), WINDOW)
        return pltpu.make_async_copy(abuf.at[rows, :], att_hbm.at[rows, :], asem.at[qb])

    upper = (
        lax.broadcasted_iota(jnp.int32, (tok, tok), 0)
        < lax.broadcasted_iota(jnp.int32, (tok, tok), 1)
    ).astype(F32)

    def picks(block):
        weight = wbuf[block, pl.ds(e, 1), :][:, :tok]
        named = jnp.where(weight > 0.0, 1.0, 0.0)
        rank = jnp.dot(
            jnp.broadcast_to(named, (16, tok)).astype(BF16),
            upper.astype(BF16),
            preferred_element_type=F32,
        )[0:1, :]
        slot = lax.broadcasted_iota(jnp.int32, (cap, tok), 0).astype(F32)
        hot = jnp.where((slot == rank) & (named > 0.0), 1.0, 0.0)
        return hot, jnp.sum(hot * weight, axis=1, keepdims=True)

    chunk = 32

    def silu_pair(g, u, f):
        g = g * f
        return g / (1.0 + jnp.exp(-g)) * (u * f)

    tile = min(256, units)

    def scale_rows(zi, row):
        def scale(i, carry):
            rows = pl.ds(pl.multiple_of(row + i * chunk, chunk), chunk)
            squares = jnp.zeros((chunk, 1), F32)
            for ti in range(tp):
                v = xbuf[zi, ti, rows, :].astype(F32)
                squares += jnp.sum(v * v, axis=1, keepdims=True)
                cols = slice(ti * width, (ti + 1) * width)
                scaled[rows, cols] = (v * gain_ref[:, cols]).astype(BF16)
            f = lax.rsqrt(squares / (tp * width) + epsilon)
            factor[rows, :] = jnp.broadcast_to(f, (chunk, LANES))
            return carry

        lax.fori_loop(0, tok // chunk, scale, 0)

    def project_pair(zi):
        def columns_of(n, carry):
            cols = pl.ds(pl.multiple_of(n * tile, tile), tile)
            g = jnp.dot(scaled[...], gate[:, cols], preferred_element_type=F32)
            u = jnp.dot(scaled[...], up[:, cols], preferred_element_type=F32)
            hid[:, cols] = silu_pair(g, u, factor[:, 0:1]).astype(BF16)
            return carry

        lax.fori_loop(0, units // tile, columns_of, 0)
        parts = []
        for ci in range(2):
            hot, _ = picks(zi * 2 + ci)
            parts.append(
                jnp.dot(
                    hot.astype(BF16),
                    hid[ci * tok : (ci + 1) * tok, :],
                    preferred_element_type=F32,
                )
            )
        hbuf[zi, t] = jnp.concatenate(parts, axis=0).astype(BF16)

    def shared_up():
        rows = pl.ds(row_c, tok)
        g = jnp.dot(scaled[rows, :], sgate[...], preferred_element_type=F32)
        u = jnp.dot(scaled[rows, :], sup[...], preferred_element_type=F32)
        shbuf[t] = silu_pair(g, u, factor[rows, 0:1]).astype(BF16)

    ctile = min(256, columns)
    chalf = columns // 2
    per_half = chalf // ctile

    def combine(zi):
        for n in range(2):
            pp_copy(zi, n).wait_recv()
            qtx[zi, n] = (pbuf[zi, n, c].astype(F32) + prx[zi, n].astype(F32)).astype(BF16)
            qq_copy(zi, n).start()

    def down_pair(zi):
        picked = [picks(zi * 2 + ci) for ci in range(2)]
        slot_weight = jnp.concatenate([p[1] for p in picked], axis=0)

        def columns_of(n, carry):
            cols = pl.ds(pl.multiple_of(n * ctile, ctile), ctile)
            acc = jnp.zeros((slots, ctile), F32)
            for ti in range(tp):
                acc += jnp.dot(
                    hbuf[zi, ti],
                    down[ti * units : (ti + 1) * units, cols],
                    preferred_element_type=F32,
                )
            weighted = acc.astype(BF16).astype(F32) * slot_weight
            part = n // per_half
            put = pl.ds(pl.multiple_of((n % per_half) * ctile, ctile), ctile)
            for ci in range(2):
                spread = lax.dot_general(
                    picked[ci][0].astype(BF16),
                    weighted[ci * cap : (ci + 1) * cap, :].astype(BF16),
                    (((0,), (0,)), ((), ())),
                    preferred_element_type=F32,
                )
                pbuf[zi, part, ci, :, put] = spread.astype(BF16)

            @pl.when(n % per_half == per_half - 1)
            def _():
                pp_copy(zi, part).start()

            @pl.when((n == per_half - 1) & (zi == z))
            def _():
                combine(o1)

            return carry

        lax.fori_loop(0, columns // ctile, columns_of, 0)

    def send_h(zi):
        for which, piece in ((0, 0), (1, 1), (0, 1), (1, 0)):
            h_copy(zi, which, piece).start()

    def forward_h(zi):
        h_landed(zi, 0, 0).wait_recv()
        g_copy(zi, 1).start()
        h_landed(zi, 1, 1).wait_recv()
        g_copy(zi, 0).start()

    def shared_down():
        for d in range(1, tp):
            s_landed((t + d) % tp).wait_recv()
        for n in range(2):
            pp_copy(z, n).wait_recv()
        for n in range(columns // ctile):
            cols = slice(n * ctile, (n + 1) * ctile)
            put = slice(n % per_half * ctile, (n % per_half + 1) * ctile)
            part = n // per_half
            acc = pbuf[z, part, c, :, put].astype(F32) + prx[z, part, :, put].astype(F32)
            for ti in range(tp):
                acc += jnp.dot(
                    shbuf[ti],
                    sdown[ti * sunits : (ti + 1) * sunits, cols],
                    preferred_element_type=F32,
                )
            base[:, cols] = acc

    none = -1
    a_end, a_mid = (1, 2, 0, 3, none, none, none, none), (1, 2, none, 0, none, none, 3, none)
    p_end = (order[0], o1, none, o2, o3, none, none, none)
    p_mid = (order[0], o1, o3, o2, none, none, none, none)
    d_end = (none, none, none, none, o1, order[0], o2, o3)
    d_mid = (none, none, none, o1, order[0], o2, o3, none)

    def step(s, carry):
        qb = by_kind(table(s, a_end), table(s, a_mid))
        zi = by_kind(table(s, p_end), table(s, p_mid))
        zq = by_kind(table(s, d_end), table(s, d_mid))

        @pl.when((s == 1) & is_end)
        def _():
            take_t(k2)

        @pl.when(s == 1)
        def _():
            take_xy(o1)

        @pl.when(s == 2)
        def _():
            @pl.when(is_mid)
            def _():
                wait_d(k6)
                send_d(k6)
                send_d(k5)
                take_xy(o3)

            @pl.when(e > 0)
            def _():
                for h in halo_up:
                    h.wait_recv()

            @pl.when(e < ep - 1)
            def _():
                for h in halo_down:
                    h.wait_recv()

            turn_rows(kraw, kbuf, kv_heads, kgain_ref[...], 0, per_window, 0)
            last = (nq + 1) * per_window
            turn_rows(kraw, kbuf, kv_heads, kgain_ref[...], last, last + per_window, 0)

        @pl.when(qb >= 0)
        def _():
            attend(qb)
            att_copy(qb).start()

        @pl.when(s == 0)
        def _():
            for piece, which in ((1, 0), (0, 1)):
                xy_landed(z, which, piece, piece * half, half).wait_recv()
                p_copy(z, (xn, yn)[which]).start()
            for which in range(2):
                diagonal_landed(which).wait_recv()
            p_copy(z, dn).start()
            send_d(z)

            @pl.when((c == 1) & (e < ep - 1))
            def _():
                for h in halo_up:
                    h.start()

            @pl.when((c == 0) & (e > 0))
            def _():
                for h in halo_down:
                    h.start()

            for d in range(1, ep):
                w_landed((e + d) % ep).wait_recv()
            for i in big:
                copies[i].wait()

        @pl.when(s == 1)
        def _():
            wait_d(k3)
            send_d(k3)

            @pl.when(is_mid)
            def _():
                take_t(k4)
                wait_d(k5)

        @pl.when((s == 3) & is_mid)
        def _():
            forward_h(o1)

        @pl.when(s == 3)
        def _():
            @pl.when(is_end)
            def _():
                wait_d(k5)

            take_xy(o2)

        @pl.when((s == 4) & is_end)
        def _():
            wait_d(k6)
            take_xy(o3)

        @pl.when(zi >= 0)
        def _():
            scale_rows(zi, row_c)
            for ti in range(tp):
                p_landed(zi, ti).wait_recv()
            scale_rows(zi, row_o)
            project_pair(zi)

        @pl.when(s == 0)
        def _():
            send_h(z)
            shared_up()
            for d in range(1, tp):
                s_copy(d).start()

        @pl.when(s == 1)
        def _():
            @pl.when(is_end)
            def _():
                take_t(k4)

            send_h(o1)
            forward_h(z)

        @pl.when(s == 3)
        def _():
            @pl.when(is_end)
            def _():
                forward_h(o1)

            send_h(o2)

        @pl.when(s == 4)
        def _():
            forward_h(o2)
            send_h(o3)

        @pl.when(zq >= 0)
        def _():
            h_landed(zq, 0, 1).wait_recv()
            h_landed(zq, 1, 0).wait_recv()
            g_landed(zq, 0).wait_recv()
            g_landed(zq, 1).wait_recv()
            down_pair(zq)

        @pl.when(zq == o2)
        def _():
            combine(o2)
            forward_h(o3)
            shared_down()

        @pl.when(zq == o3)
        def _():
            combine(o3)

        return carry

    lax.fori_loop(0, nz + 4, step, 0)

    outs = []
    for n in range(2):
        for i in range(1, nz):
            qq_landed(order[i], n).wait_recv()
        cols = slice(n * chalf, (n + 1) * chalf)
        acc = base[:, cols]
        for i in range(1, nz):
            acc += qrx[order[i], n].astype(F32)
        obuf[n] = acc.astype(BF16)
        outs.append(pltpu.make_async_copy(obuf.at[n], out_hbm.at[:, cols], osem.at[n]))
        outs[-1].start()

    def drain(zi, carry):
        along(zi, lambda way: zt_copy(zi, way).wait_send())
        along(zi, lambda way: zd_copy(zi, way).wait_send())
        for which in range(2):
            g_copy(zi, which).wait_send()
            for piece in range(2):
                h_copy(zi, which, piece).wait_send()
        for n in range(2):
            pp_copy(zi, n).wait_send()
        for ti in range(tp):
            p_copy(zi, ti).wait_send()

        @pl.when(zi != z)
        def _():
            for which in range(2):
                xy_copy(zi, which, 0, 0, tok).wait_send()
            for n in range(2):
                qq_copy(zi, n).wait_send()

        return carry

    lax.fori_loop(0, nz, drain, 0)
    for which in range(2):
        diagonal(which).wait_send()
        for piece in range(2):
            xy_copy(z, which, piece, piece * half, half).wait_send()
    for d in range(1, tp):
        s_copy(d).wait_send()
    for d in range(1, ep):
        w_copy(d).wait_send()

    @pl.when(e < ep - 1)
    def _():
        for h in halo_up:
            h.wait_send()

    @pl.when(e > 0)
    def _():
        for h in halo_down:
            h.wait_send()

    for qb in range(nq):
        att_copy(qb).wait()
    for cp in outs:
        cp.wait()


def fast_shards(
    query_vectors,
    key_vectors,
    value_vectors,
    query_gain,
    key_gain,
    sink_logits,
    moe_rows,
    norm_gain,
    expert_ids,
    route_weights,
    expert_gate,
    expert_up,
    expert_down,
    shared_gate,
    shared_up,
    shared_down,
):
    ep, tp = lax.axis_size("ep"), lax.axis_size("tp")
    nz = ep // 2
    tok, width = moe_rows.shape
    cap = max(2, 3 * tok * TOP_K // (2 * ep))
    tok_a = query_vectors.shape[0]
    heads = sink_logits.shape[0]
    kv_heads = key_vectors.shape[1] // HEAD_DIM
    group = heads // kv_heads
    units = expert_gate.shape[2]
    columns = expert_down.shape[2]
    sunits = shared_gate.shape[1]
    sizes = (ep, tp, nz, tok, width, cap, tok_a, kv_heads, group, units, columns, sunits)
    full = tp * width
    extent = tok_a + 2 * WINDOW
    padded_tok = (tok + LANES - 1) // LANES * LANES
    nq = tok_a // WINDOW

    hb = pl.BlockSpec(memory_space=pl.ANY)
    dma = pltpu.SemaphoreType.DMA
    slots = 2 * cap
    kvw = kv_heads * HEAD_DIM
    qw = heads * HEAD_DIM
    one, two, four = [dma((nz,))] * 2, [dma((nz, 2))] * 2, [dma((nz, tp))] * 2
    return pl.pallas_call(
        functools.partial(line_kernel, sizes),
        out_shape=(
            jax.ShapeDtypeStruct((tok_a, qw), BF16),
            jax.ShapeDtypeStruct((tok, columns), BF16),
        ),
        in_specs=[hb] * 16,
        out_specs=(hb, hb),
        scratch_shapes=[
            pltpu.VMEM((nz, tp, 2 * tok, width), BF16),
            pltpu.VMEM((full, units), BF16),
            pltpu.VMEM((full, units), BF16),
            pltpu.VMEM((tp * units, columns), BF16),
            pltpu.VMEM((full, sunits), BF16),
            pltpu.VMEM((full, sunits), BF16),
            pltpu.VMEM((tp * sunits, columns), BF16),
            pltpu.VMEM((tok_a, qw), BF16),
            pltpu.VMEM((tok_a, qw), BF16),
            pltpu.VMEM((extent, kvw), BF16),
            pltpu.VMEM((extent, kvw), BF16),
            pltpu.VMEM((extent, kvw), BF16),
            pltpu.VMEM((tok_a, qw), BF16),
            pltpu.VMEM((2, tok, columns // 2), BF16),
            pltpu.VMEM((tok, columns), F32),
            pltpu.VMEM((extent, LANES), F32),
            pltpu.VMEM((extent, LANES), F32),
            pltpu.VMEM((ep, ep, padded_tok), F32),
            pltpu.VMEM((1, HEAD_DIM), F32),
            pltpu.VMEM((1, HEAD_DIM), F32),
            pltpu.VMEM((1, heads), F32),
            pltpu.VMEM((1, full), F32),
            pltpu.VMEM((TOP_K, tok), jnp.int32),
            pltpu.VMEM((TOP_K, tok), F32),
            pltpu.VMEM((2 * tok, full), BF16),
            pltpu.VMEM((2 * tok, LANES), F32),
            pltpu.VMEM((2 * tok, units), BF16),
            pltpu.VMEM((nz, tp, slots, units), BF16),
            pltpu.VMEM((tp, tok, sunits), BF16),
            pltpu.VMEM((nz, 2, 2, tok, columns // 2), BF16),
            pltpu.VMEM((nz, 2, tok, columns // 2), BF16),
            pltpu.VMEM((nz, 2, tok, columns // 2), BF16),
            pltpu.VMEM((nz, 2, tok, columns // 2), BF16),
            dma((16,)),
            dma((nq,)),
            dma((2,)),
            dma((nz, 2)),
            dma((nz,)),
            dma((nz, 2)),
            dma((nz,)),
        ]
        + two * 2
        + [dma((2,))] * 2
        + four
        + two * 2
        + one * 2
        + [dma((tp,))] * 2
        + [dma((ep,))] * 2
        + [dma((4,))] * 2
        + two * 2,
        compiler_params=pltpu.CompilerParams(
            collective_id=0, has_side_effects=True, vmem_limit_bytes=50 * 1024 * 1024
        ),
    )(
        *(
            pltpu.with_memory_space_constraint(x, pltpu.HBM)
            for x in (
                query_vectors,
                key_vectors,
                value_vectors,
                query_gain[None, :],
                key_gain[None, :],
                sink_logits[None, :],
                moe_rows,
                norm_gain[None, :],
                expert_ids.T,
                route_weights.T,
                expert_gate,
                expert_up,
                expert_down,
                shared_gate,
                shared_up,
                shared_down,
            )
        )
    )


def choose(*args):
    ep, tp = lax.axis_size("ep"), lax.axis_size("tp")
    query, rows = args[0], args[6]
    kv_heads = args[1].shape[1] // HEAD_DIM
    tok, width = rows.shape
    cap = max(2, 3 * tok * TOP_K // (2 * ep))
    gathered = ep * tok * tp * width * 2
    fits = (
        gathered <= 16 * 1024 * 1024
        and tp == 4
        and ep == 8
        and (2 * cap) % 16 == 0
        and cap % 8 == 0
        and query.shape[0] % GRID_W == 0
        and query.shape[0] == WINDOW * (ep // 2)
        and tok % 32 == 0
        and tok <= 2 * LANES
    )
    return fast_shards(*args) if fits else shards(*args)


def solution(mesh):
    placed = (
        P("ep", "tp"),
        P("ep", "tp"),
        P("ep", "tp"),
        P(),
        P(),
        P("tp"),
        P("ep", "tp"),
        P(),
        P("ep", None),
        P("ep", None),
        P("ep", None, "tp"),
        P("ep", None, "tp"),
        P("ep", None, "tp"),
        P(None, "tp"),
        P(None, "tp"),
        P(None, "tp"),
    )
    return jax.shard_map(
        choose,
        mesh=mesh,
        in_specs=placed,
        out_specs=(P("ep", "tp"), P("ep", "tp")),
        check_vma=False,
    )
```

```python
import functools
import math

import jax
import jax.numpy as jnp
from jax import lax
from jax.experimental import pallas as pl
from jax.experimental.pallas import tpu as pltpu
from jax.sharding import PartitionSpec as P

HEAD_DIM = 128
WINDOW = 128
GRID_W = 64
D = 4096
TOP_K = 4


epsilon = 1e-06
rotary_base = 10000.0


def padded_2(block, sides, width):
    for axis, dim in sides:
        count = lax.axis_size(axis)
        forward = [(i, i + 1) for i in range(count - 1)]
        backward = [(target, source) for source, target in forward]
        low = lax.ppermute(
            lax.slice_in_dim(block, block.shape[dim] - width, None, axis=dim), axis, forward
        )
        high = lax.ppermute(lax.slice_in_dim(block, 0, width, axis=dim), axis, backward)
        block = jnp.concatenate([low, block, high], axis=dim)
    return block


def half_turn(halves):
    leading, trailing = jnp.split(halves, 2, axis=-1)
    return jnp.concatenate([-trailing, leading], axis=-1)


def rotate_heads(vectors, head_gain, positions):
    floats = vectors.astype(jnp.float32)
    normed = (
        floats * lax.rsqrt(jnp.mean(floats * floats, axis=-1, keepdims=True) + epsilon) * head_gain
    )
    quarter = HEAD_DIM // 4
    freq_index = jnp.arange(quarter, dtype=jnp.int32).astype(jnp.float32)
    inverse = rotary_base ** (-4.0 * freq_index / HEAD_DIM)
    grid_row = (positions // GRID_W).astype(jnp.float32)[:, None] * inverse
    grid_col = (positions % GRID_W).astype(jnp.float32)[:, None] * inverse
    angles = jnp.concatenate([grid_row, grid_row, grid_col, grid_col], axis=-1)[:, None, :]
    row_half, col_half = jnp.split(normed, 2, axis=-1)
    turned = jnp.concatenate([half_turn(row_half), half_turn(col_half)], axis=-1)
    return (normed * jnp.cos(angles) + turned * jnp.sin(angles)).astype(jnp.bfloat16)


def attend_window(query_vectors, key_vectors, value_vectors, query_gain, key_gain, sink_logits):
    length = query_vectors.shape[0]
    heads_here = sink_logits.shape[0]
    kv_here = key_vectors.shape[1] // HEAD_DIM
    grouping = heads_here // kv_here
    shard_start = lax.axis_index("ep") * length
    positions = shard_start + jnp.arange(length, dtype=jnp.int32)
    queries = rotate_heads(
        query_vectors.reshape(length, heads_here, HEAD_DIM), query_gain, positions
    )
    turned_keys = rotate_heads(key_vectors.reshape(length, kv_here, HEAD_DIM), key_gain, positions)
    turned_keys = turned_keys.reshape(length, kv_here * HEAD_DIM)
    padded = padded_2(jnp.stack([turned_keys, value_vectors]), (("ep", 1),), WINDOW)
    extent = length + 2 * WINDOW
    near_keys = padded[0].reshape(extent, kv_here, HEAD_DIM)
    near_values = padded[1].reshape(extent, kv_here, HEAD_DIM)
    key_pos = shard_start - WINDOW + jnp.arange(extent, dtype=jnp.int32)
    inside = (
        (jnp.abs(positions[:, None] - key_pos[None, :]) <= WINDOW)
        & (key_pos >= 0)[None, :]
        & (key_pos < lax.axis_size("ep") * length)[None, :]
    )
    scores = jnp.einsum(
        "qhgd,khd->hgqk",
        queries.reshape(length, kv_here, grouping, HEAD_DIM),
        near_keys,
        preferred_element_type=jnp.float32,
    ) * HEAD_DIM ** (-0.5)
    raised = jnp.where(inside, jnp.exp(scores), 0.0)
    denominator = jnp.exp(sink_logits).reshape(kv_here, grouping)[:, :, None] + jnp.sum(
        raised, axis=-1
    )
    weights = (raised / denominator[..., None]).astype(jnp.bfloat16)
    mixed = jnp.einsum("hgqk,khd->qhgd", weights, near_values, preferred_element_type=jnp.float32)
    return mixed.astype(jnp.bfloat16).reshape(length, heads_here * HEAD_DIM)


def project(block_rows, gain_piece, gate_rows, up_rows):
    floats = block_rows.astype(jnp.float32)
    weighted = (floats * gain_piece).astype(jnp.bfloat16)
    gate_sum = jnp.dot(weighted, gate_rows, preferred_element_type=jnp.float32)
    up_sum = jnp.dot(weighted, up_rows, preferred_element_type=jnp.float32)
    return (gate_sum, up_sum, jnp.sum(floats * floats, axis=1))


def activate(gate_sum, up_sum, squares):
    factor = lax.rsqrt(squares / D + epsilon)[:, None]
    return (jax.nn.silu(gate_sum * factor) * (up_sum * factor)).astype(jnp.bfloat16)


def shards(
    query_vectors,
    key_vectors,
    value_vectors,
    query_gain,
    key_gain,
    sink_logits,
    moe_rows,
    norm_gain,
    expert_ids,
    route_weights,
    expert_gate,
    expert_up,
    expert_down,
    shared_gate,
    shared_up,
    shared_down,
):
    attended = attend_window(
        query_vectors, key_vectors, value_vectors, query_gain, key_gain, sink_logits
    )
    ep_size = lax.axis_size("ep")
    tokens_here, width_here = moe_rows.shape
    capacity = max(2, 3 * tokens_here * TOP_K // (2 * ep_size))
    slots_all = ep_size * capacity
    flat_ids = expert_ids.reshape(-1)
    onehot = (flat_ids[:, None] == jnp.arange(ep_size, dtype=jnp.int32)[None, :]).astype(jnp.int32)
    slot_index = jnp.sum((jnp.cumsum(onehot, axis=0) - onehot) * onehot, axis=1)
    target = flat_ids * capacity + slot_index
    matches = target[None, :] == jnp.arange(slots_all, dtype=jnp.int32)[:, None]
    present = jnp.any(matches, axis=1)
    owner_row = jnp.arange(tokens_here * TOP_K, dtype=jnp.int32) // TOP_K
    source_row = jnp.sum(jnp.where(matches, owner_row[None, :], 0), axis=1)
    local_gate = expert_gate[0]
    local_up = expert_up[0]
    local_down = expert_down[0]
    units_here = local_gate.shape[1]
    shared_units = shared_gate.shape[1]
    outgoing = jnp.where(
        present[:, None], jnp.take(moe_rows, source_row, axis=0), jnp.zeros((), jnp.bfloat16)
    )
    arrived = lax.all_to_all(
        outgoing.reshape(ep_size, capacity, width_here),
        "ep",
        split_axis=0,
        concat_axis=0,
        tiled=True,
    )
    arrived = arrived.reshape(slots_all, width_here)
    routed = project(
        lax.all_gather(arrived, "tp", axis=1, tiled=True), norm_gain, local_gate, local_up
    )
    shared = project(
        lax.all_gather(moe_rows, "tp", axis=1, tiled=True), norm_gain, shared_gate, shared_up
    )
    gate_sum, up_sum, squares, shared_gsum, shared_usum, own_squares = tuple(
        (new_term for new_term in routed + shared)
    )
    hidden = activate(gate_sum, up_sum, squares)
    shared_hidden = activate(shared_gsum, shared_usum, own_squares)
    packing = units_here // shared_units
    stacked = jnp.concatenate(
        [hidden, shared_hidden.reshape(tokens_here // packing, units_here)], axis=0
    )
    columns = local_down.shape[1]
    portion = lax.all_gather(stacked, "tp", axis=1, tiled=True)
    shards_in = portion.shape[1] // units_here
    routed = jnp.dot(portion[:slots_all], local_down, preferred_element_type=jnp.float32)
    shared_piece = portion[slots_all:].reshape(
        tokens_here // packing, shards_in, packing, shared_units
    )
    shared_piece = shared_piece.transpose(0, 2, 1, 3).reshape(tokens_here, shards_in * shared_units)
    shared = jnp.dot(shared_piece, shared_down, preferred_element_type=jnp.float32)
    returned = lax.all_to_all(
        routed.astype(jnp.bfloat16).reshape(ep_size, capacity, columns),
        "ep",
        split_axis=0,
        concat_axis=0,
        tiled=True,
    )
    returned = returned.reshape(slots_all, columns)
    picked = jnp.take(returned, target, axis=0).reshape(tokens_here, TOP_K, columns)
    combined = shared + jnp.sum(route_weights[:, :, None] * picked.astype(jnp.float32), axis=1)
    return (attended, combined.astype(jnp.bfloat16))


F32 = jnp.float32
BF16 = jnp.bfloat16
MESH = pl.DeviceIdType.MESH
LANES = 128


def line_kernel(
    sizes,
    q_hbm,
    k_hbm,
    v_hbm,
    qgain_hbm,
    kgain_hbm,
    sink_hbm,
    x_hbm,
    gain_hbm,
    ids_hbm,
    rw_hbm,
    gate_hbm,
    up_hbm,
    down_hbm,
    sgate_hbm,
    sup_hbm,
    sdown_hbm,
    att_hbm,
    out_hbm,
    xbuf,
    gate,
    up,
    down,
    sgate,
    sup,
    sdown,
    qraw,
    qbuf,
    kraw,
    kbuf,
    vbuf,
    abuf,
    obuf,
    base,
    cos_ref,
    sin_ref,
    wbuf,
    qgain_ref,
    kgain_ref,
    sink_ref,
    gain_ref,
    ids_ref,
    rw_ref,
    scaled,
    factor,
    hid,
    hbuf,
    shbuf,
    pbuf,
    prx,
    qtx,
    qrx,
    lsem,
    asem,
    osem,
    zts,
    ztr,
    zds,
    zdr,
    zxs,
    zxr,
    xs,
    xr,
    ys,
    yr,
    fs,
    fr,
    ps,
    pr,
    hxs,
    hxr,
    hys,
    hyr,
    gxs,
    gxr,
    gys,
    gyr,
    ss,
    sr,
    ws,
    wr,
    ks,
    kr,
    pps,
    ppr,
    qqs,
    qqr,
):
    ep, tp, nz, tok, width, cap, tok_a, kv_heads, group, units, columns, sunits = sizes
    e = lax.axis_index("ep")
    t = lax.axis_index("tp")
    z, c = e // 2, e % 2
    other = 1 - c
    partner = z * 2 + other
    tx, ty = t % 2, t // 2
    xn = ty * 2 + (1 - tx)
    yn = (1 - ty) * 2 + tx
    dn = (1 - ty) * 2 + (1 - tx)
    half = tok // 2
    slots = 2 * cap
    hcut = (slots // 2 + 15) // 16 * 16
    row_c = pl.multiple_of(c * tok, 16)
    row_o = pl.multiple_of(other * tok, 16)
    has_up, has_down = z < nz - 1, z > 0
    is_end = (z == 0) | (z == nz - 1)
    is_mid = jnp.logical_not(is_end)

    def by_z(*values):
        r = values[0]
        for i in range(1, nz):
            r = jnp.where(z == i, values[i], r)
        return r

    order = (z, by_z(1, 2, 1, 2), by_z(3, 3, 0, 0), by_z(2, 0, 3, 1))
    o1, o2, o3 = order[1:]
    k1, k2 = by_z(1, 2, 1, 2), by_z(2, 0, 3, 1)
    k3, k4 = by_z(1, 0, 3, 2), by_z(3, 3, 0, 0)
    k5, k6 = by_z(3, 2, 1, 0), by_z(2, 3, 0, 1)

    def table(s, values):
        r = jnp.int32(values[0])
        for i in range(1, len(values)):
            r = jnp.where(s == i, values[i], r)
        return r

    def by_kind(end, mid):
        return jnp.where(is_end, end, mid)

    def rc(src, dst, s_sem, r_sem, dev):
        return pltpu.make_async_remote_copy(
            src_ref=src,
            dst_ref=dst,
            send_sem=s_sem,
            recv_sem=r_sem,
            device_id=dev,
            device_id_type=MESH,
        )

    loads = [
        (x_hbm, xbuf.at[z, t, pl.ds(row_c, tok), :]),
        (q_hbm, qraw),
        (k_hbm, kraw.at[pl.ds(WINDOW, tok_a), :]),
        (v_hbm, vbuf.at[pl.ds(WINDOW, tok_a), :]),
        (gate_hbm.at[0], gate),
        (up_hbm.at[0], up),
        (sgate_hbm, sgate),
        (sup_hbm, sup),
        (down_hbm.at[0], down),
        (sdown_hbm, sdown),
        (ids_hbm, ids_ref),
        (rw_hbm, rw_ref),
        (qgain_hbm, qgain_ref),
        (kgain_hbm, kgain_ref),
        (sink_hbm, sink_ref),
        (gain_hbm, gain_ref),
    ]
    copies = [pltpu.make_async_copy(a, b, lsem.at[i]) for i, (a, b) in enumerate(loads)]

    barrier = pltpu.get_barrier_semaphore()
    for d in range(1, ep):
        pl.semaphore_signal(barrier, inc=1, device_id=((e + d) % ep, t), device_id_type=MESH)
    for d in range(1, tp):
        pl.semaphore_signal(barrier, inc=1, device_id=(e, (t + d) % tp), device_id_type=MESH)
    big = (4, 5, 6, 7, 8, 9)
    for i in (0, 10, 11, 1, 12, 2, 3, 13, 14, 15) + big:
        copies[i].start()

    quarter = HEAD_DIM // 4
    half_head = HEAD_DIM // 2
    extent = tok_a + 2 * WINDOW
    grid_rows = extent // GRID_W
    first_row = (e * tok_a - WINDOW) // GRID_W

    def angles(count, start):
        lane = lax.broadcasted_iota(jnp.int32, (count, LANES), 1)
        place = lax.broadcasted_iota(jnp.int32, (count, LANES), 0)
        exponent = (lane % quarter).astype(F32) * (-4.0 / HEAD_DIM)
        return (place + start).astype(F32) * jnp.exp(exponent * math.log(rotary_base))

    row_pad = (grid_rows + 7) // 8 * 8
    row_angles = angles(row_pad, first_row)
    col_angles = angles(GRID_W, 0)
    row_cos, row_sin = jnp.cos(row_angles), jnp.sin(row_angles)
    col_cos, col_sin = jnp.cos(col_angles), jnp.sin(col_angles)
    lane64 = lax.broadcasted_iota(jnp.int32, (GRID_W, LANES), 1)
    sign = jnp.where(lane64 % half_head < quarter, -1.0, 1.0)
    for g in range(grid_rows):
        rows = slice(g * GRID_W, (g + 1) * GRID_W)
        cos_ref[rows, :] = jnp.where(lane64 < half_head, row_cos[g : g + 1, :], col_cos)
        sin_ref[rows, :] = jnp.where(lane64 < half_head, row_sin[g : g + 1, :], col_sin) * sign

    copies[10].wait()
    copies[11].wait()
    expert = lax.broadcasted_iota(jnp.int32, (ep, tok), 0)
    by_token = jnp.zeros((ep, tok), F32)
    for k in range(TOP_K):
        by_token += jnp.where(ids_ref[k : k + 1, :] == expert, rw_ref[k : k + 1, :], 0.0)
    wbuf[e] = jnp.zeros(wbuf.shape[1:], F32)
    wbuf[e, :, :tok] = by_token

    pl.semaphore_wait(barrier, ep + tp - 2)

    def unit(zi, ti, row, first=0, count=tok):
        return xbuf.at[zi, ti, pl.ds(row + first, count), :]

    up_z = jnp.minimum(z + 1, nz - 1) * 2 + c
    down_z = jnp.maximum(z - 1, 0) * 2 + c

    def zt_copy(zi, way):
        u = unit(zi, t, row_c)
        return rc(u, u, zts.at[zi, way], ztr.at[zi], ((up_z, down_z)[way], t))

    def zd_copy(zi, way):
        u = unit(zi, dn, row_c)
        return rc(u, u, zds.at[zi, way], zdr.at[zi], ((up_z, down_z)[way], t))

    def along(zi, what):
        @pl.when((zi <= z) & has_up)
        def _():
            what(0)

        @pl.when((zi >= z) & has_down)
        def _():
            what(1)

    def send_t(zi):
        along(zi, lambda way: zt_copy(zi, way).start())

    def send_d(zi):
        along(zi, lambda way: zd_copy(zi, way).start())

    def zx_copy(which):
        u = unit(z, (xn, yn)[which], row_c)
        dev = jnp.where(z == 0, up_z, down_z)
        return rc(u, u, zxs.at[which], zxr.at[which], (dev, t))

    def zx_landed(which):
        u = unit(o3, (xn, yn)[which], row_c)
        return rc(u, u, zxs.at[which], zxr.at[which], (e, xn))

    def xy_copy(zi, which, piece, first, count):
        u = unit(zi, t, row_c, first, count)
        sems = (xs, xr) if which == 0 else (ys, yr)
        return rc(u, u, sems[0].at[zi, piece], sems[1].at[zi, piece], (e, (xn, yn)[which]))

    def xy_landed(zi, which, piece, first, count):
        u = unit(zi, (xn, yn)[which], row_c, first, count)
        sems = (xs, xr) if which == 0 else (ys, yr)
        return rc(u, u, sems[0].at[zi, piece], sems[1].at[zi, piece], (e, (xn, yn)[which]))

    def diagonal(which):
        source, first = ((yn, half), (xn, 0))[which]
        u = unit(z, source, row_c, first, half)
        return rc(u, u, fs.at[which], fr.at[which], (e, (xn, yn)[which]))

    def diagonal_landed(which):
        u = unit(z, dn, row_c, (half, 0)[which], half)
        return rc(u, u, fs.at[which], fr.at[which], (e, (xn, yn)[which]))

    def p_copy(zi, ti):
        u = unit(zi, ti, row_c)
        return rc(u, u, ps.at[zi, ti], pr.at[zi, ti], (partner, t))

    def p_landed(zi, ti):
        u = unit(zi, ti, row_o)
        return rc(u, u, ps.at[zi, ti], pr.at[zi, ti], (partner, t))

    h_parts = ((0, hcut), (hcut, slots - hcut))

    def h_copy(zi, which, piece):
        u = hbuf.at[zi, t, pl.ds(*h_parts[piece]), :]
        sems = (hxs, hxr) if which == 0 else (hys, hyr)
        return rc(u, u, sems[0].at[zi, piece], sems[1].at[zi, piece], (e, (xn, yn)[which]))

    def h_landed(zi, which, piece):
        u = hbuf.at[zi, (xn, yn)[which], pl.ds(*h_parts[piece]), :]
        sems = (hxs, hxr) if which == 0 else (hys, hyr)
        return rc(u, u, sems[0].at[zi, piece], sems[1].at[zi, piece], (e, (xn, yn)[which]))

    def g_copy(zi, which):
        u = hbuf.at[zi, (yn, xn)[which], pl.ds(*h_parts[1 - which]), :]
        sems = (gxs, gxr) if which == 0 else (gys, gyr)
        return rc(u, u, sems[0].at[zi], sems[1].at[zi], (e, (xn, yn)[which]))

    def g_landed(zi, which):
        u = hbuf.at[zi, dn, pl.ds(*h_parts[1 - which]), :]
        sems = (gxs, gxr) if which == 0 else (gys, gyr)
        return rc(u, u, sems[0].at[zi], sems[1].at[zi], (e, (xn, yn)[which]))

    def s_copy(d):
        u = shbuf.at[t]
        return rc(u, u, ss.at[d], sr.at[t], (e, (t + d) % tp))

    def s_landed(ti):
        u = shbuf.at[ti]
        return rc(u, u, ss.at[0], sr.at[ti], (e, xn))

    def w_copy(d):
        u = wbuf.at[e]
        return rc(u, u, ws.at[d], wr.at[e], ((e + d) % ep, t))

    def w_landed(ei):
        u = wbuf.at[ei]
        return rc(u, u, ws.at[0], wr.at[ei], (partner, t))

    after, before = jnp.minimum(e + 1, ep - 1), jnp.maximum(e - 1, 0)
    tail, first = pl.ds(tok_a, WINDOW), pl.ds(WINDOW, WINDOW)
    low, high = pl.ds(0, WINDOW), pl.ds(WINDOW + tok_a, WINDOW)
    halo_up = [
        rc(b.at[tail, :], b.at[low, :], ks.at[i], kr.at[i], (after, t))
        for i, b in enumerate((kraw, vbuf))
    ]
    halo_down = [
        rc(b.at[first, :], b.at[high, :], ks.at[2 + i], kr.at[2 + i], (before, t))
        for i, b in enumerate((kraw, vbuf))
    ]

    def pp_copy(zi, n):
        return rc(pbuf.at[zi, n, other], prx.at[zi, n], pps.at[zi, n], ppr.at[zi, n], (partner, t))

    def qq_copy(zi, n):
        return rc(qtx.at[zi, n], qrx.at[z, n], qqs.at[zi, n], qqr.at[z, n], (zi * 2 + c, t))

    def qq_landed(zi, n):
        return rc(qrx.at[zi, n], qrx.at[zi, n], qqs.at[zi, n], qqr.at[zi, n], (partner, t))

    copies[0].wait()
    xy_copy(z, 0, 0, 0, half).start()
    xy_copy(z, 1, 1, half, half).start()
    send_t(z)
    xy_copy(z, 0, 1, half, half).start()
    xy_copy(z, 1, 0, 0, half).start()
    p_copy(z, t).start()
    for d in range(1, ep):
        w_copy(d).start()
    for i in (1, 2, 3, 12, 13, 14, 15):
        copies[i].wait()

    @pl.when(c == 0)
    def _():
        for h in halo_up:
            h.start()

    @pl.when(c == 1)
    def _():
        for h in halo_down:
            h.start()

    @pl.when(e == 0)
    def _():
        kraw[0:WINDOW, :] = jnp.zeros((WINDOW, kv_heads * HEAD_DIM), BF16)
        vbuf[0:WINDOW, :] = jnp.zeros((WINDOW, kv_heads * HEAD_DIM), BF16)

    @pl.when(e == ep - 1)
    def _():
        end = slice(WINDOW + tok_a, 2 * WINDOW + tok_a)
        kraw[end, :] = jnp.zeros((WINDOW, kv_heads * HEAD_DIM), BF16)
        vbuf[end, :] = jnp.zeros((WINDOW, kv_heads * HEAD_DIM), BF16)

    trows = WINDOW
    lane = lax.broadcasted_iota(jnp.int32, (trows, LANES), 1)
    leading = (lane % half_head) < quarter

    def turn(block, head_gain, cos, sin):
        v = block.astype(F32)
        v = v * lax.rsqrt(jnp.mean(v * v, axis=-1, keepdims=True) + epsilon) * head_gain
        swapped = jnp.where(
            leading,
            pltpu.roll(v, HEAD_DIM - quarter, 1),
            pltpu.roll(v, quarter, 1),
        )
        return (v * cos + swapped * sin).astype(BF16)

    heads = kv_heads * group

    def turn_rows(src, dst, count, head_gain, lo, hi, shift):
        def body(i, carry):
            rows = pl.ds(pl.multiple_of(i * trows, trows), trows)
            turned = pl.ds(pl.multiple_of(i * trows + shift, trows), trows)
            cos, sin = cos_ref[turned, :], sin_ref[turned, :]
            for h in range(count):
                cols = slice(h * HEAD_DIM, (h + 1) * HEAD_DIM)
                dst[rows, cols] = turn(src[rows, cols], head_gain, cos, sin)
            return carry

        lax.fori_loop(lo, hi, body, 0)

    nq = tok_a // WINDOW
    per_window = WINDOW // trows
    turn_rows(qraw, qbuf, heads, qgain_ref[...], 0, nq * per_window, WINDOW)

    xy_landed(z, 0, 0, 0, half).wait_recv()
    diagonal(1).start()
    xy_landed(z, 1, 1, half, half).wait_recv()
    diagonal(0).start()

    turn_rows(kraw, kbuf, kv_heads, kgain_ref[...], per_window, (nq + 1) * per_window, 0)

    def take_t(zi, spread=True):
        u = unit(zi, t, row_c)
        rc(u, u, zts.at[zi, 0], ztr.at[zi], (e, xn)).wait_recv()
        if spread:
            xy_copy(zi, 0, 0, 0, tok).start()
            xy_copy(zi, 1, 0, 0, tok).start()
        send_t(zi)
        p_copy(zi, t).start()

    def wait_d(zi):
        u = unit(zi, dn, row_c)
        rc(u, u, zds.at[zi, 0], zdr.at[zi], (e, xn)).wait_recv()
        p_copy(zi, dn).start()

    def take_xy(zi):
        xy_landed(zi, 0, 0, 0, tok).wait_recv()
        p_copy(zi, xn).start()
        xy_landed(zi, 1, 0, 0, tok).wait_recv()
        p_copy(zi, yn).start()

    take_t(k1)

    @pl.when(is_mid)
    def _():
        take_t(k2, spread=False)

    span = 3 * WINDOW
    near = lax.broadcasted_iota(jnp.int32, (WINDOW, WINDOW), 1)
    mine = lax.broadcasted_iota(jnp.int32, (WINDOW, WINDOW), 0)
    exp_scale = HEAD_DIM ** (-0.5)

    def attend(qb):
        rows = pl.ds(pl.multiple_of(qb * WINDOW, WINDOW), WINDOW)
        keys = pl.ds(pl.multiple_of(qb * WINDOW, WINDOW), span)
        in_low = (near >= mine) & ((e > 0) | (qb > 0))
        in_high = (near <= mine) & ((e < ep - 1) | (qb < nq - 1))
        sinks = jnp.exp(sink_ref[...])
        for kh in range(kv_heads):
            kcols = slice(kh * HEAD_DIM, (kh + 1) * HEAD_DIM)
            kk = kbuf[keys, kcols]
            vv = vbuf[keys, kcols]
            for g in range(group):
                h = kh * group + g
                qcols = slice(h * HEAD_DIM, (h + 1) * HEAD_DIM)
                scores = lax.dot_general(
                    qbuf[rows, qcols], kk, (((1,), (1,)), ((), ())), preferred_element_type=F32
                )
                raised = jnp.exp(scores * exp_scale)
                parts = [
                    jnp.where(in_low, raised[:, :WINDOW], 0.0),
                    raised[:, WINDOW : 2 * WINDOW],
                    jnp.where(in_high, raised[:, 2 * WINDOW :], 0.0),
                ]
                total = jnp.sum(parts[0] + parts[1] + parts[2], axis=-1, keepdims=True)
                inverse = 1.0 / (total + sinks[:, h : h + 1])
                weights = jnp.concatenate([(p * inverse).astype(BF16) for p in parts], axis=1)
                abuf[rows, qcols] = jnp.dot(
                    weights, vv, preferred_element_type=F32
                ).astype(BF16)

    def att_copy(qb):
        rows = pl.ds(pl.multiple_of(qb * WINDOW, WINDOW), WINDOW)
        return pltpu.make_async_copy(abuf.at[rows, :], att_hbm.at[rows, :], asem.at[qb])

    upper = (
        lax.broadcasted_iota(jnp.int32, (tok, tok), 0)
        < lax.broadcasted_iota(jnp.int32, (tok, tok), 1)
    ).astype(F32)

    def picks(block):
        weight = wbuf[block, pl.ds(e, 1), :][:, :tok]
        named = jnp.where(weight > 0.0, 1.0, 0.0)
        rank = jnp.dot(
            jnp.broadcast_to(named, (16, tok)).astype(BF16),
            upper.astype(BF16),
            preferred_element_type=F32,
        )[0:1, :]
        slot = lax.broadcasted_iota(jnp.int32, (cap, tok), 0).astype(F32)
        hot = jnp.where((slot == rank) & (named > 0.0), 1.0, 0.0)
        return hot, jnp.sum(hot * weight, axis=1, keepdims=True)

    def send_h(zi):
        for which, piece in ((0, 0), (1, 1), (0, 1), (1, 0)):
            h_copy(zi, which, piece).start()

    def forward_h(zi):
        h_landed(zi, 0, 0).wait_recv()
        g_copy(zi, 1).start()
        h_landed(zi, 1, 1).wait_recv()
        g_copy(zi, 0).start()

    chunk = 32

    def silu_pair(g, u, f):
        g = g * f
        return g / (1.0 + jnp.exp(-g)) * (u * f)

    tile = min(256, units)

    def scale_rows(zi, row):
        def scale(i, carry):
            rows = pl.ds(pl.multiple_of(row + i * chunk, chunk), chunk)
            squares = jnp.zeros((chunk, 1), F32)
            for ti in range(tp):
                v = xbuf[zi, ti, rows, :].astype(F32)
                squares += jnp.sum(v * v, axis=1, keepdims=True)
                cols = slice(ti * width, (ti + 1) * width)
                scaled[rows, cols] = (v * gain_ref[:, cols]).astype(BF16)
            f = lax.rsqrt(squares / (tp * width) + epsilon)
            factor[rows, :] = jnp.broadcast_to(f, (chunk, LANES))
            return carry

        lax.fori_loop(0, tok // chunk, scale, 0)

    def project_pair(zi):
        def columns_of(n, carry):
            @pl.when((n == 1) & is_end & (zi == z))
            def _():
                take_t(k2)

            @pl.when((n == 1) & is_end & (zi == o2))
            def _():
                forward_h(o1)

            @pl.when((n == 1) & is_end & (zi == o3))
            def _():
                forward_h(o2)

            @pl.when((n == 1) & is_mid & (zi == o2))
            def _():
                forward_h(o1)
                for which in range(2):
                    zx_landed(which).wait_recv()
                    p_copy(o3, (xn, yn)[which]).start()

            cols = pl.ds(pl.multiple_of(n * tile, tile), tile)
            g = jnp.dot(scaled[...], gate[:, cols], preferred_element_type=F32)
            u = jnp.dot(scaled[...], up[:, cols], preferred_element_type=F32)
            hid[:, cols] = silu_pair(g, u, factor[:, 0:1]).astype(BF16)
            return carry

        lax.fori_loop(0, units // tile, columns_of, 0)
        parts = []
        for ci in range(2):
            hot, _ = picks(zi * 2 + ci)
            parts.append(
                jnp.dot(
                    hot.astype(BF16),
                    hid[ci * tok : (ci + 1) * tok, :],
                    preferred_element_type=F32,
                )
            )
        hbuf[zi, t] = jnp.concatenate(parts, axis=0).astype(BF16)

    def shared_up():
        rows = pl.ds(row_c, tok)
        g = jnp.dot(scaled[rows, :], sgate[...], preferred_element_type=F32)
        u = jnp.dot(scaled[rows, :], sup[...], preferred_element_type=F32)
        shbuf[t] = silu_pair(g, u, factor[rows, 0:1]).astype(BF16)

    ctile = min(256, columns)
    chalf = columns // 2
    per_half = chalf // ctile

    def combine(zi, n):
        pp_copy(zi, n).wait_recv()
        qtx[zi, n] = (pbuf[zi, n, c].astype(F32) + prx[zi, n].astype(F32)).astype(BF16)
        qq_copy(zi, n).start()

    def down_pair(zi):
        picked = [picks(zi * 2 + ci) for ci in range(2)]
        slot_weight = jnp.concatenate([p[1] for p in picked], axis=0)

        def columns_of(n, carry):
            cols = pl.ds(pl.multiple_of(n * ctile, ctile), ctile)
            acc = jnp.zeros((slots, ctile), F32)
            for ti in range(tp):
                acc += jnp.dot(
                    hbuf[zi, ti],
                    down[ti * units : (ti + 1) * units, cols],
                    preferred_element_type=F32,
                )
            weighted = acc.astype(BF16).astype(F32) * slot_weight
            part = n // per_half
            put = pl.ds(pl.multiple_of((n % per_half) * ctile, ctile), ctile)
            for ci in range(2):
                spread = lax.dot_general(
                    picked[ci][0].astype(BF16),
                    weighted[ci * cap : (ci + 1) * cap, :].astype(BF16),
                    (((0,), (0,)), ((), ())),
                    preferred_element_type=F32,
                )
                pbuf[zi, part, ci, :, put] = spread.astype(BF16)

            @pl.when(n % per_half == per_half - 1)
            def _():
                pp_copy(zi, part).start()

            @pl.when((n == per_half - 1) & (zi == by_kind(o2, z)))
            def _():
                combine(o1, 0)
                combine(o1, 1)

            @pl.when((n == per_half) & (zi == o3))
            def _():
                combine(o3, 0)

            return carry

        lax.fori_loop(0, columns // ctile, columns_of, 0)

    def shared_down():
        for d in range(1, tp):
            s_landed((t + d) % tp).wait_recv()
        for n in range(2):
            pp_copy(z, n).wait_recv()
        for n in range(columns // ctile):
            cols = slice(n * ctile, (n + 1) * ctile)
            put = slice(n % per_half * ctile, (n % per_half + 1) * ctile)
            part = n // per_half
            acc = pbuf[z, part, c, :, put].astype(F32) + prx[z, part, :, put].astype(F32)
            for ti in range(tp):
                acc += jnp.dot(
                    shbuf[ti],
                    sdown[ti * sunits : (ti + 1) * sunits, cols],
                    preferred_element_type=F32,
                )
            base[:, cols] = acc

    none = -1
    a_end, a_mid = (1, 2, 0, none, none, none, 3, none), (1, 2, none, none, none, none, 0, 3)
    p_end = (order[0], o1, none, o2, o3, none, none, none)
    p_mid = (order[0], o1, o2, o3, none, none, none, none)
    d_end = (none, none, order[0], none, o1, o2, o3, none)
    d_mid = (none, none, none, o1, order[0], o2, o3, none)

    def step(s, carry):
        qb = by_kind(table(s, a_end), table(s, a_mid))
        zi = by_kind(table(s, p_end), table(s, p_mid))
        zq = by_kind(table(s, d_end), table(s, d_mid))

        @pl.when(s == 1)
        def _():
            @pl.when(is_mid)
            def _():
                take_t(k4)

            take_xy(o1)

        @pl.when((s == 2) & is_mid)
        def _():
            wait_d(k6)
            send_d(k6)
            send_d(k5)
            take_xy(o2)

        @pl.when(s == by_kind(2, 6))
        def _():
            @pl.when(e > 0)
            def _():
                for h in halo_up:
                    h.wait_recv()

            @pl.when(e < ep - 1)
            def _():
                for h in halo_down:
                    h.wait_recv()

            turn_rows(kraw, kbuf, kv_heads, kgain_ref[...], 0, per_window, 0)
            last = (nq + 1) * per_window
            turn_rows(kraw, kbuf, kv_heads, kgain_ref[...], last, last + per_window, 0)

        @pl.when((s == 3) & is_end)
        def _():
            take_xy(o3)

        @pl.when(qb >= 0)
        def _():
            attend(qb)
            att_copy(qb).start()

        @pl.when(s == 0)
        def _():
            for piece, which in ((1, 0), (0, 1)):
                xy_landed(z, which, piece, piece * half, half).wait_recv()
                p_copy(z, (xn, yn)[which]).start()
            for which in range(2):
                diagonal_landed(which).wait_recv()
            p_copy(z, dn).start()
            send_d(z)

            @pl.when((c == 1) & (e < ep - 1))
            def _():
                for h in halo_up:
                    h.start()

            @pl.when((c == 0) & (e > 0))
            def _():
                for h in halo_down:
                    h.start()

            @pl.when(is_end)
            def _():
                zx_copy(0).start()
                zx_copy(1).start()

            for d in range(1, ep):
                w_landed((e + d) % ep).wait_recv()
            for i in big:
                copies[i].wait()

        @pl.when(s == 1)
        def _():
            wait_d(k3)
            send_d(k3)

            @pl.when(is_mid)
            def _():
                wait_d(k5)

        @pl.when((s == 3) & is_end)
        def _():
            wait_d(k5)
            take_xy(o2)

        @pl.when((s == 4) & is_end)
        def _():
            wait_d(k6)

        @pl.when(zi >= 0)
        def _():
            scale_rows(zi, row_c)

            for ti in range(tp):
                p_landed(zi, ti).wait_recv()
            scale_rows(zi, row_o)
            project_pair(zi)

        @pl.when(s == 0)
        def _():
            send_h(z)
            shared_up()
            for d in range(1, tp):
                s_copy(d).start()

        @pl.when(s == 1)
        def _():
            forward_h(z)

            @pl.when(is_end)
            def _():
                take_t(k4)

            send_h(o1)

        @pl.when(s == by_kind(3, 2))
        def _():
            send_h(o2)

        @pl.when((s == 3) & is_mid)
        def _():
            forward_h(o2)

        @pl.when(s == by_kind(4, 3))
        def _():
            send_h(o3)

        @pl.when(zq >= 0)
        def _():
            h_landed(zq, 0, 1).wait_recv()
            h_landed(zq, 1, 0).wait_recv()
            g_landed(zq, 0).wait_recv()
            g_landed(zq, 1).wait_recv()
            down_pair(zq)

        @pl.when(zq == o2)
        def _():
            forward_h(o3)
            combine(o2, 0)
            combine(o2, 1)
            shared_down()

        @pl.when(zq == o3)
        def _():
            combine(o3, 1)

        return carry

    lax.fori_loop(0, nz + 4, step, 0)

    def drain(zi, carry):
        along(zi, lambda way: zt_copy(zi, way).wait_send())
        along(zi, lambda way: zd_copy(zi, way).wait_send())
        for which in range(2):
            g_copy(zi, which).wait_send()
            for piece in range(2):
                h_copy(zi, which, piece).wait_send()
        for n in range(2):
            pp_copy(zi, n).wait_send()
        for ti in range(tp):
            p_copy(zi, ti).wait_send()

        @pl.when((zi != z) & (is_end | (zi != o3)))
        def _():
            for which in range(2):
                xy_copy(zi, which, 0, 0, tok).wait_send()

        return carry

    lax.fori_loop(0, nz, drain, 0)
    for which in range(2):
        diagonal(which).wait_send()
        for piece in range(2):
            xy_copy(z, which, piece, piece * half, half).wait_send()
    for d in range(1, tp):
        s_copy(d).wait_send()
    for d in range(1, ep):
        w_copy(d).wait_send()

    @pl.when(e < ep - 1)
    def _():
        for h in halo_up:
            h.wait_send()

    @pl.when(e > 0)
    def _():
        for h in halo_down:
            h.wait_send()

    @pl.when(is_end)
    def _():
        for which in range(2):
            zx_copy(which).wait_send()

    for qb in range(nq):
        att_copy(qb).wait()

    outs = []
    for n in range(2):
        for i in range(1, nz):
            qq_landed(order[i], n).wait_recv()
        cols = slice(n * chalf, (n + 1) * chalf)
        acc = base[:, cols]
        for i in range(1, nz):
            acc += qrx[order[i], n].astype(F32)
        obuf[n] = acc.astype(BF16)
        outs.append(pltpu.make_async_copy(obuf.at[n], out_hbm.at[:, cols], osem.at[n]))
        outs[-1].start()

    for i in range(1, nz):
        for n in range(2):
            qq_copy(order[i], n).wait_send()
    for cp in outs:
        cp.wait()


def fast_shards(
    query_vectors,
    key_vectors,
    value_vectors,
    query_gain,
    key_gain,
    sink_logits,
    moe_rows,
    norm_gain,
    expert_ids,
    route_weights,
    expert_gate,
    expert_up,
    expert_down,
    shared_gate,
    shared_up,
    shared_down,
):
    ep, tp = lax.axis_size("ep"), lax.axis_size("tp")
    nz = ep // 2
    tok, width = moe_rows.shape
    cap = max(2, 3 * tok * TOP_K // (2 * ep))
    tok_a = query_vectors.shape[0]
    heads = sink_logits.shape[0]
    kv_heads = key_vectors.shape[1] // HEAD_DIM
    group = heads // kv_heads
    units = expert_gate.shape[2]
    columns = expert_down.shape[2]
    sunits = shared_gate.shape[1]
    sizes = (ep, tp, nz, tok, width, cap, tok_a, kv_heads, group, units, columns, sunits)
    full = tp * width
    extent = tok_a + 2 * WINDOW
    padded_tok = (tok + LANES - 1) // LANES * LANES
    nq = tok_a // WINDOW

    hb = pl.BlockSpec(memory_space=pl.ANY)
    dma = pltpu.SemaphoreType.DMA
    slots = 2 * cap
    kvw = kv_heads * HEAD_DIM
    qw = heads * HEAD_DIM
    one, two, four = [dma((nz,))] * 2, [dma((nz, 2))] * 2, [dma((nz, tp))] * 2
    return pl.pallas_call(
        functools.partial(line_kernel, sizes),
        out_shape=(
            jax.ShapeDtypeStruct((tok_a, qw), BF16),
            jax.ShapeDtypeStruct((tok, columns), BF16),
        ),
        in_specs=[hb] * 16,
        out_specs=(hb, hb),
        scratch_shapes=[
            pltpu.VMEM((nz, tp, 2 * tok, width), BF16),
            pltpu.VMEM((full, units), BF16),
            pltpu.VMEM((full, units), BF16),
            pltpu.VMEM((tp * units, columns), BF16),
            pltpu.VMEM((full, sunits), BF16),
            pltpu.VMEM((full, sunits), BF16),
            pltpu.VMEM((tp * sunits, columns), BF16),
            pltpu.VMEM((tok_a, qw), BF16),
            pltpu.VMEM((tok_a, qw), BF16),
            pltpu.VMEM((extent, kvw), BF16),
            pltpu.VMEM((extent, kvw), BF16),
            pltpu.VMEM((extent, kvw), BF16),
            pltpu.VMEM((tok_a, qw), BF16),
            pltpu.VMEM((2, tok, columns // 2), BF16),
            pltpu.VMEM((tok, columns), F32),
            pltpu.VMEM((extent, LANES), F32),
            pltpu.VMEM((extent, LANES), F32),
            pltpu.VMEM((ep, ep, padded_tok), F32),
            pltpu.VMEM((1, HEAD_DIM), F32),
            pltpu.VMEM((1, HEAD_DIM), F32),
            pltpu.VMEM((1, heads), F32),
            pltpu.VMEM((1, full), F32),
            pltpu.VMEM((TOP_K, tok), jnp.int32),
            pltpu.VMEM((TOP_K, tok), F32),
            pltpu.VMEM((2 * tok, full), BF16),
            pltpu.VMEM((2 * tok, LANES), F32),
            pltpu.VMEM((2 * tok, units), BF16),
            pltpu.VMEM((nz, tp, slots, units), BF16),
            pltpu.VMEM((tp, tok, sunits), BF16),
            pltpu.VMEM((nz, 2, 2, tok, columns // 2), BF16),
            pltpu.VMEM((nz, 2, tok, columns // 2), BF16),
            pltpu.VMEM((nz, 2, tok, columns // 2), BF16),
            pltpu.VMEM((nz, 2, tok, columns // 2), BF16),
            dma((16,)),
            dma((nq,)),
            dma((2,)),
            dma((nz, 2)),
            dma((nz,)),
            dma((nz, 2)),
            dma((nz,)),
        ]
        + [dma((2,))] * 2
        + two * 2
        + [dma((2,))] * 2
        + four
        + two * 2
        + one * 2
        + [dma((tp,))] * 2
        + [dma((ep,))] * 2
        + [dma((4,))] * 2
        + two * 2,
        compiler_params=pltpu.CompilerParams(
            collective_id=0, has_side_effects=True, vmem_limit_bytes=50 * 1024 * 1024
        ),
    )(
        *(
            pltpu.with_memory_space_constraint(x, pltpu.HBM)
            for x in (
                query_vectors,
                key_vectors,
                value_vectors,
                query_gain[None, :],
                key_gain[None, :],
                sink_logits[None, :],
                moe_rows,
                norm_gain[None, :],
                expert_ids.T,
                route_weights.T,
                expert_gate,
                expert_up,
                expert_down,
                shared_gate,
                shared_up,
                shared_down,
            )
        )
    )


def choose(*args):
    ep, tp = lax.axis_size("ep"), lax.axis_size("tp")
    query, rows = args[0], args[6]
    kv_heads = args[1].shape[1] // HEAD_DIM
    tok, width = rows.shape
    cap = max(2, 3 * tok * TOP_K // (2 * ep))
    gathered = ep * tok * tp * width * 2
    fits = (
        gathered <= 16 * 1024 * 1024
        and tp == 4
        and ep == 8
        and (2 * cap) % 16 == 0
        and cap % 8 == 0
        and query.shape[0] % GRID_W == 0
        and query.shape[0] == WINDOW * (ep // 2)
        and tok % 32 == 0
        and tok <= 2 * LANES
    )
    return fast_shards(*args) if fits else shards(*args)


def solution(mesh):
    placed = (
        P("ep", "tp"),
        P("ep", "tp"),
        P("ep", "tp"),
        P(),
        P(),
        P("tp"),
        P("ep", "tp"),
        P(),
        P("ep", None),
        P("ep", None),
        P("ep", None, "tp"),
        P("ep", None, "tp"),
        P("ep", None, "tp"),
        P(None, "tp"),
        P(None, "tp"),
        P(None, "tp"),
    )
    return jax.shard_map(
        choose,
        mesh=mesh,
        in_specs=placed,
        out_specs=(P("ep", "tp"), P("ep", "tp")),
        check_vma=False,
    )
```

```python
import functools
import math

import jax
import jax.numpy as jnp
from jax import lax
from jax.experimental import pallas as pl
from jax.experimental.pallas import tpu as pltpu
from jax.sharding import PartitionSpec as P

HEAD_DIM = 128
WINDOW = 128
GRID_W = 64
D = 4096
TOP_K = 4


epsilon = 1e-06
rotary_base = 10000.0


def padded_2(block, sides, width):
    for axis, dim in sides:
        count = lax.axis_size(axis)
        forward = [(i, i + 1) for i in range(count - 1)]
        backward = [(target, source) for source, target in forward]
        low = lax.ppermute(
            lax.slice_in_dim(block, block.shape[dim] - width, None, axis=dim), axis, forward
        )
        high = lax.ppermute(lax.slice_in_dim(block, 0, width, axis=dim), axis, backward)
        block = jnp.concatenate([low, block, high], axis=dim)
    return block


def half_turn(halves):
    leading, trailing = jnp.split(halves, 2, axis=-1)
    return jnp.concatenate([-trailing, leading], axis=-1)


def rotate_heads(vectors, head_gain, positions):
    floats = vectors.astype(jnp.float32)
    normed = (
        floats * lax.rsqrt(jnp.mean(floats * floats, axis=-1, keepdims=True) + epsilon) * head_gain
    )
    quarter = HEAD_DIM // 4
    freq_index = jnp.arange(quarter, dtype=jnp.int32).astype(jnp.float32)
    inverse = rotary_base ** (-4.0 * freq_index / HEAD_DIM)
    grid_row = (positions // GRID_W).astype(jnp.float32)[:, None] * inverse
    grid_col = (positions % GRID_W).astype(jnp.float32)[:, None] * inverse
    angles = jnp.concatenate([grid_row, grid_row, grid_col, grid_col], axis=-1)[:, None, :]
    row_half, col_half = jnp.split(normed, 2, axis=-1)
    turned = jnp.concatenate([half_turn(row_half), half_turn(col_half)], axis=-1)
    return (normed * jnp.cos(angles) + turned * jnp.sin(angles)).astype(jnp.bfloat16)


def attend_window(query_vectors, key_vectors, value_vectors, query_gain, key_gain, sink_logits):
    length = query_vectors.shape[0]
    heads_here = sink_logits.shape[0]
    kv_here = key_vectors.shape[1] // HEAD_DIM
    grouping = heads_here // kv_here
    shard_start = lax.axis_index("ep") * length
    positions = shard_start + jnp.arange(length, dtype=jnp.int32)
    queries = rotate_heads(
        query_vectors.reshape(length, heads_here, HEAD_DIM), query_gain, positions
    )
    turned_keys = rotate_heads(key_vectors.reshape(length, kv_here, HEAD_DIM), key_gain, positions)
    turned_keys = turned_keys.reshape(length, kv_here * HEAD_DIM)
    padded = padded_2(jnp.stack([turned_keys, value_vectors]), (("ep", 1),), WINDOW)
    extent = length + 2 * WINDOW
    near_keys = padded[0].reshape(extent, kv_here, HEAD_DIM)
    near_values = padded[1].reshape(extent, kv_here, HEAD_DIM)
    key_pos = shard_start - WINDOW + jnp.arange(extent, dtype=jnp.int32)
    inside = (
        (jnp.abs(positions[:, None] - key_pos[None, :]) <= WINDOW)
        & (key_pos >= 0)[None, :]
        & (key_pos < lax.axis_size("ep") * length)[None, :]
    )
    scores = jnp.einsum(
        "qhgd,khd->hgqk",
        queries.reshape(length, kv_here, grouping, HEAD_DIM),
        near_keys,
        preferred_element_type=jnp.float32,
    ) * HEAD_DIM ** (-0.5)
    raised = jnp.where(inside, jnp.exp(scores), 0.0)
    denominator = jnp.exp(sink_logits).reshape(kv_here, grouping)[:, :, None] + jnp.sum(
        raised, axis=-1
    )
    weights = (raised / denominator[..., None]).astype(jnp.bfloat16)
    mixed = jnp.einsum("hgqk,khd->qhgd", weights, near_values, preferred_element_type=jnp.float32)
    return mixed.astype(jnp.bfloat16).reshape(length, heads_here * HEAD_DIM)


def project(block_rows, gain_piece, gate_rows, up_rows):
    floats = block_rows.astype(jnp.float32)
    weighted = (floats * gain_piece).astype(jnp.bfloat16)
    gate_sum = jnp.dot(weighted, gate_rows, preferred_element_type=jnp.float32)
    up_sum = jnp.dot(weighted, up_rows, preferred_element_type=jnp.float32)
    return (gate_sum, up_sum, jnp.sum(floats * floats, axis=1))


def activate(gate_sum, up_sum, squares):
    factor = lax.rsqrt(squares / D + epsilon)[:, None]
    return (jax.nn.silu(gate_sum * factor) * (up_sum * factor)).astype(jnp.bfloat16)


def shards(
    query_vectors,
    key_vectors,
    value_vectors,
    query_gain,
    key_gain,
    sink_logits,
    moe_rows,
    norm_gain,
    expert_ids,
    route_weights,
    expert_gate,
    expert_up,
    expert_down,
    shared_gate,
    shared_up,
    shared_down,
):
    attended = attend_window(
        query_vectors, key_vectors, value_vectors, query_gain, key_gain, sink_logits
    )
    ep_size = lax.axis_size("ep")
    tokens_here, width_here = moe_rows.shape
    capacity = max(2, 3 * tokens_here * TOP_K // (2 * ep_size))
    slots_all = ep_size * capacity
    flat_ids = expert_ids.reshape(-1)
    onehot = (flat_ids[:, None] == jnp.arange(ep_size, dtype=jnp.int32)[None, :]).astype(jnp.int32)
    slot_index = jnp.sum((jnp.cumsum(onehot, axis=0) - onehot) * onehot, axis=1)
    target = flat_ids * capacity + slot_index
    matches = target[None, :] == jnp.arange(slots_all, dtype=jnp.int32)[:, None]
    present = jnp.any(matches, axis=1)
    owner_row = jnp.arange(tokens_here * TOP_K, dtype=jnp.int32) // TOP_K
    source_row = jnp.sum(jnp.where(matches, owner_row[None, :], 0), axis=1)
    local_gate = expert_gate[0]
    local_up = expert_up[0]
    local_down = expert_down[0]
    units_here = local_gate.shape[1]
    shared_units = shared_gate.shape[1]
    outgoing = jnp.where(
        present[:, None], jnp.take(moe_rows, source_row, axis=0), jnp.zeros((), jnp.bfloat16)
    )
    arrived = lax.all_to_all(
        outgoing.reshape(ep_size, capacity, width_here),
        "ep",
        split_axis=0,
        concat_axis=0,
        tiled=True,
    )
    arrived = arrived.reshape(slots_all, width_here)
    routed = project(
        lax.all_gather(arrived, "tp", axis=1, tiled=True), norm_gain, local_gate, local_up
    )
    shared = project(
        lax.all_gather(moe_rows, "tp", axis=1, tiled=True), norm_gain, shared_gate, shared_up
    )
    gate_sum, up_sum, squares, shared_gsum, shared_usum, own_squares = tuple(
        (new_term for new_term in routed + shared)
    )
    hidden = activate(gate_sum, up_sum, squares)
    shared_hidden = activate(shared_gsum, shared_usum, own_squares)
    packing = units_here // shared_units
    stacked = jnp.concatenate(
        [hidden, shared_hidden.reshape(tokens_here // packing, units_here)], axis=0
    )
    columns = local_down.shape[1]
    portion = lax.all_gather(stacked, "tp", axis=1, tiled=True)
    shards_in = portion.shape[1] // units_here
    routed = jnp.dot(portion[:slots_all], local_down, preferred_element_type=jnp.float32)
    shared_piece = portion[slots_all:].reshape(
        tokens_here // packing, shards_in, packing, shared_units
    )
    shared_piece = shared_piece.transpose(0, 2, 1, 3).reshape(tokens_here, shards_in * shared_units)
    shared = jnp.dot(shared_piece, shared_down, preferred_element_type=jnp.float32)
    returned = lax.all_to_all(
        routed.astype(jnp.bfloat16).reshape(ep_size, capacity, columns),
        "ep",
        split_axis=0,
        concat_axis=0,
        tiled=True,
    )
    returned = returned.reshape(slots_all, columns)
    picked = jnp.take(returned, target, axis=0).reshape(tokens_here, TOP_K, columns)
    combined = shared + jnp.sum(route_weights[:, :, None] * picked.astype(jnp.float32), axis=1)
    return (attended, combined.astype(jnp.bfloat16))


F32 = jnp.float32
BF16 = jnp.bfloat16
MESH = pl.DeviceIdType.MESH
LANES = 128


def line_kernel(
    sizes,
    q_hbm,
    k_hbm,
    v_hbm,
    qgain_hbm,
    kgain_hbm,
    sink_hbm,
    x_hbm,
    gain_hbm,
    ids_hbm,
    rw_hbm,
    gate_hbm,
    up_hbm,
    down_hbm,
    sgate_hbm,
    sup_hbm,
    sdown_hbm,
    att_hbm,
    out_hbm,
    xbuf,
    gate,
    up,
    down,
    sgate,
    sup,
    sdown,
    qraw,
    qbuf,
    kraw,
    kbuf,
    vbuf,
    abuf,
    obuf,
    base,
    cos_ref,
    sin_ref,
    wbuf,
    qgain_ref,
    kgain_ref,
    sink_ref,
    gain_ref,
    ids_ref,
    rw_ref,
    scaled,
    factor,
    hid,
    hbuf,
    shbuf,
    pbuf,
    prx,
    qtx,
    qrx,
    lsem,
    zts,
    ztr,
    zds,
    zdr,
    zxs,
    zxr,
    xs,
    xr,
    ys,
    yr,
    fs,
    fr,
    ps,
    pr,
    hxs,
    hxr,
    hys,
    hyr,
    gxs,
    gxr,
    gys,
    gyr,
    ss,
    sr,
    ws,
    wr,
    ks,
    kr,
    pps,
    ppr,
    qqs,
    qqr,
):
    ep, tp, nz, tok, width, cap, tok_a, kv_heads, group, units, columns, sunits = sizes
    e = lax.axis_index("ep")
    t = lax.axis_index("tp")
    z, c = e // 2, e % 2
    other = 1 - c
    partner = z * 2 + other
    tx, ty = t % 2, t // 2
    xn = ty * 2 + (1 - tx)
    yn = (1 - ty) * 2 + tx
    dn = (1 - ty) * 2 + (1 - tx)
    half = tok // 2
    slots = 2 * cap
    hcut = (slots // 2 + 15) // 16 * 16
    row_c = pl.multiple_of(c * tok, 16)
    row_o = pl.multiple_of(other * tok, 16)
    has_up, has_down = z < nz - 1, z > 0
    is_end = (z == 0) | (z == nz - 1)
    is_mid = jnp.logical_not(is_end)

    def by_z(*values):
        r = values[0]
        for i in range(1, nz):
            r = jnp.where(z == i, values[i], r)
        return r

    order = (z, by_z(1, 2, 1, 2), by_z(3, 3, 0, 0), by_z(2, 0, 3, 1))
    o1, o2, o3 = order[1:]
    k1, k2 = by_z(1, 2, 1, 2), by_z(2, 0, 3, 1)
    k3, k4 = by_z(1, 0, 3, 2), by_z(3, 3, 0, 0)
    k5, k6 = by_z(3, 2, 1, 0), by_z(2, 3, 0, 1)

    def table(s, values):
        r = jnp.int32(values[0])
        for i in range(1, len(values)):
            r = jnp.where(s == i, values[i], r)
        return r

    def by_kind(end, mid):
        return jnp.where(is_end, end, mid)

    def rc(src, dst, s_sem, r_sem, dev):
        return pltpu.make_async_remote_copy(
            src_ref=src,
            dst_ref=dst,
            send_sem=s_sem,
            recv_sem=r_sem,
            device_id=dev,
            device_id_type=MESH,
        )

    loads = [
        (x_hbm, xbuf.at[z, t, pl.ds(row_c, tok), :]),
        (q_hbm, qraw),
        (k_hbm, kraw.at[pl.ds(WINDOW, tok_a), :]),
        (v_hbm, vbuf.at[pl.ds(WINDOW, tok_a), :]),
        (gate_hbm.at[0], gate),
        (up_hbm.at[0], up),
        (sgate_hbm, sgate),
        (sup_hbm, sup),
        (down_hbm.at[0], down),
        (sdown_hbm, sdown),
        (ids_hbm, ids_ref),
        (rw_hbm, rw_ref),
        (qgain_hbm, qgain_ref),
        (kgain_hbm, kgain_ref),
        (sink_hbm, sink_ref),
        (gain_hbm, gain_ref),
    ]
    copies = [pltpu.make_async_copy(a, b, lsem.at[i]) for i, (a, b) in enumerate(loads)]

    barrier = pltpu.get_barrier_semaphore()
    for d in range(1, ep):
        pl.semaphore_signal(barrier, inc=1, device_id=((e + d) % ep, t), device_id_type=MESH)
    for d in range(1, tp):
        pl.semaphore_signal(barrier, inc=1, device_id=(e, (t + d) % tp), device_id_type=MESH)
    big = (4, 5, 6, 7, 8, 9)
    for i in (0, 10, 11, 1, 12, 2, 3, 13, 14, 15) + big:
        copies[i].start()

    quarter = HEAD_DIM // 4
    half_head = HEAD_DIM // 2
    extent = tok_a + 2 * WINDOW
    grid_rows = extent // GRID_W
    first_row = (e * tok_a - WINDOW) // GRID_W

    def angles(count, start):
        lane = lax.broadcasted_iota(jnp.int32, (count, LANES), 1)
        place = lax.broadcasted_iota(jnp.int32, (count, LANES), 0)
        exponent = (lane % quarter).astype(F32) * (-4.0 / HEAD_DIM)
        return (place + start).astype(F32) * jnp.exp(exponent * math.log(rotary_base))

    row_pad = (grid_rows + 7) // 8 * 8
    row_angles = angles(row_pad, first_row)
    col_angles = angles(GRID_W, 0)
    row_cos, row_sin = jnp.cos(row_angles), jnp.sin(row_angles)
    col_cos, col_sin = jnp.cos(col_angles), jnp.sin(col_angles)
    lane64 = lax.broadcasted_iota(jnp.int32, (GRID_W, LANES), 1)
    sign = jnp.where(lane64 % half_head < quarter, -1.0, 1.0)
    for g in range(grid_rows):
        rows = slice(g * GRID_W, (g + 1) * GRID_W)
        cos_ref[rows, :] = jnp.where(lane64 < half_head, row_cos[g : g + 1, :], col_cos)
        sin_ref[rows, :] = jnp.where(lane64 < half_head, row_sin[g : g + 1, :], col_sin) * sign

    copies[10].wait()
    copies[11].wait()
    expert = lax.broadcasted_iota(jnp.int32, (ep, tok), 0)
    by_token = jnp.zeros((ep, tok), F32)
    for k in range(TOP_K):
        by_token += jnp.where(ids_ref[k : k + 1, :] == expert, rw_ref[k : k + 1, :], 0.0)
    wbuf[e] = jnp.zeros(wbuf.shape[1:], F32)
    wbuf[e, :, :tok] = by_token

    pl.semaphore_wait(barrier, ep + tp - 2)

    def unit(zi, ti, row, first=0, count=tok):
        return xbuf.at[zi, ti, pl.ds(row + first, count), :]

    up_z = jnp.minimum(z + 1, nz - 1) * 2 + c
    down_z = jnp.maximum(z - 1, 0) * 2 + c

    def zt_copy(zi, way):
        u = unit(zi, t, row_c)
        return rc(u, u, zts.at[zi, way], ztr.at[zi], ((up_z, down_z)[way], t))

    def zd_copy(zi, way):
        u = unit(zi, dn, row_c)
        return rc(u, u, zds.at[zi, way], zdr.at[zi], ((up_z, down_z)[way], t))

    def along(zi, what):
        @pl.when((zi <= z) & has_up)
        def _():
            what(0)

        @pl.when((zi >= z) & has_down)
        def _():
            what(1)

    def send_t(zi):
        along(zi, lambda way: zt_copy(zi, way).start())

    def send_d(zi):
        along(zi, lambda way: zd_copy(zi, way).start())

    def zx_copy(which):
        u = unit(z, (xn, yn)[which], row_c)
        dev = jnp.where(z == 0, up_z, down_z)
        return rc(u, u, zxs.at[which], zxr.at[which], (dev, t))

    def zx_landed(which):
        u = unit(o3, (xn, yn)[which], row_c)
        return rc(u, u, zxs.at[which], zxr.at[which], (e, xn))

    def xy_copy(zi, which, piece, first, count):
        u = unit(zi, t, row_c, first, count)
        sems = (xs, xr) if which == 0 else (ys, yr)
        return rc(u, u, sems[0], sems[1].at[zi, piece], (e, (xn, yn)[which]))

    def xy_landed(zi, which, piece, first, count):
        u = unit(zi, (xn, yn)[which], row_c, first, count)
        sems = (xs, xr) if which == 0 else (ys, yr)
        return rc(u, u, sems[0], sems[1].at[zi, piece], (e, (xn, yn)[which]))

    def diagonal(which):
        source, first = ((yn, half), (xn, 0))[which]
        u = unit(z, source, row_c, first, half)
        return rc(u, u, fs.at[which], fr.at[which], (e, (xn, yn)[which]))

    def diagonal_landed(which):
        u = unit(z, dn, row_c, (half, 0)[which], half)
        return rc(u, u, fs.at[which], fr.at[which], (e, (xn, yn)[which]))

    def p_copy(zi, ti):
        u = unit(zi, ti, row_c)
        return rc(u, u, ps, pr.at[zi], (partner, t))

    def p_landed(zi):
        u = xbuf.at[zi, :, pl.ds(row_o, tok), :]
        return rc(u, u, ps, pr.at[zi], (partner, t))

    h_parts = ((0, hcut), (hcut, slots - hcut))

    def h_copy(zi, which, piece):
        u = hbuf.at[zi, t, pl.ds(*h_parts[piece]), :]
        sems = (hxs, hxr) if which == 0 else (hys, hyr)
        return rc(u, u, sems[0], sems[1].at[zi, piece], (e, (xn, yn)[which]))

    def h_landed(zi, which, piece):
        u = hbuf.at[zi, (xn, yn)[which], pl.ds(*h_parts[piece]), :]
        sems = (hxs, hxr) if which == 0 else (hys, hyr)
        return rc(u, u, sems[0], sems[1].at[zi, piece], (e, (xn, yn)[which]))

    def g_copy(zi, which):
        u = hbuf.at[zi, (yn, xn)[which], pl.ds(*h_parts[1 - which]), :]
        sems = (gxs, gxr) if which == 0 else (gys, gyr)
        return rc(u, u, sems[0], sems[1].at[zi], (e, (xn, yn)[which]))

    def g_landed(zi, which):
        u = hbuf.at[zi, dn, pl.ds(*h_parts[1 - which]), :]
        sems = (gxs, gxr) if which == 0 else (gys, gyr)
        return rc(u, u, sems[0], sems[1].at[zi], (e, (xn, yn)[which]))

    def s_copy(d):
        u = shbuf.at[t]
        return rc(u, u, ss, sr, (e, (t + d) % tp))

    def w_copy(d):
        u = wbuf.at[e]
        return rc(u, u, ws, wr, ((e + d) % ep, t))

    def all_s():
        u = shbuf.at[pl.ds(0, tp - 1)]
        return rc(u, u, ss, sr, (e, xn))

    def all_w():
        u = wbuf.at[pl.ds(0, ep - 1)]
        return rc(u, u, ws, wr, (partner, t))

    def all_qq(n):
        u = qrx.at[pl.ds(0, nz - 1), n]
        return rc(u, u, qqs.at[0], qqr.at[n], (partner, t))

    after, before = jnp.minimum(e + 1, ep - 1), jnp.maximum(e - 1, 0)
    tail, first = pl.ds(tok_a, WINDOW), pl.ds(WINDOW, WINDOW)
    low, high = pl.ds(0, WINDOW), pl.ds(WINDOW + tok_a, WINDOW)
    halo_up = [
        rc(b.at[tail, :], b.at[low, :], ks.at[i], kr.at[i], (after, t))
        for i, b in enumerate((kraw, vbuf))
    ]
    halo_down = [
        rc(b.at[first, :], b.at[high, :], ks.at[2 + i], kr.at[2 + i], (before, t))
        for i, b in enumerate((kraw, vbuf))
    ]

    def pp_copy(zi, n):
        return rc(pbuf.at[zi, n, other], prx.at[zi, n], pps, ppr.at[zi, n], (partner, t))

    def qq_copy(zi, n):
        return rc(qtx.at[zi, n], qrx.at[z, n], qqs.at[zi], qqr.at[n], (zi * 2 + c, t))

    copies[0].wait()
    xy_copy(z, 0, 0, 0, half).start()
    xy_copy(z, 1, 1, half, half).start()
    send_t(z)
    xy_copy(z, 0, 1, half, half).start()
    xy_copy(z, 1, 0, 0, half).start()
    p_copy(z, t).start()
    for d in range(1, ep):
        w_copy(d).start()
    for i in (1, 2, 3, 12, 13, 14, 15):
        copies[i].wait()

    @pl.when(c == 0)
    def _():
        for h in halo_up:
            h.start()

    @pl.when(c == 1)
    def _():
        for h in halo_down:
            h.start()

    @pl.when(e == 0)
    def _():
        kraw[0:WINDOW, :] = jnp.zeros((WINDOW, kv_heads * HEAD_DIM), BF16)
        vbuf[0:WINDOW, :] = jnp.zeros((WINDOW, kv_heads * HEAD_DIM), BF16)

    @pl.when(e == ep - 1)
    def _():
        end = slice(WINDOW + tok_a, 2 * WINDOW + tok_a)
        kraw[end, :] = jnp.zeros((WINDOW, kv_heads * HEAD_DIM), BF16)
        vbuf[end, :] = jnp.zeros((WINDOW, kv_heads * HEAD_DIM), BF16)

    trows = WINDOW
    lane = lax.broadcasted_iota(jnp.int32, (trows, LANES), 1)
    leading = (lane % half_head) < quarter

    def turn(block, head_gain, cos, sin):
        v = block.astype(F32)
        v = v * lax.rsqrt(jnp.mean(v * v, axis=-1, keepdims=True) + epsilon) * head_gain
        swapped = jnp.where(
            leading,
            pltpu.roll(v, HEAD_DIM - quarter, 1),
            pltpu.roll(v, quarter, 1),
        )
        return (v * cos + swapped * sin).astype(BF16)

    heads = kv_heads * group

    def turn_rows(src, dst, count, head_gain, lo, hi, shift):
        def body(i, carry):
            rows = pl.ds(pl.multiple_of(i * trows, trows), trows)
            turned = pl.ds(pl.multiple_of(i * trows + shift, trows), trows)
            cos, sin = cos_ref[turned, :], sin_ref[turned, :]
            for h in range(count):
                cols = slice(h * HEAD_DIM, (h + 1) * HEAD_DIM)
                dst[rows, cols] = turn(src[rows, cols], head_gain, cos, sin)
            return carry

        lax.fori_loop(lo, hi, body, 0)

    nq = tok_a // WINDOW
    per_window = WINDOW // trows
    turn_rows(qraw, qbuf, heads, qgain_ref[...], 0, nq * per_window, WINDOW)

    xy_landed(z, 0, 0, 0, half).wait_recv()
    diagonal(1).start()
    xy_landed(z, 1, 1, half, half).wait_recv()
    diagonal(0).start()

    turn_rows(kraw, kbuf, kv_heads, kgain_ref[...], per_window, (nq + 1) * per_window, 0)

    def take_t(zi, spread=True):
        u = unit(zi, t, row_c)
        rc(u, u, zts.at[zi, 0], ztr.at[zi], (e, xn)).wait_recv()
        if spread:
            xy_copy(zi, 0, 0, 0, tok).start()
            xy_copy(zi, 1, 0, 0, tok).start()
        send_t(zi)
        p_copy(zi, t).start()

    def wait_d(zi):
        u = unit(zi, dn, row_c)
        rc(u, u, zds.at[zi, 0], zdr.at[zi], (e, xn)).wait_recv()
        p_copy(zi, dn).start()

    def take_xy(zi):
        xy_landed(zi, 0, 0, 0, tok).wait_recv()
        p_copy(zi, xn).start()
        xy_landed(zi, 1, 0, 0, tok).wait_recv()
        p_copy(zi, yn).start()

    take_t(k1)

    @pl.when(is_mid)
    def _():
        take_t(k2, spread=False)

    span = 3 * WINDOW
    near = lax.broadcasted_iota(jnp.int32, (WINDOW, WINDOW), 1)
    mine = lax.broadcasted_iota(jnp.int32, (WINDOW, WINDOW), 0)
    exp_scale = HEAD_DIM ** (-0.5)

    def attend(qb):
        rows = pl.ds(pl.multiple_of(qb * WINDOW, WINDOW), WINDOW)
        keys = pl.ds(pl.multiple_of(qb * WINDOW, WINDOW), span)
        in_low = (near >= mine) & ((e > 0) | (qb > 0))
        in_high = (near <= mine) & ((e < ep - 1) | (qb < nq - 1))
        sinks = jnp.exp(sink_ref[...])
        for kh in range(kv_heads):
            kcols = slice(kh * HEAD_DIM, (kh + 1) * HEAD_DIM)
            kk = kbuf[keys, kcols]
            vv = vbuf[keys, kcols]
            for g in range(group):
                h = kh * group + g
                qcols = slice(h * HEAD_DIM, (h + 1) * HEAD_DIM)
                scores = lax.dot_general(
                    qbuf[rows, qcols], kk, (((1,), (1,)), ((), ())), preferred_element_type=F32
                )
                raised = jnp.exp(scores * exp_scale)
                parts = [
                    jnp.where(in_low, raised[:, :WINDOW], 0.0),
                    raised[:, WINDOW : 2 * WINDOW],
                    jnp.where(in_high, raised[:, 2 * WINDOW :], 0.0),
                ]
                total = jnp.sum(parts[0] + parts[1] + parts[2], axis=-1, keepdims=True)
                inverse = 1.0 / (total + sinks[:, h : h + 1])
                weights = jnp.concatenate([(p * inverse).astype(BF16) for p in parts], axis=1)
                abuf[rows, qcols] = jnp.dot(
                    weights, vv, preferred_element_type=F32
                ).astype(BF16)

    def att_copy(qb):
        rows = pl.ds(pl.multiple_of(qb * WINDOW, WINDOW), WINDOW)
        return pltpu.make_async_copy(abuf.at[rows, :], att_hbm.at[rows, :], lsem.at[qb])

    upper = (
        lax.broadcasted_iota(jnp.int32, (tok, tok), 0)
        < lax.broadcasted_iota(jnp.int32, (tok, tok), 1)
    ).astype(F32)

    def picks(block):
        weight = wbuf[block, pl.ds(e, 1), :][:, :tok]
        named = jnp.where(weight > 0.0, 1.0, 0.0)
        rank = jnp.dot(
            jnp.broadcast_to(named, (16, tok)).astype(BF16),
            upper.astype(BF16),
            preferred_element_type=F32,
        )[0:1, :]
        slot = lax.broadcasted_iota(jnp.int32, (cap, tok), 0).astype(F32)
        hot = jnp.where((slot == rank) & (named > 0.0), 1.0, 0.0)
        return hot, jnp.sum(hot * weight, axis=1, keepdims=True)

    def send_h(zi):
        for which, piece in ((0, 0), (1, 1), (0, 1), (1, 0)):
            h_copy(zi, which, piece).start()

    def forward_h(zi):
        h_landed(zi, 0, 0).wait_recv()
        g_copy(zi, 1).start()
        h_landed(zi, 1, 1).wait_recv()
        g_copy(zi, 0).start()

    chunk = 32

    def silu_pair(g, u, f):
        g = g * f
        return g / (1.0 + jnp.exp(-g)) * (u * f)

    tile = min(256, units)

    def scale_rows(zi, row):
        def scale(i, carry):
            rows = pl.ds(pl.multiple_of(row + i * chunk, chunk), chunk)
            squares = jnp.zeros((chunk, 1), F32)
            for ti in range(tp):
                v = xbuf[zi, ti, rows, :].astype(F32)
                squares += jnp.sum(v * v, axis=1, keepdims=True)
                cols = slice(ti * width, (ti + 1) * width)
                scaled[rows, cols] = (v * gain_ref[:, cols]).astype(BF16)
            f = lax.rsqrt(squares / (tp * width) + epsilon)
            factor[rows, :] = jnp.broadcast_to(f, (chunk, LANES))
            return carry

        lax.fori_loop(0, tok // chunk, scale, 0)

    def project_pair(zi):
        def columns_of(n, carry):
            @pl.when((n == 1) & is_end & (zi == z))
            def _():
                take_t(k2)

            @pl.when((n == 1) & is_end & (zi == o2))
            def _():
                forward_h(o1)

            @pl.when((n == 1) & is_end & (zi == o3))
            def _():
                forward_h(o2)

            @pl.when((n == 1) & is_mid & (zi == o2))
            def _():
                forward_h(o1)
                for which in range(2):
                    zx_landed(which).wait_recv()
                    p_copy(o3, (xn, yn)[which]).start()

            cols = pl.ds(pl.multiple_of(n * tile, tile), tile)
            g = jnp.dot(scaled[...], gate[:, cols], preferred_element_type=F32)
            u = jnp.dot(scaled[...], up[:, cols], preferred_element_type=F32)
            hid[:, cols] = silu_pair(g, u, factor[:, 0:1]).astype(BF16)
            return carry

        lax.fori_loop(0, units // tile, columns_of, 0)
        parts = []
        for ci in range(2):
            hot, _ = picks(zi * 2 + ci)
            parts.append(
                jnp.dot(
                    hot.astype(BF16),
                    hid[ci * tok : (ci + 1) * tok, :],
                    preferred_element_type=F32,
                )
            )
        hbuf[zi, t] = jnp.concatenate(parts, axis=0).astype(BF16)

    def shared_up():
        rows = pl.ds(row_c, tok)
        g = jnp.dot(scaled[rows, :], sgate[...], preferred_element_type=F32)
        u = jnp.dot(scaled[rows, :], sup[...], preferred_element_type=F32)
        shbuf[t] = silu_pair(g, u, factor[rows, 0:1]).astype(BF16)

    ctile = min(256, columns)
    chalf = columns // 2
    per_half = chalf // ctile

    def combine(zi, n):
        pp_copy(zi, n).wait_recv()
        qtx[zi, n] = (pbuf[zi, n, c].astype(F32) + prx[zi, n].astype(F32)).astype(BF16)
        qq_copy(zi, n).start()

    def down_pair(zi):
        picked = [picks(zi * 2 + ci) for ci in range(2)]
        slot_weight = jnp.concatenate([p[1] for p in picked], axis=0)

        def columns_of(n, carry):
            cols = pl.ds(pl.multiple_of(n * ctile, ctile), ctile)
            acc = jnp.zeros((slots, ctile), F32)
            for ti in range(tp):
                acc += jnp.dot(
                    hbuf[zi, ti],
                    down[ti * units : (ti + 1) * units, cols],
                    preferred_element_type=F32,
                )
            weighted = acc.astype(BF16).astype(F32) * slot_weight
            part = n // per_half
            put = pl.ds(pl.multiple_of((n % per_half) * ctile, ctile), ctile)
            for ci in range(2):
                spread = lax.dot_general(
                    picked[ci][0].astype(BF16),
                    weighted[ci * cap : (ci + 1) * cap, :].astype(BF16),
                    (((0,), (0,)), ((), ())),
                    preferred_element_type=F32,
                )
                pbuf[zi, part, ci, :, put] = spread.astype(BF16)

            @pl.when(n % per_half == per_half - 1)
            def _():
                pp_copy(zi, part).start()

            @pl.when((n == per_half - 1) & (zi == by_kind(o2, z)))
            def _():
                combine(o1, 0)
                combine(o1, 1)

            @pl.when((n == per_half) & (zi == o3))
            def _():
                combine(o3, 0)

            return carry

        lax.fori_loop(0, columns // ctile, columns_of, 0)

    def shared_down():
        all_s().wait_recv()
        for n in range(2):
            pp_copy(z, n).wait_recv()
        for n in range(columns // ctile):
            cols = slice(n * ctile, (n + 1) * ctile)
            put = slice(n % per_half * ctile, (n % per_half + 1) * ctile)
            part = n // per_half
            acc = pbuf[z, part, c, :, put].astype(F32) + prx[z, part, :, put].astype(F32)
            for ti in range(tp):
                acc += jnp.dot(
                    shbuf[ti],
                    sdown[ti * sunits : (ti + 1) * sunits, cols],
                    preferred_element_type=F32,
                )
            base[:, cols] = acc

    none = -1
    a_end, a_mid = (1, 2, 0, none, none, none, 3, none), (1, 2, none, none, none, none, 0, 3)
    p_end = (order[0], o1, none, o2, o3, none, none, none)
    p_mid = (order[0], o1, o2, o3, none, none, none, none)
    d_end = (none, none, order[0], none, o1, o2, o3, none)
    d_mid = (none, none, none, o1, order[0], o2, o3, none)

    def step(s, carry):
        qb = by_kind(table(s, a_end), table(s, a_mid))
        zi = by_kind(table(s, p_end), table(s, p_mid))
        zq = by_kind(table(s, d_end), table(s, d_mid))

        @pl.when(s == 1)
        def _():
            @pl.when(is_mid)
            def _():
                take_t(k4)

            take_xy(o1)

        @pl.when((s == 2) & is_mid)
        def _():
            wait_d(k6)
            send_d(k6)
            send_d(k5)
            take_xy(o2)

        @pl.when(s == by_kind(2, 6))
        def _():
            @pl.when(e > 0)
            def _():
                for h in halo_up:
                    h.wait_recv()

            @pl.when(e < ep - 1)
            def _():
                for h in halo_down:
                    h.wait_recv()

            turn_rows(kraw, kbuf, kv_heads, kgain_ref[...], 0, per_window, 0)
            last = (nq + 1) * per_window
            turn_rows(kraw, kbuf, kv_heads, kgain_ref[...], last, last + per_window, 0)

        @pl.when((s == 3) & is_end)
        def _():
            take_xy(o3)

        @pl.when(qb >= 0)
        def _():
            attend(qb)
            att_copy(qb).start()

        @pl.when(s == 0)
        def _():
            for piece, which in ((1, 0), (0, 1)):
                xy_landed(z, which, piece, piece * half, half).wait_recv()
                p_copy(z, (xn, yn)[which]).start()
            for which in range(2):
                diagonal_landed(which).wait_recv()
            p_copy(z, dn).start()
            send_d(z)

            @pl.when((c == 1) & (e < ep - 1))
            def _():
                for h in halo_up:
                    h.start()

            @pl.when((c == 0) & (e > 0))
            def _():
                for h in halo_down:
                    h.start()

            @pl.when(is_end)
            def _():
                zx_copy(0).start()
                zx_copy(1).start()

            all_w().wait_recv()
            for i in big:
                copies[i].wait()

        @pl.when(s == 1)
        def _():
            wait_d(k3)
            send_d(k3)

            @pl.when(is_mid)
            def _():
                wait_d(k5)

        @pl.when((s == 3) & is_end)
        def _():
            wait_d(k5)
            take_xy(o2)

        @pl.when((s == 4) & is_end)
        def _():
            wait_d(k6)

        @pl.when(zi >= 0)
        def _():
            scale_rows(zi, row_c)

            p_landed(zi).wait_recv()
            scale_rows(zi, row_o)
            project_pair(zi)

        @pl.when(s == 0)
        def _():
            send_h(z)
            shared_up()
            for d in range(1, tp):
                s_copy(d).start()

        @pl.when(s == 1)
        def _():
            forward_h(z)

            @pl.when(is_end)
            def _():
                take_t(k4)

            send_h(o1)

        @pl.when(s == by_kind(3, 2))
        def _():
            send_h(o2)

        @pl.when((s == 3) & is_mid)
        def _():
            forward_h(o2)

        @pl.when(s == by_kind(4, 3))
        def _():
            send_h(o3)

        @pl.when(zq >= 0)
        def _():
            h_landed(zq, 0, 1).wait_recv()
            h_landed(zq, 1, 0).wait_recv()
            g_landed(zq, 0).wait_recv()
            g_landed(zq, 1).wait_recv()
            down_pair(zq)

        @pl.when(zq == o2)
        def _():
            forward_h(o3)
            combine(o2, 0)
            combine(o2, 1)
            shared_down()

        @pl.when(zq == o3)
        def _():
            combine(o3, 1)

        return carry

    lax.fori_loop(0, nz + 4, step, 0)

    def sent(u, sem):
        rc(u, u, sem, pr.at[0], (partner, t)).wait_send()

    def drain(zi, carry):
        along(zi, lambda way: zt_copy(zi, way).wait_send())
        along(zi, lambda way: zd_copy(zi, way).wait_send())
        return carry

    lax.fori_loop(0, nz, drain, 0)

    @pl.when(is_end)
    def _():
        for sem in (xs, ys):
            sent(xbuf.at[:, t, pl.ds(row_c, tok), :], sem)

    @pl.when(is_mid)
    def _():
        for sem in (xs, ys):
            sent(xbuf.at[pl.ds(0, nz - 1), t, pl.ds(row_c, tok), :], sem)

    for which in range(2):
        sent(hbuf.at[:, t], (hxs, hys)[which])
        sent(hbuf.at[:, t, pl.ds(*h_parts[1 - which]), :], (gxs, gys)[which])
    sent(xbuf.at[:, :, pl.ds(row_c, tok), :], ps)
    sent(pbuf.at[:, :, other], pps)
    all_s().wait_send()
    all_w().wait_send()
    for which in range(2):
        diagonal(which).wait_send()

    @pl.when(e < ep - 1)
    def _():
        for h in halo_up:
            h.wait_send()

    @pl.when(e > 0)
    def _():
        for h in halo_down:
            h.wait_send()

    @pl.when(is_end)
    def _():
        for which in range(2):
            zx_copy(which).wait_send()

    for qb in range(nq):
        att_copy(qb).wait()

    outs = []
    for n in range(2):
        all_qq(n).wait_recv()
        cols = slice(n * chalf, (n + 1) * chalf)
        acc = base[:, cols]
        for i in range(1, nz):
            acc += qrx[order[i], n].astype(F32)
        obuf[n] = acc.astype(BF16)
        outs.append(pltpu.make_async_copy(obuf.at[n], out_hbm.at[:, cols], lsem.at[4 + n]))
        outs[-1].start()

    for i in range(1, nz):
        sent(qtx.at[order[i]], qqs.at[order[i]])
    for cp in outs:
        cp.wait()


def fast_shards(
    query_vectors,
    key_vectors,
    value_vectors,
    query_gain,
    key_gain,
    sink_logits,
    moe_rows,
    norm_gain,
    expert_ids,
    route_weights,
    expert_gate,
    expert_up,
    expert_down,
    shared_gate,
    shared_up,
    shared_down,
):
    ep, tp = lax.axis_size("ep"), lax.axis_size("tp")
    nz = ep // 2
    tok, width = moe_rows.shape
    cap = max(2, 3 * tok * TOP_K // (2 * ep))
    tok_a = query_vectors.shape[0]
    heads = sink_logits.shape[0]
    kv_heads = key_vectors.shape[1] // HEAD_DIM
    group = heads // kv_heads
    units = expert_gate.shape[2]
    columns = expert_down.shape[2]
    sunits = shared_gate.shape[1]
    sizes = (ep, tp, nz, tok, width, cap, tok_a, kv_heads, group, units, columns, sunits)
    full = tp * width
    extent = tok_a + 2 * WINDOW
    padded_tok = (tok + LANES - 1) // LANES * LANES
    nq = tok_a // WINDOW

    hb = pl.BlockSpec(memory_space=pl.ANY)
    dma = pltpu.SemaphoreType.DMA
    slots = 2 * cap
    kvw = kv_heads * HEAD_DIM
    qw = heads * HEAD_DIM
    return pl.pallas_call(
        functools.partial(line_kernel, sizes),
        out_shape=(
            jax.ShapeDtypeStruct((tok_a, qw), BF16),
            jax.ShapeDtypeStruct((tok, columns), BF16),
        ),
        in_specs=[hb] * 16,
        out_specs=(hb, hb),
        scratch_shapes=[
            pltpu.VMEM((nz, tp, 2 * tok, width), BF16),
            pltpu.VMEM((full, units), BF16),
            pltpu.VMEM((full, units), BF16),
            pltpu.VMEM((tp * units, columns), BF16),
            pltpu.VMEM((full, sunits), BF16),
            pltpu.VMEM((full, sunits), BF16),
            pltpu.VMEM((tp * sunits, columns), BF16),
            pltpu.VMEM((tok_a, qw), BF16),
            pltpu.VMEM((tok_a, qw), BF16),
            pltpu.VMEM((extent, kvw), BF16),
            pltpu.VMEM((extent, kvw), BF16),
            pltpu.VMEM((extent, kvw), BF16),
            pltpu.VMEM((tok_a, qw), BF16),
            pltpu.VMEM((2, tok, columns // 2), BF16),
            pltpu.VMEM((tok, columns), F32),
            pltpu.VMEM((extent, LANES), F32),
            pltpu.VMEM((extent, LANES), F32),
            pltpu.VMEM((ep, ep, padded_tok), F32),
            pltpu.VMEM((1, HEAD_DIM), F32),
            pltpu.VMEM((1, HEAD_DIM), F32),
            pltpu.VMEM((1, heads), F32),
            pltpu.VMEM((1, full), F32),
            pltpu.VMEM((TOP_K, tok), jnp.int32),
            pltpu.VMEM((TOP_K, tok), F32),
            pltpu.VMEM((2 * tok, full), BF16),
            pltpu.VMEM((2 * tok, LANES), F32),
            pltpu.VMEM((2 * tok, units), BF16),
            pltpu.VMEM((nz, tp, slots, units), BF16),
            pltpu.VMEM((tp, tok, sunits), BF16),
            pltpu.VMEM((nz, 2, 2, tok, columns // 2), BF16),
            pltpu.VMEM((nz, 2, tok, columns // 2), BF16),
            pltpu.VMEM((nz, 2, tok, columns // 2), BF16),
            pltpu.VMEM((nz, 2, tok, columns // 2), BF16),
            dma((16,)),
            dma((nz, 2)),
            dma((nz,)),
            dma((nz, 2)),
            dma((nz,)),
        ]
        + [dma((2,))] * 2
        + [dma, dma((nz, 2))] * 2
        + [dma((2,))] * 2
        + [dma, dma((nz,))]
        + [dma, dma((nz, 2))] * 2
        + [dma, dma((nz,))] * 2
        + [dma] * 4
        + [dma((4,))] * 2
        + [dma, dma((nz, 2)), dma((nz,)), dma((2,))],
        compiler_params=pltpu.CompilerParams(
            collective_id=0, has_side_effects=True, vmem_limit_bytes=50 * 1024 * 1024
        ),
    )(
        *(
            pltpu.with_memory_space_constraint(x, pltpu.HBM)
            for x in (
                query_vectors,
                key_vectors,
                value_vectors,
                query_gain[None, :],
                key_gain[None, :],
                sink_logits[None, :],
                moe_rows,
                norm_gain[None, :],
                expert_ids.T,
                route_weights.T,
                expert_gate,
                expert_up,
                expert_down,
                shared_gate,
                shared_up,
                shared_down,
            )
        )
    )


def choose(*args):
    ep, tp = lax.axis_size("ep"), lax.axis_size("tp")
    query, rows = args[0], args[6]
    kv_heads = args[1].shape[1] // HEAD_DIM
    tok, width = rows.shape
    cap = max(2, 3 * tok * TOP_K // (2 * ep))
    gathered = ep * tok * tp * width * 2
    fits = (
        gathered <= 16 * 1024 * 1024
        and tp == 4
        and ep == 8
        and (2 * cap) % 16 == 0
        and cap % 8 == 0
        and query.shape[0] % GRID_W == 0
        and query.shape[0] == WINDOW * (ep // 2)
        and tok % 32 == 0
        and tok <= 2 * LANES
    )
    return fast_shards(*args) if fits else shards(*args)


def solution(mesh):
    placed = (
        P("ep", "tp"),
        P("ep", "tp"),
        P("ep", "tp"),
        P(),
        P(),
        P("tp"),
        P("ep", "tp"),
        P(),
        P("ep", None),
        P("ep", None),
        P("ep", None, "tp"),
        P("ep", None, "tp"),
        P("ep", None, "tp"),
        P(None, "tp"),
        P(None, "tp"),
        P(None, "tp"),
    )
    return jax.shard_map(
        choose,
        mesh=mesh,
        in_specs=placed,
        out_specs=(P("ep", "tp"), P("ep", "tp")),
        check_vma=False,
    )
```

```python
import functools
import math

import jax
import jax.numpy as jnp
from jax import lax
from jax.experimental import pallas as pl
from jax.experimental.pallas import tpu as pltpu
from jax.sharding import PartitionSpec as P

HEAD_DIM = 128
WINDOW = 128
GRID_W = 64
D = 4096
TOP_K = 4


epsilon = 1e-06
rotary_base = 10000.0


def padded_2(block, sides, width):
    for axis, dim in sides:
        count = lax.axis_size(axis)
        forward = [(i, i + 1) for i in range(count - 1)]
        backward = [(target, source) for source, target in forward]
        low = lax.ppermute(
            lax.slice_in_dim(block, block.shape[dim] - width, None, axis=dim), axis, forward
        )
        high = lax.ppermute(lax.slice_in_dim(block, 0, width, axis=dim), axis, backward)
        block = jnp.concatenate([low, block, high], axis=dim)
    return block


def half_turn(halves):
    leading, trailing = jnp.split(halves, 2, axis=-1)
    return jnp.concatenate([-trailing, leading], axis=-1)


def rotate_heads(vectors, head_gain, positions):
    floats = vectors.astype(jnp.float32)
    normed = (
        floats * lax.rsqrt(jnp.mean(floats * floats, axis=-1, keepdims=True) + epsilon) * head_gain
    )
    quarter = HEAD_DIM // 4
    freq_index = jnp.arange(quarter, dtype=jnp.int32).astype(jnp.float32)
    inverse = rotary_base ** (-4.0 * freq_index / HEAD_DIM)
    grid_row = (positions // GRID_W).astype(jnp.float32)[:, None] * inverse
    grid_col = (positions % GRID_W).astype(jnp.float32)[:, None] * inverse
    angles = jnp.concatenate([grid_row, grid_row, grid_col, grid_col], axis=-1)[:, None, :]
    row_half, col_half = jnp.split(normed, 2, axis=-1)
    turned = jnp.concatenate([half_turn(row_half), half_turn(col_half)], axis=-1)
    return (normed * jnp.cos(angles) + turned * jnp.sin(angles)).astype(jnp.bfloat16)


def attend_window(query_vectors, key_vectors, value_vectors, query_gain, key_gain, sink_logits):
    length = query_vectors.shape[0]
    heads_here = sink_logits.shape[0]
    kv_here = key_vectors.shape[1] // HEAD_DIM
    grouping = heads_here // kv_here
    shard_start = lax.axis_index("ep") * length
    positions = shard_start + jnp.arange(length, dtype=jnp.int32)
    queries = rotate_heads(
        query_vectors.reshape(length, heads_here, HEAD_DIM), query_gain, positions
    )
    turned_keys = rotate_heads(key_vectors.reshape(length, kv_here, HEAD_DIM), key_gain, positions)
    turned_keys = turned_keys.reshape(length, kv_here * HEAD_DIM)
    padded = padded_2(jnp.stack([turned_keys, value_vectors]), (("ep", 1),), WINDOW)
    extent = length + 2 * WINDOW
    near_keys = padded[0].reshape(extent, kv_here, HEAD_DIM)
    near_values = padded[1].reshape(extent, kv_here, HEAD_DIM)
    key_pos = shard_start - WINDOW + jnp.arange(extent, dtype=jnp.int32)
    inside = (
        (jnp.abs(positions[:, None] - key_pos[None, :]) <= WINDOW)
        & (key_pos >= 0)[None, :]
        & (key_pos < lax.axis_size("ep") * length)[None, :]
    )
    scores = jnp.einsum(
        "qhgd,khd->hgqk",
        queries.reshape(length, kv_here, grouping, HEAD_DIM),
        near_keys,
        preferred_element_type=jnp.float32,
    ) * HEAD_DIM ** (-0.5)
    raised = jnp.where(inside, jnp.exp(scores), 0.0)
    denominator = jnp.exp(sink_logits).reshape(kv_here, grouping)[:, :, None] + jnp.sum(
        raised, axis=-1
    )
    weights = (raised / denominator[..., None]).astype(jnp.bfloat16)
    mixed = jnp.einsum("hgqk,khd->qhgd", weights, near_values, preferred_element_type=jnp.float32)
    return mixed.astype(jnp.bfloat16).reshape(length, heads_here * HEAD_DIM)


def project(block_rows, gain_piece, gate_rows, up_rows):
    floats = block_rows.astype(jnp.float32)
    weighted = (floats * gain_piece).astype(jnp.bfloat16)
    gate_sum = jnp.dot(weighted, gate_rows, preferred_element_type=jnp.float32)
    up_sum = jnp.dot(weighted, up_rows, preferred_element_type=jnp.float32)
    return (gate_sum, up_sum, jnp.sum(floats * floats, axis=1))


def activate(gate_sum, up_sum, squares):
    factor = lax.rsqrt(squares / D + epsilon)[:, None]
    return (jax.nn.silu(gate_sum * factor) * (up_sum * factor)).astype(jnp.bfloat16)


def shards(
    query_vectors,
    key_vectors,
    value_vectors,
    query_gain,
    key_gain,
    sink_logits,
    moe_rows,
    norm_gain,
    expert_ids,
    route_weights,
    expert_gate,
    expert_up,
    expert_down,
    shared_gate,
    shared_up,
    shared_down,
):
    attended = attend_window(
        query_vectors, key_vectors, value_vectors, query_gain, key_gain, sink_logits
    )
    ep_size = lax.axis_size("ep")
    tokens_here, width_here = moe_rows.shape
    capacity = max(2, 3 * tokens_here * TOP_K // (2 * ep_size))
    slots_all = ep_size * capacity
    flat_ids = expert_ids.reshape(-1)
    onehot = (flat_ids[:, None] == jnp.arange(ep_size, dtype=jnp.int32)[None, :]).astype(jnp.int32)
    slot_index = jnp.sum((jnp.cumsum(onehot, axis=0) - onehot) * onehot, axis=1)
    target = flat_ids * capacity + slot_index
    matches = target[None, :] == jnp.arange(slots_all, dtype=jnp.int32)[:, None]
    present = jnp.any(matches, axis=1)
    owner_row = jnp.arange(tokens_here * TOP_K, dtype=jnp.int32) // TOP_K
    source_row = jnp.sum(jnp.where(matches, owner_row[None, :], 0), axis=1)
    local_gate = expert_gate[0]
    local_up = expert_up[0]
    local_down = expert_down[0]
    units_here = local_gate.shape[1]
    shared_units = shared_gate.shape[1]
    outgoing = jnp.where(
        present[:, None], jnp.take(moe_rows, source_row, axis=0), jnp.zeros((), jnp.bfloat16)
    )
    arrived = lax.all_to_all(
        outgoing.reshape(ep_size, capacity, width_here),
        "ep",
        split_axis=0,
        concat_axis=0,
        tiled=True,
    )
    arrived = arrived.reshape(slots_all, width_here)
    routed = project(
        lax.all_gather(arrived, "tp", axis=1, tiled=True), norm_gain, local_gate, local_up
    )
    shared = project(
        lax.all_gather(moe_rows, "tp", axis=1, tiled=True), norm_gain, shared_gate, shared_up
    )
    gate_sum, up_sum, squares, shared_gsum, shared_usum, own_squares = tuple(
        (new_term for new_term in routed + shared)
    )
    hidden = activate(gate_sum, up_sum, squares)
    shared_hidden = activate(shared_gsum, shared_usum, own_squares)
    packing = units_here // shared_units
    stacked = jnp.concatenate(
        [hidden, shared_hidden.reshape(tokens_here // packing, units_here)], axis=0
    )
    columns = local_down.shape[1]
    portion = lax.all_gather(stacked, "tp", axis=1, tiled=True)
    shards_in = portion.shape[1] // units_here
    routed = jnp.dot(portion[:slots_all], local_down, preferred_element_type=jnp.float32)
    shared_piece = portion[slots_all:].reshape(
        tokens_here // packing, shards_in, packing, shared_units
    )
    shared_piece = shared_piece.transpose(0, 2, 1, 3).reshape(tokens_here, shards_in * shared_units)
    shared = jnp.dot(shared_piece, shared_down, preferred_element_type=jnp.float32)
    returned = lax.all_to_all(
        routed.astype(jnp.bfloat16).reshape(ep_size, capacity, columns),
        "ep",
        split_axis=0,
        concat_axis=0,
        tiled=True,
    )
    returned = returned.reshape(slots_all, columns)
    picked = jnp.take(returned, target, axis=0).reshape(tokens_here, TOP_K, columns)
    combined = shared + jnp.sum(route_weights[:, :, None] * picked.astype(jnp.float32), axis=1)
    return (attended, combined.astype(jnp.bfloat16))


F32 = jnp.float32
BF16 = jnp.bfloat16
MESH = pl.DeviceIdType.MESH
LANES = 128


def line_kernel(
    sizes,
    q_hbm,
    k_hbm,
    v_hbm,
    qgain_hbm,
    kgain_hbm,
    sink_hbm,
    x_hbm,
    gain_hbm,
    ids_hbm,
    rw_hbm,
    gate_hbm,
    up_hbm,
    down_hbm,
    sgate_hbm,
    sup_hbm,
    sdown_hbm,
    att_hbm,
    out_hbm,
    xbuf,
    gate,
    up,
    down,
    sgate,
    sup,
    sdown,
    qraw,
    qbuf,
    kraw,
    kbuf,
    vbuf,
    abuf,
    obuf,
    base,
    cos_ref,
    sin_ref,
    wbuf,
    qgain_ref,
    kgain_ref,
    sink_ref,
    gain_ref,
    ids_ref,
    rw_ref,
    scaled,
    factor,
    hid,
    hbuf,
    shbuf,
    pbuf,
    prx,
    qtx,
    qrx,
    lsem,
    zts,
    ztr,
    zds,
    zdr,
    zxs,
    zxr,
    xs,
    xr,
    ys,
    yr,
    fs,
    fr,
    ps,
    pr,
    hxs,
    hxr,
    hys,
    hyr,
    gxs,
    gxr,
    gys,
    gyr,
    ss,
    sr,
    ws,
    wr,
    ks,
    kr,
    pps,
    ppr,
    qqs,
    qqr,
):
    ep, tp, nz, tok, width, cap, tok_a, kv_heads, group, units, columns, sunits = sizes
    e = lax.axis_index("ep")
    t = lax.axis_index("tp")
    z, c = e // 2, e % 2
    other = 1 - c
    partner = z * 2 + other
    tx, ty = t % 2, t // 2
    xn = ty * 2 + (1 - tx)
    yn = (1 - ty) * 2 + tx
    dn = (1 - ty) * 2 + (1 - tx)
    half = tok // 2
    slots = 2 * cap
    hcut = (slots // 2 + 15) // 16 * 16
    row_c = pl.multiple_of(c * tok, 16)
    row_o = pl.multiple_of(other * tok, 16)
    has_up, has_down = z < nz - 1, z > 0
    is_end = (z == 0) | (z == nz - 1)
    is_mid = jnp.logical_not(is_end)

    def by_z(*values):
        r = values[0]
        for i in range(1, nz):
            r = jnp.where(z == i, values[i], r)
        return r

    order = (z, by_z(1, 2, 1, 2), by_z(3, 3, 0, 0), by_z(2, 0, 3, 1))
    o1, o2, o3 = order[1:]
    k1, k2 = by_z(1, 2, 1, 2), by_z(2, 0, 3, 1)
    k3, k4 = by_z(1, 0, 3, 2), by_z(3, 3, 0, 0)
    k5, k6 = by_z(3, 2, 1, 0), by_z(2, 3, 0, 1)

    def table(s, values):
        r = jnp.int32(values[0])
        for i in range(1, len(values)):
            r = jnp.where(s == i, values[i], r)
        return r

    def by_kind(end, mid):
        return jnp.where(is_end, end, mid)

    def rc(src, dst, s_sem, r_sem, dev):
        return pltpu.make_async_remote_copy(
            src_ref=src,
            dst_ref=dst,
            send_sem=s_sem,
            recv_sem=r_sem,
            device_id=dev,
            device_id_type=MESH,
        )

    loads = [
        (x_hbm, xbuf.at[z, t, pl.ds(row_c, tok), :]),
        (q_hbm, qraw),
        (k_hbm, kraw.at[pl.ds(WINDOW, tok_a), :]),
        (v_hbm, vbuf.at[pl.ds(WINDOW, tok_a), :]),
        (gate_hbm.at[0], gate),
        (up_hbm.at[0], up),
        (sgate_hbm, sgate),
        (sup_hbm, sup),
        (down_hbm.at[0], down),
        (sdown_hbm, sdown),
        (ids_hbm, ids_ref),
        (rw_hbm, rw_ref),
        (qgain_hbm, qgain_ref),
        (kgain_hbm, kgain_ref),
        (sink_hbm, sink_ref),
        (gain_hbm, gain_ref),
    ]
    copies = [pltpu.make_async_copy(a, b, lsem.at[i]) for i, (a, b) in enumerate(loads)]

    barrier = pltpu.get_barrier_semaphore()
    for d in range(1, ep):
        pl.semaphore_signal(barrier, inc=1, device_id=((e + d) % ep, t), device_id_type=MESH)
    for d in range(1, tp):
        pl.semaphore_signal(barrier, inc=1, device_id=(e, (t + d) % tp), device_id_type=MESH)
    big = (4, 5, 6, 7, 8, 9)
    for i in (0, 10, 11, 1, 12, 2, 3, 13, 14, 15) + big:
        copies[i].start()

    quarter = HEAD_DIM // 4
    half_head = HEAD_DIM // 2
    extent = tok_a + 2 * WINDOW
    grid_rows = extent // GRID_W
    first_row = (e * tok_a - WINDOW) // GRID_W

    def angles(count, start):
        lane = lax.broadcasted_iota(jnp.int32, (count, LANES), 1)
        place = lax.broadcasted_iota(jnp.int32, (count, LANES), 0)
        exponent = (lane % quarter).astype(F32) * (-4.0 / HEAD_DIM)
        return (place + start).astype(F32) * jnp.exp(exponent * math.log(rotary_base))

    row_pad = (grid_rows + 7) // 8 * 8
    row_angles = angles(row_pad, first_row)
    col_angles = angles(GRID_W, 0)
    row_cos, row_sin = jnp.cos(row_angles), jnp.sin(row_angles)
    col_cos, col_sin = jnp.cos(col_angles), jnp.sin(col_angles)
    lane64 = lax.broadcasted_iota(jnp.int32, (GRID_W, LANES), 1)
    sign = jnp.where(lane64 % half_head < quarter, -1.0, 1.0)
    for g in range(grid_rows):
        rows = slice(g * GRID_W, (g + 1) * GRID_W)
        cos_ref[rows, :] = jnp.where(lane64 < half_head, row_cos[g : g + 1, :], col_cos)
        sin_ref[rows, :] = jnp.where(lane64 < half_head, row_sin[g : g + 1, :], col_sin) * sign

    copies[10].wait()
    copies[11].wait()
    expert = lax.broadcasted_iota(jnp.int32, (ep, tok), 0)
    by_token = jnp.zeros((ep, tok), F32)
    for k in range(TOP_K):
        by_token += jnp.where(ids_ref[k : k + 1, :] == expert, rw_ref[k : k + 1, :], 0.0)
    wbuf[e] = jnp.zeros(wbuf.shape[1:], F32)
    wbuf[e, :, :tok] = by_token

    pl.semaphore_wait(barrier, ep + tp - 2)

    def unit(zi, ti, row, first=0, count=tok):
        return xbuf.at[zi, ti, pl.ds(row + first, count), :]

    up_z = jnp.minimum(z + 1, nz - 1) * 2 + c
    down_z = jnp.maximum(z - 1, 0) * 2 + c

    def zt_copy(zi, way):
        u = unit(zi, t, row_c)
        return rc(u, u, zts.at[zi, way], ztr.at[zi], ((up_z, down_z)[way], t))

    def zd_copy(zi, way):
        u = unit(zi, dn, row_c)
        return rc(u, u, zds.at[zi, way], zdr.at[zi], ((up_z, down_z)[way], t))

    def along(zi, what):
        @pl.when((zi <= z) & has_up)
        def _():
            what(0)

        @pl.when((zi >= z) & has_down)
        def _():
            what(1)

    def send_t(zi):
        along(zi, lambda way: zt_copy(zi, way).start())

    def send_d(zi):
        along(zi, lambda way: zd_copy(zi, way).start())

    def zx_copy(which):
        u = unit(z, (xn, yn)[which], row_c)
        dev = jnp.where(z == 0, up_z, down_z)
        return rc(u, u, zxs.at[which], zxr.at[which], (dev, t))

    def zx_landed(which):
        u = unit(o3, (xn, yn)[which], row_c)
        return rc(u, u, zxs.at[which], zxr.at[which], (e, xn))

    def xy_copy(zi, which, piece, first, count):
        u = unit(zi, t, row_c, first, count)
        sems = (xs, xr) if which == 0 else (ys, yr)
        return rc(u, u, sems[0], sems[1].at[zi, piece], (e, (xn, yn)[which]))

    def xy_landed(zi, which, piece, first, count):
        u = unit(zi, (xn, yn)[which], row_c, first, count)
        sems = (xs, xr) if which == 0 else (ys, yr)
        return rc(u, u, sems[0], sems[1].at[zi, piece], (e, (xn, yn)[which]))

    def diagonal(which):
        source, first = ((yn, half), (xn, 0))[which]
        u = unit(z, source, row_c, first, half)
        return rc(u, u, fs.at[which], fr.at[which], (e, (xn, yn)[which]))

    def diagonal_landed(which):
        u = unit(z, dn, row_c, (half, 0)[which], half)
        return rc(u, u, fs.at[which], fr.at[which], (e, (xn, yn)[which]))

    def p_copy(zi, ti):
        u = unit(zi, ti, row_c)
        return rc(u, u, ps, pr.at[zi], (partner, t))

    def p_landed(zi):
        u = xbuf.at[zi, :, pl.ds(row_o, tok), :]
        return rc(u, u, ps, pr.at[zi], (partner, t))

    h_parts = ((0, hcut), (hcut, slots - hcut))

    def h_copy(zi, which, piece):
        u = hbuf.at[zi, t, pl.ds(*h_parts[piece]), :]
        sems = (hxs, hxr) if which == 0 else (hys, hyr)
        return rc(u, u, sems[0], sems[1].at[zi, piece], (e, (xn, yn)[which]))

    def h_landed(zi, which, piece):
        u = hbuf.at[zi, (xn, yn)[which], pl.ds(*h_parts[piece]), :]
        sems = (hxs, hxr) if which == 0 else (hys, hyr)
        return rc(u, u, sems[0], sems[1].at[zi, piece], (e, (xn, yn)[which]))

    def g_copy(zi, which):
        u = hbuf.at[zi, (yn, xn)[which], pl.ds(*h_parts[1 - which]), :]
        sems = (gxs, gxr) if which == 0 else (gys, gyr)
        return rc(u, u, sems[0], sems[1].at[zi], (e, (xn, yn)[which]))

    def g_landed(zi, which):
        u = hbuf.at[zi, dn, pl.ds(*h_parts[1 - which]), :]
        sems = (gxs, gxr) if which == 0 else (gys, gyr)
        return rc(u, u, sems[0], sems[1].at[zi], (e, (xn, yn)[which]))

    def s_copy(d):
        u = shbuf.at[t]
        return rc(u, u, ss, sr, (e, (t + d) % tp))

    def w_copy(d):
        u = wbuf.at[e]
        return rc(u, u, ws, wr, ((e + d) % ep, t))

    def all_s():
        u = shbuf.at[pl.ds(0, tp - 1)]
        return rc(u, u, ss, sr, (e, xn))

    def all_w():
        u = wbuf.at[pl.ds(0, ep - 1)]
        return rc(u, u, ws, wr, (partner, t))

    def all_qq(n):
        u = qrx.at[pl.ds(0, nz - 1), n]
        return rc(u, u, qqs.at[0], qqr.at[n], (partner, t))

    after, before = jnp.minimum(e + 1, ep - 1), jnp.maximum(e - 1, 0)
    tail, first = pl.ds(tok_a, WINDOW), pl.ds(WINDOW, WINDOW)
    low, high = pl.ds(0, WINDOW), pl.ds(WINDOW + tok_a, WINDOW)
    halo_up = [
        rc(b.at[tail, :], b.at[low, :], ks.at[i], kr.at[i], (after, t))
        for i, b in enumerate((kraw, vbuf))
    ]
    halo_down = [
        rc(b.at[first, :], b.at[high, :], ks.at[2 + i], kr.at[2 + i], (before, t))
        for i, b in enumerate((kraw, vbuf))
    ]

    def pp_copy(zi, n):
        return rc(pbuf.at[zi, n, other], prx.at[zi, n], pps, ppr.at[zi, n], (partner, t))

    def qq_copy(zi, n):
        return rc(qtx.at[zi, n], qrx.at[z, n], qqs.at[zi], qqr.at[n], (zi * 2 + c, t))

    copies[0].wait()
    xy_copy(z, 0, 0, 0, half).start()
    xy_copy(z, 1, 1, half, half).start()
    send_t(z)
    xy_copy(z, 0, 1, half, half).start()
    xy_copy(z, 1, 0, 0, half).start()
    p_copy(z, t).start()
    for d in range(1, ep):
        w_copy(d).start()
    for i in (1, 2, 3, 12, 13, 14, 15):
        copies[i].wait()

    @pl.when(c == 0)
    def _():
        for h in halo_up:
            h.start()

    @pl.when(c == 1)
    def _():
        for h in halo_down:
            h.start()

    @pl.when(e == 0)
    def _():
        kraw[0:WINDOW, :] = jnp.zeros((WINDOW, kv_heads * HEAD_DIM), BF16)
        vbuf[0:WINDOW, :] = jnp.zeros((WINDOW, kv_heads * HEAD_DIM), BF16)

    @pl.when(e == ep - 1)
    def _():
        end = slice(WINDOW + tok_a, 2 * WINDOW + tok_a)
        kraw[end, :] = jnp.zeros((WINDOW, kv_heads * HEAD_DIM), BF16)
        vbuf[end, :] = jnp.zeros((WINDOW, kv_heads * HEAD_DIM), BF16)

    trows = WINDOW
    lane = lax.broadcasted_iota(jnp.int32, (trows, LANES), 1)
    leading = (lane % half_head) < quarter

    def turn(block, head_gain, cos, sin):
        v = block.astype(F32)
        v = v * lax.rsqrt(jnp.mean(v * v, axis=-1, keepdims=True) + epsilon) * head_gain
        swapped = jnp.where(
            leading,
            pltpu.roll(v, HEAD_DIM - quarter, 1),
            pltpu.roll(v, quarter, 1),
        )
        return (v * cos + swapped * sin).astype(BF16)

    heads = kv_heads * group

    def turn_rows(src, dst, count, head_gain, lo, hi, shift):
        def body(i, carry):
            rows = pl.ds(pl.multiple_of(i * trows, trows), trows)
            turned = pl.ds(pl.multiple_of(i * trows + shift, trows), trows)
            cos, sin = cos_ref[turned, :], sin_ref[turned, :]
            for h in range(count):
                cols = slice(h * HEAD_DIM, (h + 1) * HEAD_DIM)
                dst[rows, cols] = turn(src[rows, cols], head_gain, cos, sin)
            return carry

        lax.fori_loop(lo, hi, body, 0)

    nq = tok_a // WINDOW
    per_window = WINDOW // trows
    turn_rows(qraw, qbuf, heads, qgain_ref[...], 0, nq * per_window, WINDOW)

    xy_landed(z, 0, 0, 0, half).wait_recv()
    diagonal(1).start()
    xy_landed(z, 1, 1, half, half).wait_recv()
    diagonal(0).start()

    turn_rows(kraw, kbuf, kv_heads, kgain_ref[...], per_window, (nq + 1) * per_window, 0)

    def take_t(zi, spread=True):
        u = unit(zi, t, row_c)
        rc(u, u, zts.at[zi, 0], ztr.at[zi], (e, xn)).wait_recv()
        if spread:
            xy_copy(zi, 0, 0, 0, tok).start()
            xy_copy(zi, 1, 0, 0, tok).start()
        send_t(zi)
        p_copy(zi, t).start()

    def wait_d(zi):
        u = unit(zi, dn, row_c)
        rc(u, u, zds.at[zi, 0], zdr.at[zi], (e, xn)).wait_recv()
        p_copy(zi, dn).start()

    def take_xy(zi):
        xy_landed(zi, 0, 0, 0, tok).wait_recv()
        p_copy(zi, xn).start()
        xy_landed(zi, 1, 0, 0, tok).wait_recv()
        p_copy(zi, yn).start()

    take_t(k1)

    @pl.when(is_mid)
    def _():
        take_t(k2, spread=False)

    span = 3 * WINDOW
    near = lax.broadcasted_iota(jnp.int32, (WINDOW, WINDOW), 1)
    mine = lax.broadcasted_iota(jnp.int32, (WINDOW, WINDOW), 0)
    exp_scale = HEAD_DIM ** (-0.5)

    def attend(qb):
        rows = pl.ds(pl.multiple_of(qb * WINDOW, WINDOW), WINDOW)
        keys = pl.ds(pl.multiple_of(qb * WINDOW, WINDOW), span)
        in_low = (near >= mine) & ((e > 0) | (qb > 0))
        in_high = (near <= mine) & ((e < ep - 1) | (qb < nq - 1))
        sinks = jnp.exp(sink_ref[...])
        for kh in range(kv_heads):
            kcols = slice(kh * HEAD_DIM, (kh + 1) * HEAD_DIM)
            kk = kbuf[keys, kcols]
            vv = vbuf[keys, kcols]
            for g in range(group):
                h = kh * group + g
                qcols = slice(h * HEAD_DIM, (h + 1) * HEAD_DIM)
                scores = lax.dot_general(
                    qbuf[rows, qcols], kk, (((1,), (1,)), ((), ())), preferred_element_type=F32
                )
                raised = jnp.exp(scores * exp_scale)
                parts = [
                    jnp.where(in_low, raised[:, :WINDOW], 0.0),
                    raised[:, WINDOW : 2 * WINDOW],
                    jnp.where(in_high, raised[:, 2 * WINDOW :], 0.0),
                ]
                total = jnp.sum(parts[0] + parts[1] + parts[2], axis=-1, keepdims=True)
                inverse = 1.0 / (total + sinks[:, h : h + 1])
                weights = jnp.concatenate([(p * inverse).astype(BF16) for p in parts], axis=1)
                abuf[rows, qcols] = jnp.dot(
                    weights, vv, preferred_element_type=F32
                ).astype(BF16)

    def att_copy(qb):
        rows = pl.ds(pl.multiple_of(qb * WINDOW, WINDOW), WINDOW)
        return pltpu.make_async_copy(abuf.at[rows, :], att_hbm.at[rows, :], lsem.at[qb])

    upper = (
        lax.broadcasted_iota(jnp.int32, (tok, tok), 0)
        < lax.broadcasted_iota(jnp.int32, (tok, tok), 1)
    ).astype(F32)

    def picks(block):
        weight = wbuf[block, pl.ds(e, 1), :][:, :tok]
        named = jnp.where(weight > 0.0, 1.0, 0.0)
        rank = jnp.dot(
            jnp.broadcast_to(named, (16, tok)).astype(BF16),
            upper.astype(BF16),
            preferred_element_type=F32,
        )[0:1, :]
        slot = lax.broadcasted_iota(jnp.int32, (cap, tok), 0).astype(F32)
        hot = jnp.where((slot == rank) & (named > 0.0), 1.0, 0.0)
        return hot, jnp.sum(hot * weight, axis=1, keepdims=True)

    def send_h(zi):
        for which, piece in ((0, 0), (1, 1), (0, 1), (1, 0)):
            h_copy(zi, which, piece).start()

    def forward_h(zi):
        h_landed(zi, 0, 0).wait_recv()
        g_copy(zi, 1).start()
        h_landed(zi, 1, 1).wait_recv()
        g_copy(zi, 0).start()

    chunk = 32

    def silu_pair(g, u, f):
        g = g * f
        return g / (1.0 + jnp.exp(-g)) * (u * f)

    tile = min(256, units)

    def scale_rows(zi, row):
        def scale(i, carry):
            rows = pl.ds(pl.multiple_of(row + i * chunk, chunk), chunk)
            squares = jnp.zeros((chunk, 1), F32)
            for ti in range(tp):
                v = xbuf[zi, ti, rows, :].astype(F32)
                squares += jnp.sum(v * v, axis=1, keepdims=True)
                cols = slice(ti * width, (ti + 1) * width)
                scaled[rows, cols] = (v * gain_ref[:, cols]).astype(BF16)
            f = lax.rsqrt(squares / (tp * width) + epsilon)
            factor[rows, :] = jnp.broadcast_to(f, (chunk, LANES))
            return carry

        lax.fori_loop(0, tok // chunk, scale, 0)

    def project_pair(zi):
        def columns_of(n, carry):
            @pl.when((n == 1) & is_end & (zi == z))
            def _():
                take_t(k2)

            @pl.when((n == 1) & is_end & (zi == o2))
            def _():
                forward_h(o1)

            @pl.when((n == 1) & is_end & (zi == o3))
            def _():
                forward_h(o2)

            @pl.when((n == 1) & is_mid & (zi == o2))
            def _():
                forward_h(o1)
                for which in range(2):
                    zx_landed(which).wait_recv()
                    p_copy(o3, (xn, yn)[which]).start()

            cols = pl.ds(pl.multiple_of(n * tile, tile), tile)
            g = jnp.dot(scaled[...], gate[:, cols], preferred_element_type=F32)
            u = jnp.dot(scaled[...], up[:, cols], preferred_element_type=F32)
            hid[:, cols] = silu_pair(g, u, factor[:, 0:1]).astype(BF16)
            return carry

        lax.fori_loop(0, units // tile, columns_of, 0)
        parts = []
        for ci in range(2):
            hot, _ = picks(zi * 2 + ci)
            parts.append(
                jnp.dot(
                    hot.astype(BF16),
                    hid[ci * tok : (ci + 1) * tok, :],
                    preferred_element_type=F32,
                )
            )
        hbuf[zi, t] = jnp.concatenate(parts, axis=0).astype(BF16)

    def shared_up():
        rows = pl.ds(row_c, tok)
        g = jnp.dot(scaled[rows, :], sgate[...], preferred_element_type=F32)
        u = jnp.dot(scaled[rows, :], sup[...], preferred_element_type=F32)
        shbuf[t] = silu_pair(g, u, factor[rows, 0:1]).astype(BF16)

    ctile = min(256, columns)
    chalf = columns // 2
    per_half = chalf // ctile

    def combine(zi, n):
        pp_copy(zi, n).wait_recv()
        qtx[zi, n] = (pbuf[zi, n, c].astype(F32) + prx[zi, n].astype(F32)).astype(BF16)
        qq_copy(zi, n).start()

    def down_pair(zi):
        picked = [picks(zi * 2 + ci) for ci in range(2)]
        slot_weight = jnp.concatenate([p[1] for p in picked], axis=0)

        def columns_of(n, carry):
            cols = pl.ds(pl.multiple_of(n * ctile, ctile), ctile)
            acc = jnp.zeros((slots, ctile), F32)
            for ti in range(tp):
                acc += jnp.dot(
                    hbuf[zi, ti],
                    down[ti * units : (ti + 1) * units, cols],
                    preferred_element_type=F32,
                )
            weighted = acc.astype(BF16).astype(F32) * slot_weight
            part = n // per_half
            put = pl.ds(pl.multiple_of((n % per_half) * ctile, ctile), ctile)
            for ci in range(2):
                spread = lax.dot_general(
                    picked[ci][0].astype(BF16),
                    weighted[ci * cap : (ci + 1) * cap, :].astype(BF16),
                    (((0,), (0,)), ((), ())),
                    preferred_element_type=F32,
                )
                pbuf[zi, part, ci, :, put] = spread.astype(BF16)

            @pl.when(n % per_half == per_half - 1)
            def _():
                pp_copy(zi, part).start()

            @pl.when((n == per_half - 1) & (zi == by_kind(o2, z)))
            def _():
                combine(o1, 0)
                combine(o1, 1)

            @pl.when((n == per_half) & (zi == o3))
            def _():
                combine(o3, 0)

            return carry

        lax.fori_loop(0, columns // ctile, columns_of, 0)

    def shared_down():
        all_s().wait_recv()
        for n in range(2):
            pp_copy(z, n).wait_recv()
        for n in range(columns // ctile):
            cols = slice(n * ctile, (n + 1) * ctile)
            put = slice(n % per_half * ctile, (n % per_half + 1) * ctile)
            part = n // per_half
            acc = pbuf[z, part, c, :, put].astype(F32) + prx[z, part, :, put].astype(F32)
            for ti in range(tp):
                acc += jnp.dot(
                    shbuf[ti],
                    sdown[ti * sunits : (ti + 1) * sunits, cols],
                    preferred_element_type=F32,
                )
            base[:, cols] = acc

    none = -1
    a_end, a_mid = (1, 2, 0, none, none, none, none, 3, none), (1, 2, none, none, none, none, none, 0, 3)
    p_end = (order[0], o1, none, o2, o3, none, none, none, none)
    p_mid = (order[0], o1, o2, o3, none, none, none, none, none)
    d_end = (none, none, order[0], none, o1, o2, o3, none, none)
    d_mid = (none, none, none, o1, order[0], o2, o3, none, none)

    def step(s, carry):
        qb = by_kind(table(s, a_end), table(s, a_mid))
        zi = by_kind(table(s, p_end), table(s, p_mid))
        zq = by_kind(table(s, d_end), table(s, d_mid))

        @pl.when(s == 1)
        def _():
            @pl.when(is_mid)
            def _():
                take_t(k4)

            take_xy(o1)

        @pl.when((s == 2) & is_mid)
        def _():
            wait_d(k6)
            send_d(k6)
            send_d(k5)
            take_xy(o2)

        @pl.when(s == by_kind(2, 7))
        def _():
            @pl.when(e > 0)
            def _():
                for h in halo_up:
                    h.wait_recv()

            @pl.when(e < ep - 1)
            def _():
                for h in halo_down:
                    h.wait_recv()

            turn_rows(kraw, kbuf, kv_heads, kgain_ref[...], 0, per_window, 0)
            last = (nq + 1) * per_window
            turn_rows(kraw, kbuf, kv_heads, kgain_ref[...], last, last + per_window, 0)

        @pl.when((s == 3) & is_end)
        def _():
            take_xy(o3)

        @pl.when(qb >= 0)
        def _():
            attend(qb)
            att_copy(qb).start()

        @pl.when(s == 0)
        def _():
            for piece, which in ((1, 0), (0, 1)):
                xy_landed(z, which, piece, piece * half, half).wait_recv()
                p_copy(z, (xn, yn)[which]).start()
            for which in range(2):
                diagonal_landed(which).wait_recv()
            p_copy(z, dn).start()
            send_d(z)

            @pl.when((c == 1) & (e < ep - 1))
            def _():
                for h in halo_up:
                    h.start()

            @pl.when((c == 0) & (e > 0))
            def _():
                for h in halo_down:
                    h.start()

            @pl.when(is_end)
            def _():
                zx_copy(0).start()
                zx_copy(1).start()

            all_w().wait_recv()
            for i in big:
                copies[i].wait()

        @pl.when(s == 1)
        def _():
            wait_d(k3)
            send_d(k3)

            @pl.when(is_mid)
            def _():
                wait_d(k5)

        @pl.when((s == 3) & is_end)
        def _():
            wait_d(k5)
            take_xy(o2)

        @pl.when((s == 4) & is_end)
        def _():
            wait_d(k6)

        @pl.when(zi >= 0)
        def _():
            scale_rows(zi, row_c)

            p_landed(zi).wait_recv()
            scale_rows(zi, row_o)
            project_pair(zi)

        @pl.when(s == 0)
        def _():
            send_h(z)
            shared_up()
            for d in range(1, tp):
                s_copy(d).start()

        @pl.when(s == 1)
        def _():
            forward_h(z)

            @pl.when(is_end)
            def _():
                take_t(k4)

            send_h(o1)

        @pl.when(s == by_kind(3, 2))
        def _():
            send_h(o2)

        @pl.when((s == 3) & is_mid)
        def _():
            forward_h(o2)

        @pl.when(s == by_kind(4, 3))
        def _():
            send_h(o3)

        @pl.when(zq >= 0)
        def _():
            h_landed(zq, 0, 1).wait_recv()
            h_landed(zq, 1, 0).wait_recv()
            g_landed(zq, 0).wait_recv()
            g_landed(zq, 1).wait_recv()
            down_pair(zq)

        @pl.when(zq == o2)
        def _():
            forward_h(o3)
            combine(o2, 0)
            combine(o2, 1)
            shared_down()

        @pl.when(zq == o3)
        def _():
            combine(o3, 1)

        return carry

    lax.fori_loop(0, nz + 5, step, 0)

    def sent(u, sem):
        rc(u, u, sem, pr.at[0], (partner, t)).wait_send()

    def drain(zi, carry):
        along(zi, lambda way: zt_copy(zi, way).wait_send())
        along(zi, lambda way: zd_copy(zi, way).wait_send())
        return carry

    lax.fori_loop(0, nz, drain, 0)

    @pl.when(is_end)
    def _():
        for sem in (xs, ys):
            sent(xbuf.at[:, t, pl.ds(row_c, tok), :], sem)

    @pl.when(is_mid)
    def _():
        for sem in (xs, ys):
            sent(xbuf.at[pl.ds(0, nz - 1), t, pl.ds(row_c, tok), :], sem)

    for which in range(2):
        sent(hbuf.at[:, t], (hxs, hys)[which])
        sent(hbuf.at[:, t, pl.ds(*h_parts[1 - which]), :], (gxs, gys)[which])
    sent(xbuf.at[:, :, pl.ds(row_c, tok), :], ps)
    sent(pbuf.at[:, :, other], pps)
    all_s().wait_send()
    all_w().wait_send()
    for which in range(2):
        diagonal(which).wait_send()

    @pl.when(e < ep - 1)
    def _():
        for h in halo_up:
            h.wait_send()

    @pl.when(e > 0)
    def _():
        for h in halo_down:
            h.wait_send()

    @pl.when(is_end)
    def _():
        for which in range(2):
            zx_copy(which).wait_send()

    for qb in range(nq):
        att_copy(qb).wait()

    outs = []
    for n in range(2):
        all_qq(n).wait_recv()
        cols = slice(n * chalf, (n + 1) * chalf)
        acc = base[:, cols]
        for i in range(1, nz):
            acc += qrx[order[i], n].astype(F32)
        obuf[n] = acc.astype(BF16)
        outs.append(pltpu.make_async_copy(obuf.at[n], out_hbm.at[:, cols], lsem.at[4 + n]))
        outs[-1].start()

    for i in range(1, nz):
        sent(qtx.at[order[i]], qqs.at[order[i]])
    for cp in outs:
        cp.wait()


def fast_shards(
    query_vectors,
    key_vectors,
    value_vectors,
    query_gain,
    key_gain,
    sink_logits,
    moe_rows,
    norm_gain,
    expert_ids,
    route_weights,
    expert_gate,
    expert_up,
    expert_down,
    shared_gate,
    shared_up,
    shared_down,
):
    ep, tp = lax.axis_size("ep"), lax.axis_size("tp")
    nz = ep // 2
    tok, width = moe_rows.shape
    cap = max(2, 3 * tok * TOP_K // (2 * ep))
    tok_a = query_vectors.shape[0]
    heads = sink_logits.shape[0]
    kv_heads = key_vectors.shape[1] // HEAD_DIM
    group = heads // kv_heads
    units = expert_gate.shape[2]
    columns = expert_down.shape[2]
    sunits = shared_gate.shape[1]
    sizes = (ep, tp, nz, tok, width, cap, tok_a, kv_heads, group, units, columns, sunits)
    full = tp * width
    extent = tok_a + 2 * WINDOW
    padded_tok = (tok + LANES - 1) // LANES * LANES
    nq = tok_a // WINDOW

    hb = pl.BlockSpec(memory_space=pl.ANY)
    dma = pltpu.SemaphoreType.DMA
    slots = 2 * cap
    kvw = kv_heads * HEAD_DIM
    qw = heads * HEAD_DIM
    return pl.pallas_call(
        functools.partial(line_kernel, sizes),
        out_shape=(
            jax.ShapeDtypeStruct((tok_a, qw), BF16),
            jax.ShapeDtypeStruct((tok, columns), BF16),
        ),
        in_specs=[hb] * 16,
        out_specs=(hb, hb),
        scratch_shapes=[
            pltpu.VMEM((nz, tp, 2 * tok, width), BF16),
            pltpu.VMEM((full, units), BF16),
            pltpu.VMEM((full, units), BF16),
            pltpu.VMEM((tp * units, columns), BF16),
            pltpu.VMEM((full, sunits), BF16),
            pltpu.VMEM((full, sunits), BF16),
            pltpu.VMEM((tp * sunits, columns), BF16),
            pltpu.VMEM((tok_a, qw), BF16),
            pltpu.VMEM((tok_a, qw), BF16),
            pltpu.VMEM((extent, kvw), BF16),
            pltpu.VMEM((extent, kvw), BF16),
            pltpu.VMEM((extent, kvw), BF16),
            pltpu.VMEM((tok_a, qw), BF16),
            pltpu.VMEM((2, tok, columns // 2), BF16),
            pltpu.VMEM((tok, columns), F32),
            pltpu.VMEM((extent, LANES), F32),
            pltpu.VMEM((extent, LANES), F32),
            pltpu.VMEM((ep, ep, padded_tok), F32),
            pltpu.VMEM((1, HEAD_DIM), F32),
            pltpu.VMEM((1, HEAD_DIM), F32),
            pltpu.VMEM((1, heads), F32),
            pltpu.VMEM((1, full), F32),
            pltpu.VMEM((TOP_K, tok), jnp.int32),
            pltpu.VMEM((TOP_K, tok), F32),
            pltpu.VMEM((2 * tok, full), BF16),
            pltpu.VMEM((2 * tok, LANES), F32),
            pltpu.VMEM((2 * tok, units), BF16),
            pltpu.VMEM((nz, tp, slots, units), BF16),
            pltpu.VMEM((tp, tok, sunits), BF16),
            pltpu.VMEM((nz, 2, 2, tok, columns // 2), BF16),
            pltpu.VMEM((nz, 2, tok, columns // 2), BF16),
            pltpu.VMEM((nz, 2, tok, columns // 2), BF16),
            pltpu.VMEM((nz, 2, tok, columns // 2), BF16),
            dma((16,)),
            dma((nz, 2)),
            dma((nz,)),
            dma((nz, 2)),
            dma((nz,)),
        ]
        + [dma((2,))] * 2
        + [dma, dma((nz, 2))] * 2
        + [dma((2,))] * 2
        + [dma, dma((nz,))]
        + [dma, dma((nz, 2))] * 2
        + [dma, dma((nz,))] * 2
        + [dma] * 4
        + [dma((4,))] * 2
        + [dma, dma((nz, 2)), dma((nz,)), dma((2,))],
        compiler_params=pltpu.CompilerParams(
            collective_id=0, has_side_effects=True, vmem_limit_bytes=50 * 1024 * 1024
        ),
    )(
        *(
            pltpu.with_memory_space_constraint(x, pltpu.HBM)
            for x in (
                query_vectors,
                key_vectors,
                value_vectors,
                query_gain[None, :],
                key_gain[None, :],
                sink_logits[None, :],
                moe_rows,
                norm_gain[None, :],
                expert_ids.T,
                route_weights.T,
                expert_gate,
                expert_up,
                expert_down,
                shared_gate,
                shared_up,
                shared_down,
            )
        )
    )


def choose(*args):
    ep, tp = lax.axis_size("ep"), lax.axis_size("tp")
    query, rows = args[0], args[6]
    kv_heads = args[1].shape[1] // HEAD_DIM
    tok, width = rows.shape
    cap = max(2, 3 * tok * TOP_K // (2 * ep))
    gathered = ep * tok * tp * width * 2
    fits = (
        gathered <= 16 * 1024 * 1024
        and tp == 4
        and ep == 8
        and (2 * cap) % 16 == 0
        and cap % 8 == 0
        and query.shape[0] % GRID_W == 0
        and query.shape[0] == WINDOW * (ep // 2)
        and tok % 32 == 0
        and tok <= 2 * LANES
    )
    return fast_shards(*args) if fits else shards(*args)


def solution(mesh):
    placed = (
        P("ep", "tp"),
        P("ep", "tp"),
        P("ep", "tp"),
        P(),
        P(),
        P("tp"),
        P("ep", "tp"),
        P(),
        P("ep", None),
        P("ep", None),
        P("ep", None, "tp"),
        P("ep", None, "tp"),
        P("ep", None, "tp"),
        P(None, "tp"),
        P(None, "tp"),
        P(None, "tp"),
    )
    return jax.shard_map(
        choose,
        mesh=mesh,
        in_specs=placed,
        out_specs=(P("ep", "tp"), P("ep", "tp")),
        check_vma=False,
    )
```
